32 devices in a mesh: rep: 2 (over x), fs: 8 (over z, y), tp: 2 (over core).
Axes of the slice: x: 2, y: 2, z: 4, core: 2. Of those that a mesh axis runs over, the one named last changes fastest.
Arguments:
- inputs: bfloat16 [4096, 2048], P(('rep', 'fs', 'tp')), may hold values from -6 to 6
- cotangent: bfloat16 [4096, 2048], P(('rep', 'fs', 'tp')), may hold values from -6 to 6
- up_weight: bfloat16 [2048, 4096], P('fs', 'tp'), may hold values from -0.125 to 0.125
- down_weight: bfloat16 [4096, 2048], P('tp', 'fs'), may hold values from -0.09375 to 0.09375
Outputs:
- input_grad: bfloat16 [4096, 2048], P(('rep', 'fs', 'tp'))
- up_grad: float32 [2048, 4096], P('fs', 'tp')
- down_grad: float32 [4096, 2048], P('tp', 'fs')
The draws below stay inside these ranges and needn't reach their ends.
All inputs are finite; a program needn't handle non-finite values.
Results may differ from the reference program's by a relative error of at most 0.013.
Values may be sent and summed in bfloat16 or wider, within the bound.
A program may use at most 128 MiB of HBM per device.

```python
import jax
import jax.numpy as jnp
from jax import lax

D = 2048
FF = 4096
TOKENS = 4096
N_TP = 2


def raised(array, stream_key, source, target, blocks, factor):
    owner, partner = [(jnp.arange(array.shape[dim]) // (array.shape[dim] // blocks)).reshape([-1 if axis == dim else 1 for axis in range(array.ndim)]) for dim in (source, target)]
    chosen = jax.random.permutation(stream_key, blocks)[partner]
    strong = (owner == chosen) | (owner == (partner + blocks // 2) % blocks)
    return jnp.where(strong, factor * array, array)


def shard_levels(key, shape, pieces, low, top_value):
    def one(axis_at, blocks):
        steps = jax.random.uniform(jax.random.fold_in(jax.random.fold_in(key, 6), axis_at), (blocks,), jnp.float32, low / len(pieces), top_value / len(pieces))
        return jnp.repeat(jnp.exp(steps), shape[axis_at] // blocks).reshape((-1,) + (1,) * (len(shape) - axis_at - 1))

    level = one(*pieces[0])
    for cut in pieces[1:]:
        level = level * one(*cut)
    return level


def gaussian(key, shape, scale, bound, cuts=(), held_as=jnp.bfloat16):
    level = shard_levels(key, shape, cuts, -0.22, 0.18) if cuts else 1.0
    drawn = jax.random.normal(key, shape, jnp.float32) * scale * level
    return jnp.minimum(jnp.maximum(drawn, -bound), bound).astype(held_as)


def noise_with(stream_key, dims, deviation, bound, pieces, heavy, held_as=jnp.bfloat16):
    entries = deviation * jax.random.normal(stream_key, dims, jnp.float32)
    if pieces:
        entries = entries * shard_levels(stream_key, dims, pieces, -0.22, 0.18)
    return jnp.clip(raised(entries, jax.random.fold_in(stream_key, 3), *heavy), -bound, bound).astype(held_as)


def setup_inputs(seed: int = 0) -> dict:
    key_list = jax.random.split(jax.random.key(seed), 5)
    inputs = noise_with(key_list[0], (TOKENS, D), 1.0, 6.0, ((0, 32),), (0, 1, 32, 2.75))
    cotangent = noise_with(key_list[1], (TOKENS, D), 1.0, 6.0, ((0, 32),), (0, 1, 32, 2.75))
    up_weight = gaussian(key_list[2], (D, FF), D ** -0.5, 0.125, ((0, 8), (1, 2)))
    down_weight = gaussian(key_list[3], (FF, D), FF ** -0.5, 0.09375, ((0, 2), (1, 8)))
    return dict(inputs=inputs, cotangent=cotangent, up_weight=up_weight, down_weight=down_weight)


def reference(inputs, cotangent, up_weight, down_weight):
    pre_active = jnp.dot(inputs, up_weight, preferred_element_type=jnp.float32)
    active = jnp.maximum(pre_active, 0.0)
    activation = (active * active).astype(jnp.bfloat16)
    activation_grad = jnp.dot(cotangent, down_weight.T, preferred_element_type=jnp.float32)
    pre_grad = (2.0 * active * activation_grad).astype(jnp.bfloat16)
    block_width = FF // N_TP

    def add_block(index, running):
        offset = (index * block_width).astype(jnp.int32)
        grad_cols = lax.dynamic_slice_in_dim(pre_grad, offset, block_width, 1)
        weight_cols = lax.dynamic_slice_in_dim(up_weight, offset, block_width, 1)
        partial_sum = jnp.dot(grad_cols, weight_cols.T, preferred_element_type=jnp.float32)
        rounded = lax.optimization_barrier(partial_sum.astype(jnp.bfloat16))
        return running + rounded.astype(jnp.float32)

    start_sum = jnp.zeros((inputs.shape[0], D), jnp.float32)
    input_grad = lax.fori_loop(jnp.int32(0), jnp.int32(N_TP), add_block, start_sum).astype(jnp.bfloat16)
    loss_scale = TOKENS ** -0.5
    up_grad = jnp.dot(inputs.T, pre_grad, preferred_element_type=jnp.float32) * loss_scale
    down_grad = jnp.dot(activation.T, cotangent, preferred_element_type=jnp.float32) * loss_scale
    return (input_grad, up_grad, down_grad)
```

```python
import functools
import math

import jax
import jax.numpy as jnp
from jax import lax
from jax.experimental import pallas as pl
from jax.experimental.pallas import tpu as pltpu
from jax.sharding import PartitionSpec as P

MESH = pl.DeviceIdType.MESH
CHUNKS = 2
BF16, F32 = jnp.bfloat16, jnp.float32
NT = (((1,), (1,)), ((), ()))


def ring_place(f, n):
    odd = lax.rem(f, 2)
    half = lax.div(f, 2)
    return half * (1 - odd) + (n - 1 - half) * odd


def ring_member(p, n):
    back = lax.div(p, (n + 1) // 2)
    return 2 * p * (1 - back) + (2 * n - 1 - 2 * p) * back


def tile_of(size, most):
    while size % most:
        most //= 2
    return most


def ring_kernel(
    R, n, T,
    x_ref, c_ref, u_ref, d_ref,
    ig_ref, gu_ref, gd_ref,
    xg, cg, xt, ug, dg, pre, agr, pg, at,
    igp, itr, isum, irr, us, ur, ds_, dr_, fu, fd, fur, fdr,
    ag_ss, ag_rs, rs_ss, rs_rs, tr_ss, tr_rs, tt_ss, tt_rs,
    it_ss, it_rs, ir_ss, ir_rs, f_ss, f_rs,
):
    r, f, t = lax.axis_index("rep"), lax.axis_index("fs"), lax.axis_index("tp")
    tok, db = x_ref.shape[0], u_ref.shape[0]
    C, w = pre.shape[0], pre.shape[2]
    hb = C * w
    rows = R * T * tok

    def hidden(place, ch):
        return pl.ds(pl.multiple_of(place * hb + ch * w, w), w)

    for ref, full in ((x_ref, xg), (c_ref, cg)):
        for q in range(n):
            full[q, 0:tok, :] = ref[:, q * db:(q + 1) * db]
    p = ring_place(f, n)

    def member(q):
        return ring_member(lax.rem(p + q + n, n), n)

    def ring_dev(sign):
        return (r, member(sign), t)

    def rep_dev(q):
        return (lax.rem(r + q + R, R), f, t)

    def tp_dev(q):
        return (r, f, lax.rem(t + q + T, T))

    barrier = pltpu.get_barrier_semaphore()
    peers = [ring_dev(1), ring_dev(-1)]
    peers += [rep_dev(q) for q in range(1, R)] + [tp_dev(q) for q in range(1, T)]
    for peer in peers:
        pl.semaphore_signal(barrier, inc=1, device_id=peer, device_id_type=MESH)
    pl.semaphore_wait(barrier, len(peers))

    def remote(src, dst, ssem, rsem, dev):
        return pltpu.make_async_remote_copy(
            src_ref=src, dst_ref=dst, send_sem=ssem, recv_sem=rsem,
            device_id=dev, device_id_type=MESH,
        )

    long, short = n // 2, (n - 1) // 2
    streams = [(0, 1, long), (0, -1, short), (1, 1, short), (1, -1, long)]
    hops = max(long, short)
    def own(g, ch):
        return u_ref.at[:, hidden(r, ch)] if g == 0 else d_ref.at[hidden(r, ch), :]

    held = (ug, dg)

    def slot(sign, s):
        return (n - s if sign > 0 else s) - 1

    def gather_copy(ch, i, s):
        g, sign, _ = streams[i]
        src = own(g, ch) if s == 1 else held[g].at[slot(sign, s - 1), ch]
        return remote(
            src, held[g].at[slot(sign, s), ch],
            ag_ss.at[ch, i, s - 1], ag_rs.at[ch, i, s - 1], ring_dev(sign),
        )

    sends = []

    def go(copy):
        copy.start()
        sends.append(copy)
        return copy

    flying = {}

    def gather_first(ch):
        for i, (g, sign, k) in enumerate(streams):
            if k >= 1:
                flying[ch, i, 1] = go(gather_copy(ch, i, 1))

    gather_first(0)

    tokens = tuple((full.at[:, 0:tok, :], full) for full in (xg, cg))

    def span(dt, dr):
        return pl.ds((dt * R + dr) * tok, tok)

    rep_copies = {}
    for dr in range(1, R):
        for j, (ref, full) in enumerate(tokens):
            rep_copies[j, dr] = go(remote(
                ref, full.at[:, span(0, dr), :], tr_ss.at[j, dr], tr_rs.at[j, dr], rep_dev(-dr)
            ))
    tp_copies = {}
    for dt in range(1, T):
        for j, (ref, full) in enumerate(tokens):
            tp_copies[j, dt, 0] = go(remote(
                ref, full.at[:, span(dt, 0), :], tt_ss.at[j, dt, 0], tt_rs.at[j, dt, 0],
                tp_dev(-dt),
            ))

    row_tile = tile_of(rows, 256)

    def gather_dot(ch, g, block, q, first=False):
        b = member(q)
        out, full = ((pre, xg), (agr, cg))[g]

        @pl.loop(0, rows // row_tile)
        def _(i):
            part = pl.ds(pl.multiple_of(i * row_tile, row_tile), row_tile)
            lhs = full[b, part, :]
            if g == 0:
                val = jnp.dot(lhs, block[...], preferred_element_type=F32)
            else:
                val = lax.dot_general(lhs, block[...], NT, preferred_element_type=F32)
            if first:
                out[ch, part, :] = val
            else:
                out[ch, part, :] += val

    def finish_tokens():
        for dr in range(1, R):
            for j, (ref, full) in enumerate(tokens):
                rep_copies[j, dr].wait_recv()
                for dt in range(1, T):
                    tp_copies[j, dt, dr] = go(remote(
                        full.at[:, span(0, dr), :], full.at[:, span(dt, dr), :],
                        tt_ss.at[j, dt, dr], tt_rs.at[j, dt, dr], tp_dev(-dt),
                    ))
        for copy in tp_copies.values():
            copy.wait_recv()

        @pl.loop(0, n)
        def _(b):
            xt[b] = xg[b].T

        for ch in range(C):
            gather_dot(ch, 0, own(0, ch), 0, True)
            gather_dot(ch, 1, own(1, ch), 0, True)

    act_tile = tile_of(rows, 128)

    def activate(ch):
        @pl.loop(0, rows // act_tile)
        def _(i):
            part = pl.ds(pl.multiple_of(i * act_tile, act_tile), act_tile)
            active = jnp.maximum(pre[ch, part, :], 0.0)
            pg[ch, part, :] = (2.0 * active * agr[ch, part, :]).astype(BF16)
            at[ch, :, part] = (active * active).astype(BF16).T

    def gather(ch, before_last):
        for s in range(1, hops + 1):
            if s == hops:
                before_last()
            for i, (g, sign, k) in enumerate(streams):
                if s <= k:
                    flying[ch, i, s].wait_recv()
                    if s < k:
                        flying[ch, i, s + 1] = go(gather_copy(ch, i, s + 1))
            if s == 1 and ch == 0:
                finish_tokens()
            for i, (g, sign, k) in enumerate(streams):
                if s <= k:
                    gather_dot(ch, g, held[g].at[slot(sign, s), ch], -sign * s)
        if hops == 0:
            if ch == 0:
                finish_tokens()
            before_last()
        activate(ch)

    def grad_block(ch, g, q, dst, arrived):
        b = member(q)
        height = (db, w)[g]
        tile = tile_of(height, 256)

        @pl.loop(0, height // tile)
        def _(i):
            part = pl.ds(pl.multiple_of(i * tile, tile), tile)
            if g == 0:
                val = jnp.dot(xt[b, part, :], pg[ch], preferred_element_type=F32)
            else:
                val = jnp.dot(at[ch, part, :], cg[b], preferred_element_type=F32)
            for a in arrived:
                val = val + a[part, :].astype(F32)
            dst[part, :] = val.astype(BF16)

    rs_send, rs_recv = (us, ds_), (ur, dr_)

    def rs_index(i, s):
        g, sign, _ = streams[i]
        return s - 1 if sign > 0 else (long, short)[g] + s - 1

    reducing = {}

    def reduce_step(ch, i, s):
        g, sign, k = streams[i]
        arrived = []
        if s > 1:
            reducing[ch, i, s - 1].wait_recv()
            arrived = [rs_recv[g].at[rs_index(i, s - 1), ch]]
        mine = rs_send[g].at[rs_index(i, s), ch]
        grad_block(ch, g, sign * (k - s + 1), mine, arrived)
        reducing[ch, i, s] = go(remote(
            mine, rs_recv[g].at[rs_index(i, s), ch],
            rs_ss.at[ch, i, s - 1], rs_rs.at[ch, i, s - 1], ring_dev(sign),
        ))

    def reduce_all(ch, s):
        for i, (g, sign, k) in enumerate(streams):
            if s <= k:
                reduce_step(ch, i, s)

    for ch in range(C):
        if ch + 1 < C:
            gather(ch, functools.partial(gather_first, ch + 1))
        elif C > 1:
            gather(ch, functools.partial(reduce_all, 0, 1))
        else:
            gather(ch, lambda: None)
            reduce_all(ch, 1)

    for q in range(n):
        b = member(q)

        @pl.loop(0, rows // row_tile)
        def _(i):
            part = pl.ds(pl.multiple_of(i * row_tile, row_tile), row_tile)
            val = 0.0
            for ch in range(C):
                block = own(0, ch) if q == 0 else ug.at[q - 1, ch]
                val = val + lax.dot_general(
                    pg[ch, part, :], block[...], NT, preferred_element_type=F32
                )
            igp[b, part, :] = val.astype(BF16)

    wide = R * tok
    it_copies = [
        go(remote(
            igp.at[:, pl.ds(dt * wide, wide), :], itr.at[dt - 1],
            it_ss.at[dt], it_rs.at[dt], tp_dev(dt),
        ))
        for dt in range(1, T)
    ]
    ir_copies = []

    def finish_tp():
        for copy in it_copies:
            copy.wait_recv()

        @pl.loop(0, n)
        def _(b):
            for dr in range(R):
                part = pl.ds(dr * tok, tok)
                val = igp[b, part, :].astype(F32)
                for dt in range(1, T):
                    val = val + itr[dt - 1, b, part, :].astype(F32)
                isum[dr, b] = val.astype(BF16)

        for dr in range(1, R):
            ir_copies.append(go(remote(
                isum.at[dr], irr.at[dr - 1], ir_ss.at[dr], ir_rs.at[dr], rep_dev(dr)
            )))

    def finish_rep():
        for copy in ir_copies:
            copy.wait_recv()

        for b in range(n):
            val = isum[0, b].astype(F32)
            for dr in range(1, R):
                val = val + irr[dr - 1, b].astype(F32)
            ig_ref[:, b * db:(b + 1) * db] = val.astype(BF16)

    finish_tp()

    finals = ((fu, fur, gu_ref), (fd, fdr, gd_ref))
    fin_copies = {}

    def put(g, place, ch, val):
        if g == 0:
            gu_ref[:, hidden(place, ch)] = val
        else:
            gd_ref[hidden(place, ch), :] = val

    def finish(ch, g):
        mine, theirs, out = finals[g]
        arrived = []
        for i, (h, sign, k) in enumerate(streams):
            if h == g and k >= 1:
                reducing[ch, i, k].wait_recv()
                arrived.append(rs_recv[g].at[rs_index(i, k), ch])
        grad_block(ch, g, 0, mine.at[ch], arrived)
        for dr in range(1, R):
            fin_copies[ch, g, dr] = go(remote(
                mine.at[ch], theirs.at[dr - 1, ch],
                f_ss.at[ch, g, dr], f_rs.at[ch, g, dr], rep_dev(-dr),
            ))
        put(g, r, ch, mine[ch])

    for ch in range(C):
        for s in range(2, hops + 1):
            reduce_all(ch, s)
            if ch == 0 and s == 2:
                finish_rep()
        if ch == 0 and hops < 2:
            finish_rep()
        if ch + 1 < C:
            reduce_all(ch + 1, 1)
        for g in range(2):
            finish(ch, g)
    for (ch, g, dr), copy in fin_copies.items():
        _, theirs, out = finals[g]
        copy.wait_recv()
        put(g, lax.rem(r + dr, R), ch, theirs[dr - 1, ch])
    for copy in sends:
        copy.wait_send()


def plane_kernel(
    Z,
    x_ref, c_ref, u_ref, d_ref,
    ig_ref, gu_ref, gd_ref,
    xg, cg, xt, ug, dg, pre, pg, at,
    igp, itr, isum, ira, irb, ipt, ift, su, sd, ru, rd, fu, fd,
    yw_s, yw_r, zg_s, zg_r, tx_s, tx_r, ty_s, ty_r, tt_s, tt_r,
    rs_s, rs_r, fy_s, fy_r, fx_s, fx_r, ig_s, ig_r,
):
    r, f, t = lax.axis_index("rep"), lax.axis_index("fs"), lax.axis_index("tp")
    z, y = lax.div(f, 2), lax.rem(f, 2)
    tok, D = x_ref.shape
    db = u_ref.shape[0]
    C, hc = pg.shape[0], pg.shape[2]
    hw, half, wide = C * hc, tok // 2, 2 * tok
    n = 2 * Z
    xdev, ydev, tdev = (1 - r, f, t), (r, f + 1 - 2 * y, t), (r, f, 1 - t)

    def zdev(s):
        return (r, f + 2 * s, t)

    low = z < Z // 2
    m = jnp.where(low, z, Z - 1 - z)
    near = (jnp.where(low, 0, 1), jnp.where(low, 1, -1))
    far = (1 - near[0], -near[1])

    barrier = pltpu.get_barrier_semaphore()

    def greet(dev):
        pl.semaphore_signal(barrier, inc=1, device_id=dev, device_id_type=MESH)

    for dev in (xdev, ydev, tdev):
        greet(dev)
    ahead = {1: z < Z - 1, -1: z > 0}
    for s in (1, -1):
        pl.when(ahead[s])(functools.partial(greet, zdev(s)))
    pl.semaphore_wait(barrier, 3 + sum(jnp.where(ahead[s], 1, 0) for s in (1, -1)))

    sends = []

    def remote(src, dst, ssem, rsem, dev):
        return pltpu.make_async_remote_copy(
            src_ref=src, dst_ref=dst, send_sem=ssem, recv_sem=rsem,
            device_id=dev, device_id_type=MESH,
        )

    def go(make, cond=None):
        make().start()
        sends.append((cond, make))

    def span(at_, size):
        return pl.ds(pl.multiple_of(at_, size), size)

    def blk(b):
        return span(b * db, db)

    def hid(q, ch):
        return span(q * hw + ch * hc, hc)

    mine, other = 2 * r + y, 2 * r + 1 - y

    def own(g, q, ch):
        return u_ref.at[:, hid(q, ch)] if g == 0 else d_ref.at[hid(q, ch), :]

    def held(g, ch, b):
        return ug.at[ch, blk(b), :] if g == 0 else dg.at[ch, :, blk(b)]

    def swap(ch, g):
        return remote(own(g, other, ch), held(g, ch, f), yw_s.at[ch, g], yw_r.at[ch, g], ydev)

    def origin(s, k, e):
        return f - 2 * s * k + e * (1 - 2 * y)

    def pass_on(ch, g, s, k, e):
        block = held(g, ch, origin(s, k, e))
        src = own(g, mine, ch) if k == 0 and e == 0 else block
        i = (ch, (1 - s) // 2, k, e, g)
        return remote(src, block, zg_s.at[i], zg_r.at[i], zdev(s))

    def landed(ch, g, s, k, e):
        block = held(g, ch, origin(s, k, e))
        i = (ch, (1 - s) // 2, k - 1, e, g)
        return remote(block, block, zg_s.at[i], zg_r.at[i], zdev(s))

    def begin(ch, g, e, also=None):
        for s in (1, -1):
            cond = ahead[s] if also is None else ahead[s] & also
            pl.when(cond)(functools.partial(
                go, functools.partial(pass_on, ch, g, s, 0, e), cond))

    level = [m == m0 for m0 in range(Z // 2)]
    reached = {}
    for k in range(1, Z):
        reached[1, k], reached[-1, k] = z >= k, z < Z - k
    passing = {key: reached[key] & ahead[key[0]] for key in reached}

    def relay(ch, g, k):
        for e in range(2):
            for s in (1, -1):
                cond = passing[s, k]

                @pl.when(cond)
                def _():
                    landed(ch, g, s, k, e).wait_recv()
                    go(functools.partial(pass_on, ch, g, s, k, e), cond)

    def collect(ch, g):
        for k in range(1, Z):
            for e in range(2):
                for s in (1, -1):

                    @pl.when(reached[s, k] & jnp.logical_not(ahead[s]))
                    def _():
                        landed(ch, g, s, k, e).wait_recv()

    def swapped(ch, g, also=None):
        begin(ch, g, 1, also)

    def rows(k, dt, part=(0, 2)):
        lo, hi = part
        return pl.ds((2 * k + dt) * tok + lo * half, (hi - lo) * half)

    def quarter(i):
        return span(jnp.where(low, Z - 1 - i, i) * 2 * db, 2 * db)

    A, B, AB = (0, 1), (1, 2), (0, 2)

    def hop(sems, i, dev, full, src, dst, cols, ref=None):
        def make():
            where = slice(None) if cols is None else quarter(cols)
            if ref is None:
                take = full.at[rows(*src), where]
            else:
                take = ref.at[pl.ds(src[2][0] * half, (src[2][1] - src[2][0]) * half), where]
            return remote(
                take, full.at[rows(*dst), where], sems[0].at[i], sems[1].at[i], dev
            )

        return make

    X, Y, S = (tx_s, tx_r), (ty_s, ty_r), (tt_s, tt_r)
    moves = {}
    for i, part in enumerate((A, B)):
        moves["x", "x", i] = hop(X, i, xdev, xg, (0, 0, part), (1, 0, part), None, x_ref)
        moves["y", "x", i] = hop(Y, i, ydev, xg, (0, 0, part), (2, 0, part), None, x_ref)
        moves["d", "x", i] = hop(X, 2 + i, xdev, xg, (2, 0, part), (3, 0, part), None)
    moves["s", "x", 0] = hop(S, 0, tdev, xg, (0, 0, AB), (0, 1, AB), None, x_ref)
    moves["s", "c", 0] = hop(S, 1, tdev, cg, (0, 0, AB), (0, 1, AB), None, c_ref)
    for k in range(1, 4):
        moves["s", "x", k] = hop(S, 1 + k, tdev, xg, (k, 0, AB), (k, 1, AB), None)
    for i in range(Z):
        moves["x", "c", i] = hop(X, 4 + 2 * i, xdev, cg, (0, 0, AB), (1, 0, AB), i, c_ref)
        moves["y", "c", i] = hop(Y, 2 + 2 * i, ydev, cg, (0, 0, AB), (2, 0, AB), i, c_ref)
        moves["dx", "c", i] = hop(X, 5 + 2 * i, xdev, cg, (2, 0, A), (3, 0, A), i)
        moves["dy", "c", i] = hop(Y, 3 + 2 * i, ydev, cg, (1, 0, B), (3, 0, B), i)
        for k in range(1, 4):
            moves["s%d" % k, "c", i] = hop(
                S, 5 + (k - 1) * Z + i, tdev, cg, (k, 0, AB), (k, 1, AB), i)

    def start(*key):
        go(moves[key])

    def arrive(*key):
        moves[key]().wait_recv()

    def flip(k):
        part = pl.ds(k * wide, wide)

        @pl.loop(0, n)
        def _(b):
            xt[blk(b), part] = xg[part, blk(b)].T

    def forward(ch, first, last):
        @pl.loop(first, last)
        def _(k):
            part = span(k * wide, wide)
            active = jnp.maximum(
                jnp.dot(xg[part, :], ug[ch], preferred_element_type=F32), 0.0)
            pre[ch, part, :] = active
            at[ch, :, part] = (active * active).astype(BF16).T

    def backward(ch):
        @pl.loop(0, 4)
        def _(k):
            part = span(k * wide, wide)
            val = lax.dot_general(cg[part, :], dg[ch], NT, preferred_element_type=F32)
            pg[ch, part, :] = (2.0 * pre[ch, part, :] * val).astype(BF16)

    def grad(ch, g, b):
        if g == 0:
            return jnp.dot(xt[blk(b), :], pg[ch], preferred_element_type=F32)
        return jnp.dot(at[ch], cg[:, blk(b)], preferred_element_type=F32)

    out_buf, in_buf, fin = (su, sd), (ru, rd), (fu, fd)

    def partial_copy(ch, g, way, j):
        d, s = way
        return remote(
            out_buf[g].at[d, j, ch], in_buf[g].at[d, j, ch],
            rs_s.at[d, j, ch, g], rs_r.at[d, j, ch, g], zdev(s))

    def reduce(ch, g, way, j, m0):
        cond = level[m0]
        to = jnp.where(way[1] > 0, Z - 1 - j, j)
        make = functools.partial(partial_copy, ch, g, way, j)
        more = m0 > 0 or way is far
        if more:
            make().wait_recv()

        @pl.loop(0, 2)
        def _(h):
            val = grad(ch, g, 2 * to + h)
            if more:
                val = val + in_buf[g][way[0], j, ch, h].astype(F32)
            out_buf[g][way[0], j, ch, h] = val.astype(BF16)

        go(make, cond)

    def place(g, q, ch):
        return gu_ref.at[:, hid(q, ch)] if g == 0 else gd_ref.at[hid(q, ch), :]

    def final_y(ch, g):
        return remote(
            fin[g].at[ch, 1 - y], place(g, mine, ch), fy_s.at[ch, g], fy_r.at[ch, g], ydev)

    def final_y_in(ch, g):
        return remote(
            place(g, other, ch), place(g, other, ch), fy_s.at[ch, g], fy_r.at[ch, g], ydev)

    def final_x(ch, g, e):
        src = fin[g].at[ch, y] if e == 0 else place(g, other, ch)
        q = other if e else mine
        i = (ch, g, e)
        return remote(src, place(g, q, ch), fx_s.at[i], fx_r.at[i], xdev)

    def final_x_in(ch, g, e):
        q = 2 * (1 - r) + (1 - y if e else y)
        i = (ch, g, e)
        return remote(place(g, q, ch), place(g, q, ch), fx_s.at[i], fx_r.at[i], xdev)

    def finish(ch, g, m0):
        cond = level[m0]
        ways = [(far, m0)] + ([(near, Z - 1 - m0)] if m0 else [])
        for way, j in ways:
            partial_copy(ch, g, way, j).wait_recv()

        @pl.loop(0, 2)
        def _(h):
            val = grad(ch, g, 2 * z + h)
            for way, j in ways:
                val = val + in_buf[g][way[0], j, ch, h].astype(F32)
            fin[g][ch, h] = val.astype(BF16)

        go(functools.partial(final_y, ch, g), cond)
        go(functools.partial(final_x, ch, g, 0), cond)
        if g == 0:
            gu_ref[:, hid(mine, ch)] = fu[ch, y]
        else:
            gd_ref[hid(mine, ch), :] = fd[ch, y]

    def spread(ch, g, m0):
        final_y_in(ch, g).wait_recv()
        go(functools.partial(final_x, ch, g, 1), level[m0])

    hd = D // 2

    def ig_copy(i):
        if i == 0:
            return remote(igp.at[:, pl.ds(tok, tok), :], itr, ig_s.at[0], ig_r.at[0], tdev)
        side, step = (i - 1) % 2, (i - 1) // 2
        if step < 2:
            src = isum.at[side, 3 if step else 1 + side]
            dst = (ira, irb)[side].at[step]
        else:
            src, dst = ipt.at[side], ift.at[side]
        dev = (xdev, ydev)[side if step < 2 else 1 - side]
        return remote(src, dst, ig_s.at[i], ig_r.at[i], dev)

    def ig_go(i, cond):
        go(functools.partial(ig_copy, i), cond)

    def ig_partial(cond):
        @pl.loop(0, 4)
        def _(k):
            part = span(k * wide, wide)

            @pl.loop(0, n)
            def _(b):
                val = 0.0
                for ch in range(C):
                    val = val + lax.dot_general(
                        pg[ch, part, :], ug[ch, blk(b), :], NT, preferred_element_type=F32)
                igp[k, :, blk(b)] = val.astype(BF16)

        ig_go(0, cond)

    def ig_first(cond):
        ig_copy(0).wait_recv()

        @pl.loop(0, 4)
        def _(k):
            for side in range(2):
                cols = pl.ds(side * hd, hd)
                val = igp[k, 0:tok, cols].astype(F32) + itr[k, :, cols].astype(F32)
                isum[side, k] = val.astype(BF16)

        for i in range(1, 5):
            ig_go(i, cond)

    def ig_second(cond):
        for i in range(1, 5):
            ig_copy(i).wait_recv()
        for side, got in enumerate((ira, irb)):
            val = isum[side, 2 - side].astype(F32) + got[1].astype(F32)
            ipt[side] = val.astype(BF16)
            ig_go(5 + side, cond)

    def ig_last():
        for side, got in enumerate((ira, irb)):
            ig_copy(5 + side).wait_recv()
            val = isum[side, 0].astype(F32) + got[0].astype(F32) + ift[side].astype(F32)
            ig_ref[:, side * hd:(side + 1) * hd] = val.astype(BF16)

    edge, inner = level[0], m > 0
    last = C - 1

    begin(0, 0, 0)
    go(functools.partial(swap, 0, 0))
    for i in range(2):
        start("x", "x", i)
        start("y", "x", i)
    begin(0, 1, 0, edge)
    start("s", "x", 0)
    start("s", "c", 0)
    for ch in range(C):
        for g in range(2):
            if ch or g:
                go(functools.partial(swap, ch, g))
    xg[0:tok, :] = x_ref[...]
    cg[0:tok, :] = c_ref[...]
    for ch in range(C):
        ug[ch, blk(f), :] = u_ref[:, hid(mine, ch)]
        dg[ch, :, blk(f)] = d_ref[hid(mine, ch), :]

    swap(0, 0).wait_recv()
    begin(0, 0, 1)
    for ch in range(1, C):
        for g in range(2):
            begin(ch, g, 0, edge)
    relay(0, 0, 1)
    arrive("s", "x", 0)
    arrive("s", "c", 0)
    flip(0)
    arrive("y", "x", 0)
    start("d", "x", 0)
    for k in range(2, Z - 1):
        relay(0, 0, k)
    begin(0, 1, 0, inner)
    for i in range(2):
        arrive("x", "x", i)
    start("s", "x", 1)
    arrive("y", "x", 1)
    start("d", "x", 1)
    start("x", "c", 0)
    start("y", "c", 0)
    start("s", "x", 2)
    swap(0, 1).wait_recv()
    begin(0, 1, 1)
    arrive("s", "x", 1)
    flip(1)
    arrive("s", "x", 2)
    flip(2)
    relay(0, 1, 1)
    collect(0, 0)
    forward(0, 0, 3)
    for ch in range(1, C):
        for g in range(2):
            swap(ch, g).wait_recv()
            begin(ch, g, 1, edge)
    for i in range(2):
        arrive("d", "x", i)
    start("s", "x", 3)
    for k in range(2, Z - 1):
        relay(0, 1, k)
    for ch in range(1, C):
        begin(ch, 0, 0, inner)
        begin(ch, 0, 1, inner)
    arrive("s", "x", 3)
    flip(3)
    forward(0, 3, 4)
    for i in range(Z):
        if i + 1 < Z:
            start("x", "c", i + 1)
            start("y", "c", i + 1)
        arrive("x", "c", i)
        start("dy", "c", i)
        start("s1", "c", i)
        arrive("y", "c", i)
        start("dx", "c", i)
        start("s2", "c", i)
        if 1 <= i < Z - 1:
            for ch in range(1, C):
                relay(ch, 0, i)
                if i == Z - 2:
                    begin(ch, 1, 0, inner)
                    begin(ch, 1, 1, inner)
        arrive("dy", "c", i)
        arrive("dx", "c", i)
        start("s3", "c", i)
        for k in range(1, 4):
            arrive("s%d" % k, "c", i)
        if i < Z - 1:
            pl.when(edge)(functools.partial(reduce, 0, 1, near, i, 0))
    collect(0, 1)
    backward(0)

    def edges():
        for j in range(Z - 1):
            reduce(0, 0, near, j, 0)
        for ch in range(1, C):
            collect(ch, 0)
            forward(ch, 0, 4)
            for j in range(Z - 1):
                reduce(ch, 1, near, j, 0)
            collect(ch, 1)
            backward(ch)
            for j in range(Z - 1):
                reduce(ch, 0, near, j, 0)
        ig_partial(edge)
        finish(0, 1, 0)
        ig_first(edge)
        spread(0, 1, 0)
        finish(0, 0, 0)
        ig_second(edge)
        spread(0, 0, 0)
        for ch in range(1, C):
            finish(ch, 1, 0)
            if ch == 1:
                ig_last()
            spread(ch, 1, 0)
            finish(ch, 0, 0)
            spread(ch, 0, 0)

    def inside(m0):
        cond = level[m0]

        def some(ch, g):
            for j in range(Z - 1 - m0):
                reduce(ch, g, near, j, m0)
                if j < m0:
                    reduce(ch, g, far, j, m0)

        for j in range(Z - 1 - m0):
            reduce(0, 1, near, j, m0)
            if j + 1 < Z - 1:
                for ch in range(1, C):
                    relay(ch, 1, j + 1)
        for ch in range(1, C):
            for k in range(Z - m0, Z - 1):
                relay(ch, 1, k)
        for j in range(m0):
            reduce(0, 1, far, j, m0)
        for ch in range(1, C):
            forward(ch, 0, 4)
            backward(ch)
        ig_partial(cond)
        reduce(0, 0, near, 0, m0)
        ig_first(cond)
        finish(0, 1, m0)
        for j in range(1, Z - 1 - m0):
            reduce(0, 0, near, j, m0)
        spread(0, 1, m0)
        for j in range(m0):
            reduce(0, 0, far, j, m0)
        ig_second(cond)
        finish(0, 0, m0)
        for ch in range(1, C):
            reduce(ch, 1, near, 0, m0)
            if ch == 1:
                spread(0, 0, m0)
                ig_last()
            for j in range(1, Z - 1 - m0):
                reduce(ch, 1, near, j, m0)
            for j in range(m0):
                reduce(ch, 1, far, j, m0)
            finish(ch, 1, m0)
            reduce(ch, 0, near, 0, m0)
            spread(ch, 1, m0)
            for j in range(1, Z - 1 - m0):
                reduce(ch, 0, near, j, m0)
            for j in range(m0):
                reduce(ch, 0, far, j, m0)
            finish(ch, 0, m0)
            spread(ch, 0, m0)

    pl.when(edge)(edges)
    for m0 in range(1, Z // 2):
        pl.when(level[m0])(functools.partial(inside, m0))
    for ch in range(C):
        for g in (1, 0):
            for e in range(2):
                final_x_in(ch, g, e).wait_recv()
    for cond, make in sends:
        if cond is None:
            make().wait_send()
        else:
            pl.when(cond)(lambda: make().wait_send())


def ring_call(inputs, up_weight):
    R, n, T = axis_sizes()
    tok, D = inputs.shape
    db, hb = up_weight.shape[0], up_weight.shape[1] // R
    rows = R * T * tok
    C = tile_of(hb // 128, CHUNKS) if hb > 128 else 1
    w = hb // C
    V, S = pltpu.VMEM, pltpu.SemaphoreType.DMA
    hops = max(n // 2, 1)
    m = max(n - 1, 1)
    scratch = [
        V((n, rows, db), BF16), V((n, rows, db), BF16), V((n, db, rows), BF16),
        V((m, C, db, w), BF16), V((m, C, w, db), BF16),
        V((C, rows, w), F32), V((C, rows, w), F32), V((C, rows, w), BF16), V((C, w, rows), BF16),
        V((n, rows, db), BF16), V((max(T - 1, 1), n, R * tok, db), BF16),
        V((R, n, tok, db), BF16), V((max(R - 1, 1), n, tok, db), BF16),
        V((m, C, db, w), BF16), V((m, C, db, w), BF16),
        V((m, C, w, db), BF16), V((m, C, w, db), BF16),
        V((C, db, w), BF16), V((C, w, db), BF16),
        V((max(R - 1, 1), C, db, w), BF16), V((max(R - 1, 1), C, w, db), BF16),
        S((C, 4, hops)), S((C, 4, hops)), S((C, 4, hops)), S((C, 4, hops)),
        S((2, R)), S((2, R)), S((2, T, R)), S((2, T, R)),
        S((T,)), S((T,)), S((R,)), S((R,)), S((C, 2, R)), S((C, 2, R)),
    ]
    return functools.partial(ring_kernel, R, n, T), scratch, (R, hb)


def axis_sizes():
    return lax.axis_size("rep"), lax.axis_size("fs"), lax.axis_size("tp")


def plane_call(inputs, up_weight):
    R, n, T = axis_sizes()
    tok, D = inputs.shape
    db, HB = up_weight.shape
    Z, G = n // 2, 2 * R
    if R != 2 or T != 2 or n % 4 or tok % 32 or HB % (128 * G) or db % 128:
        return None
    hw = HB // G
    C = tile_of(hw // 128, CHUNKS)
    hc = hw // C
    rows, hd = 8 * tok, D // 2
    V, S = pltpu.VMEM, pltpu.SemaphoreType.DMA
    data = [
        ((rows, D), BF16), ((rows, D), BF16), ((D, rows), BF16),
        ((C, D, hc), BF16), ((C, hc, D), BF16),
        ((C, rows, hc), F32), ((C, rows, hc), BF16), ((C, hc, rows), BF16),
        ((4, 2 * tok, D), BF16), ((4, tok, D), BF16), ((2, 4, tok, hd), BF16),
        ((2, tok, hd), BF16), ((2, tok, hd), BF16), ((2, tok, hd), BF16), ((2, tok, hd), BF16),
        ((2, Z - 1, C, 2, db, hc), BF16), ((2, Z - 1, C, 2, hc, db), BF16),
        ((2, Z - 1, C, 2, db, hc), BF16), ((2, Z - 1, C, 2, hc, db), BF16),
        ((C, 2, db, hc), BF16), ((C, 2, hc, db), BF16),
    ]
    size = sum(math.prod(s) * jnp.dtype(d).itemsize for s, d in data)
    if size > 50 * 2**20:
        return None
    sems = [
        (C, 2), (C, 2, Z - 1, 2, 2), (4 + 2 * Z,), (2 + 2 * Z,), (5 + 3 * Z,),
        (2, Z - 1, C, 2), (C, 2), (C, 2, 2), (7,),
    ]
    scratch = [V(s, d) for s, d in data] + [S(s) for s in sems for _ in range(2)]
    return functools.partial(plane_kernel, Z), scratch, (1, HB)


def shards(inputs, cotangent, up_weight, down_weight):
    R, n, T = axis_sizes()
    tok, D = inputs.shape
    db = up_weight.shape[0]
    body, scratch, (parts, hb) = plane_call(inputs, up_weight) or ring_call(inputs, up_weight)
    vmem = pl.BlockSpec(memory_space=pltpu.VMEM)
    ig, gu, gd = pl.pallas_call(
        body,
        out_shape=(
            jax.ShapeDtypeStruct((tok, D), BF16),
            jax.ShapeDtypeStruct((db, parts * hb), BF16),
            jax.ShapeDtypeStruct((parts * hb, db), BF16),
        ),
        in_specs=[vmem] * 4,
        out_specs=(vmem,) * 3,
        scratch_shapes=scratch,
        compiler_params=pltpu.CompilerParams(
            collective_id=0, has_side_effects=True, vmem_limit_bytes=60 * 2**20
        ),
    )(inputs, cotangent, up_weight, down_weight)
    total_tokens = tok * R * n * T
    loss_scale = 1.0 / math.sqrt(total_tokens)
    return ig, gu.astype(F32) * loss_scale, gd.astype(F32) * loss_scale


def solution(mesh):
    token, up, down = P(("rep", "fs", "tp"), None), P("fs", "tp"), P("tp", "fs")
    return jax.shard_map(
        shards,
        mesh=mesh,
        in_specs=(token, token, up, down),
        out_specs=(token, up, down),
        check_vma=False,
    )
```

```python
import functools
import math

import jax
import jax.numpy as jnp
from jax import lax
from jax.experimental import pallas as pl
from jax.experimental.pallas import tpu as pltpu
from jax.sharding import PartitionSpec as P

MESH = pl.DeviceIdType.MESH
CHUNKS = 2
BF16, F32 = jnp.bfloat16, jnp.float32
NT = (((1,), (1,)), ((), ()))


def ring_place(f, n):
    odd = lax.rem(f, 2)
    half = lax.div(f, 2)
    return half * (1 - odd) + (n - 1 - half) * odd


def ring_member(p, n):
    back = lax.div(p, (n + 1) // 2)
    return 2 * p * (1 - back) + (2 * n - 1 - 2 * p) * back


def tile_of(size, most):
    while size % most:
        most //= 2
    return most


def ring_kernel(
    R, n, T,
    x_ref, c_ref, u_ref, d_ref,
    ig_ref, gu_ref, gd_ref,
    xg, cg, xt, ug, dg, pre, agr, pg, at,
    igp, itr, isum, irr, us, ur, ds_, dr_, fu, fd, fur, fdr,
    ag_ss, ag_rs, rs_ss, rs_rs, tr_ss, tr_rs, tt_ss, tt_rs,
    it_ss, it_rs, ir_ss, ir_rs, f_ss, f_rs,
):
    r, f, t = lax.axis_index("rep"), lax.axis_index("fs"), lax.axis_index("tp")
    tok, db = x_ref.shape[0], u_ref.shape[0]
    C, w = pre.shape[0], pre.shape[2]
    hb = C * w
    rows = R * T * tok

    def hidden(place, ch):
        return pl.ds(pl.multiple_of(place * hb + ch * w, w), w)

    for ref, full in ((x_ref, xg), (c_ref, cg)):
        for q in range(n):
            full[q, 0:tok, :] = ref[:, q * db:(q + 1) * db]
    p = ring_place(f, n)

    def member(q):
        return ring_member(lax.rem(p + q + n, n), n)

    def ring_dev(sign):
        return (r, member(sign), t)

    def rep_dev(q):
        return (lax.rem(r + q + R, R), f, t)

    def tp_dev(q):
        return (r, f, lax.rem(t + q + T, T))

    barrier = pltpu.get_barrier_semaphore()
    peers = [ring_dev(1), ring_dev(-1)]
    peers += [rep_dev(q) for q in range(1, R)] + [tp_dev(q) for q in range(1, T)]
    for peer in peers:
        pl.semaphore_signal(barrier, inc=1, device_id=peer, device_id_type=MESH)
    pl.semaphore_wait(barrier, len(peers))

    def remote(src, dst, ssem, rsem, dev):
        return pltpu.make_async_remote_copy(
            src_ref=src, dst_ref=dst, send_sem=ssem, recv_sem=rsem,
            device_id=dev, device_id_type=MESH,
        )

    long, short = n // 2, (n - 1) // 2
    streams = [(0, 1, long), (0, -1, short), (1, 1, short), (1, -1, long)]
    hops = max(long, short)
    def own(g, ch):
        return u_ref.at[:, hidden(r, ch)] if g == 0 else d_ref.at[hidden(r, ch), :]

    held = (ug, dg)

    def slot(sign, s):
        return (n - s if sign > 0 else s) - 1

    def gather_copy(ch, i, s):
        g, sign, _ = streams[i]
        src = own(g, ch) if s == 1 else held[g].at[slot(sign, s - 1), ch]
        return remote(
            src, held[g].at[slot(sign, s), ch],
            ag_ss.at[ch, i, s - 1], ag_rs.at[ch, i, s - 1], ring_dev(sign),
        )

    sends = []

    def go(copy):
        copy.start()
        sends.append(copy)
        return copy

    flying = {}

    def gather_first(ch):
        for i, (g, sign, k) in enumerate(streams):
            if k >= 1:
                flying[ch, i, 1] = go(gather_copy(ch, i, 1))

    gather_first(0)

    tokens = tuple((full.at[:, 0:tok, :], full) for full in (xg, cg))

    def span(dt, dr):
        return pl.ds((dt * R + dr) * tok, tok)

    rep_copies = {}
    for dr in range(1, R):
        for j, (ref, full) in enumerate(tokens):
            rep_copies[j, dr] = go(remote(
                ref, full.at[:, span(0, dr), :], tr_ss.at[j, dr], tr_rs.at[j, dr], rep_dev(-dr)
            ))
    tp_copies = {}
    for dt in range(1, T):
        for j, (ref, full) in enumerate(tokens):
            tp_copies[j, dt, 0] = go(remote(
                ref, full.at[:, span(dt, 0), :], tt_ss.at[j, dt, 0], tt_rs.at[j, dt, 0],
                tp_dev(-dt),
            ))

    row_tile = tile_of(rows, 256)

    def gather_dot(ch, g, block, q, first=False):
        b = member(q)
        out, full = ((pre, xg), (agr, cg))[g]

        @pl.loop(0, rows // row_tile)
        def _(i):
            part = pl.ds(pl.multiple_of(i * row_tile, row_tile), row_tile)
            lhs = full[b, part, :]
            if g == 0:
                val = jnp.dot(lhs, block[...], preferred_element_type=F32)
            else:
                val = lax.dot_general(lhs, block[...], NT, preferred_element_type=F32)
            if first:
                out[ch, part, :] = val
            else:
                out[ch, part, :] += val

    def finish_tokens():
        for dr in range(1, R):
            for j, (ref, full) in enumerate(tokens):
                rep_copies[j, dr].wait_recv()
                for dt in range(1, T):
                    tp_copies[j, dt, dr] = go(remote(
                        full.at[:, span(0, dr), :], full.at[:, span(dt, dr), :],
                        tt_ss.at[j, dt, dr], tt_rs.at[j, dt, dr], tp_dev(-dt),
                    ))
        for copy in tp_copies.values():
            copy.wait_recv()

        @pl.loop(0, n)
        def _(b):
            xt[b] = xg[b].T

        for ch in range(C):
            gather_dot(ch, 0, own(0, ch), 0, True)
            gather_dot(ch, 1, own(1, ch), 0, True)

    act_tile = tile_of(rows, 128)

    def activate(ch):
        @pl.loop(0, rows // act_tile)
        def _(i):
            part = pl.ds(pl.multiple_of(i * act_tile, act_tile), act_tile)
            active = jnp.maximum(pre[ch, part, :], 0.0)
            pg[ch, part, :] = (2.0 * active * agr[ch, part, :]).astype(BF16)
            at[ch, :, part] = (active * active).astype(BF16).T

    def gather(ch, before_last):
        for s in range(1, hops + 1):
            if s == hops:
                before_last()
            for i, (g, sign, k) in enumerate(streams):
                if s <= k:
                    flying[ch, i, s].wait_recv()
                    if s < k:
                        flying[ch, i, s + 1] = go(gather_copy(ch, i, s + 1))
            if s == 1 and ch == 0:
                finish_tokens()
            for i, (g, sign, k) in enumerate(streams):
                if s <= k:
                    gather_dot(ch, g, held[g].at[slot(sign, s), ch], -sign * s)
        if hops == 0:
            if ch == 0:
                finish_tokens()
            before_last()
        activate(ch)

    def grad_block(ch, g, q, dst, arrived):
        b = member(q)
        height = (db, w)[g]
        tile = tile_of(height, 256)

        @pl.loop(0, height // tile)
        def _(i):
            part = pl.ds(pl.multiple_of(i * tile, tile), tile)
            if g == 0:
                val = jnp.dot(xt[b, part, :], pg[ch], preferred_element_type=F32)
            else:
                val = jnp.dot(at[ch, part, :], cg[b], preferred_element_type=F32)
            for a in arrived:
                val = val + a[part, :].astype(F32)
            dst[part, :] = val.astype(BF16)

    rs_send, rs_recv = (us, ds_), (ur, dr_)

    def rs_index(i, s):
        g, sign, _ = streams[i]
        return s - 1 if sign > 0 else (long, short)[g] + s - 1

    reducing = {}

    def reduce_step(ch, i, s):
        g, sign, k = streams[i]
        arrived = []
        if s > 1:
            reducing[ch, i, s - 1].wait_recv()
            arrived = [rs_recv[g].at[rs_index(i, s - 1), ch]]
        mine = rs_send[g].at[rs_index(i, s), ch]
        grad_block(ch, g, sign * (k - s + 1), mine, arrived)
        reducing[ch, i, s] = go(remote(
            mine, rs_recv[g].at[rs_index(i, s), ch],
            rs_ss.at[ch, i, s - 1], rs_rs.at[ch, i, s - 1], ring_dev(sign),
        ))

    def reduce_all(ch, s):
        for i, (g, sign, k) in enumerate(streams):
            if s <= k:
                reduce_step(ch, i, s)

    for ch in range(C):
        if ch + 1 < C:
            gather(ch, functools.partial(gather_first, ch + 1))
        elif C > 1:
            gather(ch, functools.partial(reduce_all, 0, 1))
        else:
            gather(ch, lambda: None)
            reduce_all(ch, 1)

    for q in range(n):
        b = member(q)

        @pl.loop(0, rows // row_tile)
        def _(i):
            part = pl.ds(pl.multiple_of(i * row_tile, row_tile), row_tile)
            val = 0.0
            for ch in range(C):
                block = own(0, ch) if q == 0 else ug.at[q - 1, ch]
                val = val + lax.dot_general(
                    pg[ch, part, :], block[...], NT, preferred_element_type=F32
                )
            igp[b, part, :] = val.astype(BF16)

    wide = R * tok
    it_copies = [
        go(remote(
            igp.at[:, pl.ds(dt * wide, wide), :], itr.at[dt - 1],
            it_ss.at[dt], it_rs.at[dt], tp_dev(dt),
        ))
        for dt in range(1, T)
    ]
    ir_copies = []

    def finish_tp():
        for copy in it_copies:
            copy.wait_recv()

        @pl.loop(0, n)
        def _(b):
            for dr in range(R):
                part = pl.ds(dr * tok, tok)
                val = igp[b, part, :].astype(F32)
                for dt in range(1, T):
                    val = val + itr[dt - 1, b, part, :].astype(F32)
                isum[dr, b] = val.astype(BF16)

        for dr in range(1, R):
            ir_copies.append(go(remote(
                isum.at[dr], irr.at[dr - 1], ir_ss.at[dr], ir_rs.at[dr], rep_dev(dr)
            )))

    def finish_rep():
        for copy in ir_copies:
            copy.wait_recv()

        for b in range(n):
            val = isum[0, b].astype(F32)
            for dr in range(1, R):
                val = val + irr[dr - 1, b].astype(F32)
            ig_ref[:, b * db:(b + 1) * db] = val.astype(BF16)

    finish_tp()

    finals = ((fu, fur, gu_ref), (fd, fdr, gd_ref))
    fin_copies = {}

    def put(g, place, ch, val):
        if g == 0:
            gu_ref[:, hidden(place, ch)] = val
        else:
            gd_ref[hidden(place, ch), :] = val

    def finish(ch, g):
        mine, theirs, out = finals[g]
        arrived = []
        for i, (h, sign, k) in enumerate(streams):
            if h == g and k >= 1:
                reducing[ch, i, k].wait_recv()
                arrived.append(rs_recv[g].at[rs_index(i, k), ch])
        grad_block(ch, g, 0, mine.at[ch], arrived)
        for dr in range(1, R):
            fin_copies[ch, g, dr] = go(remote(
                mine.at[ch], theirs.at[dr - 1, ch],
                f_ss.at[ch, g, dr], f_rs.at[ch, g, dr], rep_dev(-dr),
            ))
        put(g, r, ch, mine[ch])

    for ch in range(C):
        for s in range(2, hops + 1):
            reduce_all(ch, s)
            if ch == 0 and s == 2:
                finish_rep()
        if ch == 0 and hops < 2:
            finish_rep()
        if ch + 1 < C:
            reduce_all(ch + 1, 1)
        for g in range(2):
            finish(ch, g)
    for (ch, g, dr), copy in fin_copies.items():
        _, theirs, out = finals[g]
        copy.wait_recv()
        put(g, lax.rem(r + dr, R), ch, theirs[dr - 1, ch])
    for copy in sends:
        copy.wait_send()


def plane_kernel(
    Z,
    x_ref, c_ref, u_ref, d_ref,
    ig_ref, gu_ref, gd_ref,
    xg, cg, xt, ug, dg, pre, pg, at,
    igp, itr, isum0, isum1, ira, irb, ipt0, ipt1, ift0, ift1, igo, su, sd, ru, rd, fu, fd, uo, do, yu, yd,
    yw_s, yw_r, zg_s, zg_r, tx_s, tx_r, ty_s, ty_r, tt_s, tt_r,
    rs_s, rs_r, fy_s, fy_r, fx_s, fx_r, ig_s, ig_r, ld_s, st_s,
):
    r, f, t = lax.axis_index("rep"), lax.axis_index("fs"), lax.axis_index("tp")
    z, y = lax.div(f, 2), lax.rem(f, 2)
    tok, D = x_ref.shape
    db = u_ref.shape[0]
    C, hc = pg.shape[0], pg.shape[2]
    hw, half, wide = C * hc, tok // 2, 2 * tok
    n = 2 * Z
    xdev, ydev, tdev = (1 - r, f, t), (r, f + 1 - 2 * y, t), (r, f, 1 - t)

    def zdev(s):
        return (r, f + 2 * s, t)

    low = z < Z // 2
    m = jnp.where(low, z, Z - 1 - z)
    near = (jnp.where(low, 0, 1), jnp.where(low, 1, -1))
    far = (1 - near[0], -near[1])

    ahead = {1: z < Z - 1, -1: z > 0}
    sends = []

    def remote(src, dst, ssem, rsem, dev):
        return pltpu.make_async_remote_copy(
            src_ref=src, dst_ref=dst, send_sem=ssem, recv_sem=rsem,
            device_id=dev, device_id_type=MESH,
        )

    def go(make, cond=None):
        make().start()
        sends.append((cond, make))

    def span(at_, size):
        return pl.ds(pl.multiple_of(at_, size), size)

    def blk(b):
        return span(b * db, db)

    def hid(q, ch):
        return span(q * hw + ch * hc, hc)

    mine, other = 2 * r + y, 2 * r + 1 - y

    def held(g, ch, b):
        return ug.at[ch, blk(b), :] if g == 0 else dg.at[ch, :, blk(b)]

    spare = (uo, do)
    weights = (u_ref, d_ref)

    def strip(g, ref, q, ch):
        return ref.at[:, hid(q, ch)] if g == 0 else ref.at[hid(q, ch), :]

    own_x, own_c = xg.at[pl.ds(0, tok), :], cg.at[pl.ds(0, tok), :]
    loads = {}
    for ch in range(C):
        for g in range(2):
            loads["other", ch, g] = (strip(g, weights[g], other, ch), spare[g].at[ch])
            loads["mine", ch, g] = (strip(g, weights[g], mine, ch), held(g, ch, f))
        if ch == 0:
            loads["x"] = (x_ref, own_x)
            loads["c"] = (c_ref, own_c)
    loads = {
        key: pltpu.make_async_copy(src, dst, ld_s.at[i])
        for i, (key, (src, dst)) in enumerate(loads.items())
    }
    for copy in loads.values():
        copy.start()

    barrier = pltpu.get_barrier_semaphore()

    def greet(dev):
        pl.semaphore_signal(barrier, inc=1, device_id=dev, device_id_type=MESH)

    for dev in (xdev, ydev, tdev):
        greet(dev)
    for s in (1, -1):
        pl.when(ahead[s])(functools.partial(greet, zdev(s)))
    pl.semaphore_wait(barrier, 3 + sum(jnp.where(ahead[s], 1, 0) for s in (1, -1)))

    def swap(ch, g):
        return remote(spare[g].at[ch], held(g, ch, f), yw_s.at[ch, g], yw_r.at[ch, g], ydev)

    def origin(s, k, e):
        return f - 2 * s * k + e * (1 - 2 * y)

    def pass_on(ch, g, s, k, e):
        block = held(g, ch, origin(s, k, e))
        i = (ch, (1 - s) // 2, k, e, g)
        return remote(block, block, zg_s.at[i], zg_r.at[i], zdev(s))

    def landed(ch, g, s, k, e):
        block = held(g, ch, origin(s, k, e))
        i = (ch, (1 - s) // 2, k - 1, e, g)
        return remote(block, block, zg_s.at[i], zg_r.at[i], zdev(s))

    def begin(ch, g, e, also=None):
        for s in (1, -1):
            cond = ahead[s] if also is None else ahead[s] & also
            pl.when(cond)(functools.partial(
                go, functools.partial(pass_on, ch, g, s, 0, e), cond))

    level = [m == m0 for m0 in range(Z // 2)]
    reached = {}
    for k in range(1, Z):
        reached[1, k], reached[-1, k] = z >= k, z < Z - k
    passing = {key: reached[key] & ahead[key[0]] for key in reached}

    outward = {1: low, -1: jnp.logical_not(low)}
    split = {}
    for (s, k), cond in passing.items():
        split[s, k, 0] = cond & outward[s]
        split[s, k, 1] = cond & outward[-s]

    def relay(ch, g, k, es=(0, 1), toward=None):
        for e in es:
            for s in (1, -1):
                cond = passing[s, k] if toward is None else split[s, k, toward]

                @pl.when(cond)
                def _():
                    landed(ch, g, s, k, e).wait_recv()
                    go(functools.partial(pass_on, ch, g, s, k, e), cond)

    def collect(ch, g):
        for k in range(1, Z):
            for e in range(2):
                for s in (1, -1):

                    @pl.when(reached[s, k] & jnp.logical_not(ahead[s]))
                    def _():
                        landed(ch, g, s, k, e).wait_recv()

    def swapped(ch, g, also=None):
        begin(ch, g, 1, also)

    def rows(k, dt, part=(0, 2)):
        lo, hi = part
        return pl.ds((2 * k + dt) * tok + lo * half, (hi - lo) * half)

    def quarter(i):
        return span(jnp.where(low, Z - 1 - i, i) * 2 * db, 2 * db)

    A, B, AB = (0, 1), (1, 2), (0, 2)

    def hop(sems, i, dev, full, src, dst, cols):
        def make():
            where = slice(None) if cols is None else quarter(cols)
            return remote(
                full.at[rows(*src), where], full.at[rows(*dst), where],
                sems[0].at[i], sems[1].at[i], dev,
            )

        return make

    X, Y, S = (tx_s, tx_r), (ty_s, ty_r), (tt_s, tt_r)
    moves = {}
    for i, part in enumerate((A, B)):
        moves["x", "x", i] = hop(X, i, xdev, xg, (0, 0, part), (1, 0, part), None)
        moves["y", "x", i] = hop(Y, i, ydev, xg, (0, 0, part), (2, 0, part), None)
        moves["d", "x", i] = hop(X, 2 + i, xdev, xg, (2, 0, part), (3, 0, part), None)
    moves["s", "x", 0] = hop(S, 0, tdev, xg, (0, 0, AB), (0, 1, AB), None)
    moves["s", "c", 0] = hop(S, 1, tdev, cg, (0, 0, AB), (0, 1, AB), None)
    for k in range(1, 4):
        moves["s", "x", k] = hop(S, 1 + k, tdev, xg, (k, 0, AB), (k, 1, AB), None)
    for i in range(Z):
        moves["x", "c", i] = hop(X, 4 + 2 * i, xdev, cg, (0, 0, AB), (1, 0, AB), i)
        moves["y", "c", i] = hop(Y, 2 + 2 * i, ydev, cg, (0, 0, AB), (2, 0, AB), i)
        moves["dx", "c", i] = hop(X, 5 + 2 * i, xdev, cg, (2, 0, A), (3, 0, A), i)
        moves["dy", "c", i] = hop(Y, 3 + 2 * i, ydev, cg, (1, 0, B), (3, 0, B), i)
        for k in range(1, 4):
            moves["s%d" % k, "c", i] = hop(
                S, 5 + (k - 1) * Z + i, tdev, cg, (k, 0, AB), (k, 1, AB), i)

    def start(*key):
        go(moves[key])

    def arrive(*key):
        moves[key]().wait_recv()

    def flip(k):
        part = pl.ds(k * wide, wide)

        @pl.loop(0, n)
        def _(b):
            xt[blk(b), part] = xg[part, blk(b)].T

    def forward(ch, first, last):
        @pl.loop(first, last)
        def _(k):
            part = span(k * wide, wide)
            active = jnp.maximum(
                jnp.dot(xg[part, :], ug[ch], preferred_element_type=F32), 0.0)
            pre[ch, part, :] = active
            at[ch, :, part] = (active * active).astype(BF16).T

    def backward(ch):
        @pl.loop(0, 4)
        def _(k):
            part = span(k * wide, wide)
            val = lax.dot_general(cg[part, :], dg[ch], NT, preferred_element_type=F32)
            pg[ch, part, :] = (2.0 * pre[ch, part, :] * val).astype(BF16)

    def grad(ch, g, b):
        if g == 0:
            return jnp.dot(xt[blk(b), :], pg[ch], preferred_element_type=F32)
        return jnp.dot(at[ch], cg[:, blk(b)], preferred_element_type=F32)

    out_buf, in_buf, fin = (su, sd), (ru, rd), (fu, fd)

    def partial_copy(ch, g, way, j, e):
        d, s = way
        return remote(
            out_buf[g].at[d, j, ch, e], in_buf[g].at[d, j, ch, e],
            rs_s.at[d, j, ch, g, e], rs_r.at[d, j, ch, g, e], zdev(s))

    def side_of(e):
        return e * y + (1 - e) * (1 - y)

    def reduce(ch, g, way, j, m0):
        cond = level[m0]
        to = jnp.where(way[1] > 0, Z - 1 - j, j)
        more = m0 > 0 or way is far

        @pl.loop(0, 2)
        def _(e):
            val = grad(ch, g, 2 * to + side_of(e))
            if more:
                partial_copy(ch, g, way, j, e).wait_recv()
                val = val + in_buf[g][way[0], j, ch, e].astype(F32)
            out_buf[g][way[0], j, ch, e] = val.astype(BF16)
            partial_copy(ch, g, way, j, e).start()

        for e in range(2):
            sends.append((cond, functools.partial(partial_copy, ch, g, way, j, e)))

    outs, passed = (gu_ref, gd_ref), (yu, yd)

    def store(ch, g, e):
        if ch == C:
            return pltpu.make_async_copy(igo, ig_ref, st_s.at[4 * C])
        src = passed[g].at[ch] if e else fin[g].at[ch, 1]
        dst = strip(g, outs[g], other if e else mine, ch)
        return pltpu.make_async_copy(src, dst, st_s.at[4 * ch + 2 * g + e])

    def final_y(ch, g):
        return remote(
            fin[g].at[ch, 0], passed[g].at[ch], fy_s.at[ch, g], fy_r.at[ch, g], ydev)

    def final_x(ch, g, e):
        src = passed[g].at[ch] if e else fin[g].at[ch, 1]
        i = (ch, g, e)
        return remote(
            src, strip(g, outs[g], other if e else mine, ch), fx_s.at[i], fx_r.at[i], xdev)

    def final_x_in(ch, g, e):
        q = 2 * (1 - r) + (1 - y if e else y)
        src = passed[g].at[ch] if e else fin[g].at[ch, 1]
        i = (ch, g, e)
        return remote(src, strip(g, outs[g], q, ch), fx_s.at[i], fx_r.at[i], xdev)

    def finish(ch, g, m0, between=None):
        cond = level[m0]
        ways = [(far, m0)] + ([(near, Z - 1 - m0)] if m0 else [])
        for e in range(2):
            val = grad(ch, g, 2 * z + side_of(e))
            for way, j in ways:
                partial_copy(ch, g, way, j, e).wait_recv()
                val = val + in_buf[g][way[0], j, ch, e].astype(F32)
            fin[g][ch, e] = val.astype(BF16)
            if e == 0:
                go(functools.partial(final_y, ch, g), cond)
                if between:
                    between()
            else:
                go(functools.partial(final_x, ch, g, 0), cond)
        store(ch, g, 0).start()

    def spread(ch, g, m0):
        final_y(ch, g).wait_recv()
        go(functools.partial(final_x, ch, g, 1), level[m0])
        store(ch, g, 1).start()

    h0 = isum0.shape[2]
    cuts = ((0, h0), (h0, D))
    isum, igot, ipt, ift = (isum0, isum1), (ira, irb), (ipt0, ipt1), (ift0, ift1)

    def ig_copy(i):
        if i == 0:
            return remote(igp.at[1], itr, ig_s.at[0], ig_r.at[0], tdev)
        if i > 6:
            side, part = (i - 7) % 2, pl.ds((i - 7) // 2 * half, half)
            src, dst = isum[side].at[1 + side, part, :], igot[side].at[0, part, :]
            return remote(src, dst, ig_s.at[i], ig_r.at[i], (xdev, ydev)[side])
        side, step = (i - 1) % 2, (i - 1) // 2
        if step == 1:
            src, dst = isum[side].at[3], igot[side].at[1]
        else:
            src, dst = ipt[side], ift[side]
        dev = (xdev, ydev)[side if step < 2 else 1 - side]
        return remote(src, dst, ig_s.at[i], ig_r.at[i], dev)

    def ig_go(i, cond):
        go(functools.partial(ig_copy, i), cond)

    def ig_part(cond):
        for dt in (1, 0):

            @pl.loop(0, n, unroll=2)
            def _(b):
                val = 0.0
                for ch in range(C):
                    lhs = jnp.concatenate([pg[ch, rows(k, dt), :] for k in range(4)], 0)
                    val = val + lax.dot_general(
                        lhs, ug[ch, blk(b), :], NT, preferred_element_type=F32)
                val = val.astype(BF16)
                for k in range(4):
                    igp[dt, k, :, blk(b)] = val[k * tok:(k + 1) * tok]

            if dt:
                ig_go(0, cond)

    def ig_first(cond):
        ig_copy(0).wait_recv()

        @pl.loop(0, 4)
        def _(k):
            val = igp[0, k].astype(F32) + itr[k].astype(F32)
            for side, (lo, hi) in enumerate(cuts):
                isum[side][k] = val[:, lo:hi].astype(BF16)

        for i in (4, 3):
            ig_go(i, cond)

    def ig_more(cond, part):
        for side in range(2):
            ig_go(7 + 2 * part + side, cond)

    def ig_second(cond):
        for side in range(2):
            ig_copy(3 + side).wait_recv()
            val = isum[side][2 - side].astype(F32) + igot[side][1].astype(F32)
            ipt[side][...] = val.astype(BF16)
            ig_go(5 + side, cond)

    def ig_last():
        for side, (lo, hi) in enumerate(cuts):
            for i in (5, 7, 9):
                ig_copy(i + side).wait_recv()
            val = isum[side][0].astype(F32) + igot[side][0].astype(F32)
            igo[:, lo:hi] = (val + ift[side][...].astype(F32)).astype(BF16)
        store(C, 0, 0).start()

    edge, inner = level[0], m > 0
    last = C - 1

    units = [(ch, g) for ch in range(C) for g in range(2)]

    loads["other", 0, 0].wait()
    go(functools.partial(swap, 0, 0))
    loads["mine", 0, 0].wait()
    begin(0, 0, 0)
    loads["x"].wait()
    for i in range(2):
        start("x", "x", i)
        start("y", "x", i)
    loads["mine", 0, 1].wait()
    begin(0, 1, 0, edge)
    start("s", "x", 0)
    loads["c"].wait()
    start("s", "c", 0)
    for unit in units[1:]:
        loads[("other",) + unit].wait()
        go(functools.partial(swap, *unit))
        if unit != units[1]:
            loads[("mine",) + unit].wait()

    swap(0, 0).wait_recv()
    begin(0, 0, 1)
    for unit in units[2:]:
        begin(*unit, 0, edge)
    relay(0, 0, 1)
    arrive("s", "x", 0)
    arrive("s", "c", 0)
    flip(0)
    arrive("y", "x", 0)
    start("d", "x", 0)
    for k in range(2, Z - 1):
        relay(0, 0, k)
    for unit in units[1:3]:
        begin(*unit, 0, inner)
    for i in range(2):
        arrive("x", "x", i)
    start("s", "x", 1)
    arrive("y", "x", 1)
    start("d", "x", 1)
    for i in range(min(2, Z)):
        start("x", "c", i)
        start("y", "c", i)
    start("s", "x", 2)
    swap(0, 1).wait_recv()
    begin(0, 1, 1)
    relay(0, 1, 1, (0,))
    arrive("s", "x", 1)
    flip(1)
    for k in range(2, Z - 1):
        relay(0, 1, k, (0,))
    relay(0, 1, 1, (1,))
    arrive("s", "x", 2)
    flip(2)
    collect(0, 0)
    forward(0, 0, 3)
    for unit in units[2:]:
        swap(*unit).wait_recv()
        begin(*unit, 1, edge)
    for i in range(2):
        arrive("d", "x", i)
    start("s", "x", 3)

    def ready(i):
        for k in range(1, 4):
            arrive("s%d" % k, "c", i)
        if i < Z - 1:
            pl.when(edge)(functools.partial(reduce, 0, 1, near, i, 0))

    tasks = [(unit, k) for unit in units[2:] for k in range(1, Z - 1)]
    for i in range(Z):
        arrive("x", "c", i)
        start("dy", "c", i)
        start("s1", "c", i)
        arrive("y", "c", i)
        start("dx", "c", i)
        start("s2", "c", i)
        if i + 2 < Z:
            start("x", "c", i + 2)
            start("y", "c", i + 2)
        if i == 0:
            for k in range(2, Z - 1):
                relay(0, 1, k, (1,))
            for unit in units[2:]:
                if unit != units[2]:
                    begin(*unit, 0, inner)
                begin(*unit, 1, inner)
            for unit in units[2:]:
                for k in range(1, Z // 2):
                    relay(*unit, k, toward=0)
            arrive("s", "x", 3)
            flip(3)
            forward(0, 3, 4)
        else:
            ready(i - 1)
            if i == Z - 1:
                for m0 in range(1, Z // 2):
                    pl.when(level[m0])(functools.partial(reduce, 0, 1, near, 0, m0))
        arrive("dy", "c", i)
        arrive("dx", "c", i)
        start("s3", "c", i)
        if i == 1 and tasks:
            unit, k = tasks.pop(0)
            relay(*unit, k, toward=1)
    ready(Z - 1)

    early = list(sends)
    sends.clear()

    def drain(some):
        for cond, make in some:
            if cond is None:
                make().wait_send()
            else:
                pl.when(cond)(lambda: make().wait_send())

    def flush(base, count):
        some = sends[base:count]
        del sends[base:count]
        drain(some)

    def edges():
        base = len(sends)
        collect(0, 1)
        backward(0)
        for j in range(Z - 1):
            reduce(0, 0, near, j, 0)
        drain(early)
        for ch in range(1, C):
            collect(ch, 0)
            forward(ch, 0, 4)
            for j in range(Z - 1):
                reduce(ch, 1, near, j, 0)
            collect(ch, 1)
            backward(ch)
            if ch < C - 1:
                for j in range(Z - 1):
                    reduce(ch, 0, near, j, 0)
        count = len(sends)
        ig_part(edge)
        finish(0, 1, 0)
        ig_first(edge)
        if C > 1:
            for j in range(Z - 1):
                reduce(C - 1, 0, near, j, 0)
        finish(0, 0, 0)
        spread(0, 1, 0)
        for ch in range(1, C):
            finish(ch, 1, 0)
            if ch == 1:
                ig_second(edge)
            spread(ch - 1, 0, 0)
            if ch == 1:
                ig_more(edge, 0)
                flush(base, count)
            finish(ch, 0, 0, lambda: spread(ch, 1, 0))
            if ch == 1:
                ig_more(edge, 1)
        if C == 1:
            ig_second(edge)
            ig_more(edge, 0)
            ig_more(edge, 1)
        spread(C - 1, 0, 0)
        ig_last()

    def inside(m0):
        cond, base = level[m0], len(sends)
        left = list(tasks)

        def relays(count):
            for _ in range(min(count, len(left))):
                unit, k = left.pop(0)
                relay(*unit, k, toward=1)

        def nears(ch, g, js):
            for j in js:
                reduce(ch, g, near, j, m0)

        def fars(ch, g):
            for j in range(m0):
                reduce(ch, g, far, j, m0)

        first, rest = range(1), range(1, Z - 1 - m0)
        keep = (Z - 2) * (C > 1)
        relays(len(left) - keep)
        nears(0, 1, rest)
        relays(keep - 1)
        backward(0)
        for ch in range(1, C):
            forward(ch, 0, 4)
        relays(1)
        fars(0, 1)
        for ch in range(1, C):
            backward(ch)
        nears(0, 0, first)
        finish(0, 1, m0)
        nears(0, 0, rest)
        spread(0, 1, m0)
        fars(0, 0)
        ig_part(cond)
        drain(early)
        finish(0, 0, m0)
        for ch in range(1, C):
            nears(ch, 1, first)
            if ch == 1:
                ig_first(cond)
            spread(ch - 1, 0, m0)
            if ch == 1:
                ig_more(cond, 0)
            nears(ch, 1, rest)
            fars(ch, 1)
            if ch == 1:
                ig_second(cond)
            finish(ch, 1, m0)
            count = len(sends)
            nears(ch, 0, (0, *rest))
            fars(ch, 0)
            if ch == 1:
                ig_more(cond, 1)
            spread(ch, 1, m0)
            if ch == C - 1:
                flush(base, count)
            finish(ch, 0, m0)
        if C == 1:
            ig_first(cond)
            ig_more(cond, 0)
            ig_more(cond, 1)
            ig_second(cond)
        spread(C - 1, 0, m0)
        ig_last()

    pl.when(edge)(edges)
    for m0 in range(1, Z // 2):
        pl.when(level[m0])(functools.partial(inside, m0))

    def settle():
        for ch in range(C):
            for g in (1, 0):
                for e in range(2):
                    final_x_in(ch, g, e).wait_recv()
                    store(ch, g, e).wait()
        store(C, 0, 0).wait()

    settle()
    drain(sends)


def ring_call(inputs, up_weight):
    R, n, T = axis_sizes()
    tok, D = inputs.shape
    db, hb = up_weight.shape[0], up_weight.shape[1] // R
    rows = R * T * tok
    C = tile_of(hb // 128, CHUNKS) if hb > 128 else 1
    w = hb // C
    V, S = pltpu.VMEM, pltpu.SemaphoreType.DMA
    hops = max(n // 2, 1)
    m = max(n - 1, 1)
    scratch = [
        V((n, rows, db), BF16), V((n, rows, db), BF16), V((n, db, rows), BF16),
        V((m, C, db, w), BF16), V((m, C, w, db), BF16),
        V((C, rows, w), F32), V((C, rows, w), F32), V((C, rows, w), BF16), V((C, w, rows), BF16),
        V((n, rows, db), BF16), V((max(T - 1, 1), n, R * tok, db), BF16),
        V((R, n, tok, db), BF16), V((max(R - 1, 1), n, tok, db), BF16),
        V((m, C, db, w), BF16), V((m, C, db, w), BF16),
        V((m, C, w, db), BF16), V((m, C, w, db), BF16),
        V((C, db, w), BF16), V((C, w, db), BF16),
        V((max(R - 1, 1), C, db, w), BF16), V((max(R - 1, 1), C, w, db), BF16),
        S((C, 4, hops)), S((C, 4, hops)), S((C, 4, hops)), S((C, 4, hops)),
        S((2, R)), S((2, R)), S((2, T, R)), S((2, T, R)),
        S((T,)), S((T,)), S((R,)), S((R,)), S((C, 2, R)), S((C, 2, R)),
    ]
    return functools.partial(ring_kernel, R, n, T), scratch, (R, hb), pltpu.VMEM


def axis_sizes():
    return lax.axis_size("rep"), lax.axis_size("fs"), lax.axis_size("tp")


def plane_call(inputs, up_weight):
    R, n, T = axis_sizes()
    tok, D = inputs.shape
    db, HB = up_weight.shape
    Z, G = n // 2, 2 * R
    if R != 2 or T != 2 or n % 4 or tok % 32 or HB % (128 * G) or db % 128 or D % 1024:
        return None
    hw = HB // G
    C = tile_of(hw // 128, CHUNKS)
    hc = hw // C
    rows, h0 = 8 * tok, D // 8
    h1 = D - h0
    V, S = pltpu.VMEM, pltpu.SemaphoreType.DMA
    data = [
        ((rows, D), BF16), ((rows, D), BF16), ((D, rows), BF16),
        ((C, D, hc), BF16), ((C, hc, D), BF16),
        ((C, rows, hc), F32), ((C, rows, hc), BF16), ((C, hc, rows), BF16),
        ((2, 4, tok, D), BF16), ((4, tok, D), BF16), ((4, tok, h0), BF16), ((4, tok, h1), BF16),
        ((2, tok, h0), BF16), ((2, tok, h1), BF16), ((tok, h0), BF16), ((tok, h1), BF16),
        ((tok, h0), BF16), ((tok, h1), BF16),
        ((tok, D), BF16),
        ((2, Z - 1, C, 2, db, hc), BF16), ((2, Z - 1, C, 2, hc, db), BF16),
        ((2, Z - 1, C, 2, db, hc), BF16), ((2, Z - 1, C, 2, hc, db), BF16),
        ((C, 2, db, hc), BF16), ((C, 2, hc, db), BF16),
        ((C, db, hc), BF16), ((C, hc, db), BF16), ((C, db, hc), BF16), ((C, hc, db), BF16),
    ]
    size = sum(math.prod(s) * jnp.dtype(d).itemsize for s, d in data)
    if size > 50 * 2**20:
        return None
    sems = [
        (C, 2), (C, 2, Z - 1, 2, 2), (4 + 2 * Z,), (2 + 2 * Z,), (5 + 3 * Z,),
        (2, Z - 1, C, 2, 2), (C, 2), (C, 2, 2), (11,),
    ]
    scratch = [V(s, d) for s, d in data] + [S(s) for s in sems for _ in range(2)]
    scratch += [S((4 * C + 2,)), S((4 * C + 1,))]
    return functools.partial(plane_kernel, Z), scratch, (1, HB), pl.ANY


def shards(inputs, cotangent, up_weight, down_weight):
    R, n, T = axis_sizes()
    tok, D = inputs.shape
    db = up_weight.shape[0]
    chosen = plane_call(inputs, up_weight) or ring_call(inputs, up_weight)
    body, scratch, (parts, hb), space = chosen
    spec = pl.BlockSpec(memory_space=space)
    ig, gu, gd = pl.pallas_call(
        body,
        out_shape=(
            jax.ShapeDtypeStruct((tok, D), BF16),
            jax.ShapeDtypeStruct((db, parts * hb), BF16),
            jax.ShapeDtypeStruct((parts * hb, db), BF16),
        ),
        in_specs=[spec] * 4,
        out_specs=(spec,) * 3,
        scratch_shapes=scratch,
        compiler_params=pltpu.CompilerParams(
            collective_id=0, has_side_effects=True, vmem_limit_bytes=60 * 2**20
        ),
    )(inputs, cotangent, up_weight, down_weight)
    total_tokens = tok * R * n * T
    loss_scale = 1.0 / math.sqrt(total_tokens)
    return ig, gu.astype(F32) * loss_scale, gd.astype(F32) * loss_scale


def solution(mesh):
    token, up, down = P(("rep", "fs", "tp"), None), P("fs", "tp"), P("tp", "fs")
    return jax.shard_map(
        shards,
        mesh=mesh,
        in_specs=(token, token, up, down),
        out_specs=(token, up, down),
        check_vma=False,
    )
```

```python
import functools
import math

import jax
import jax.numpy as jnp
from jax import lax
from jax.experimental import pallas as pl
from jax.experimental.pallas import tpu as pltpu
from jax.sharding import PartitionSpec as P

MESH = pl.DeviceIdType.MESH
CHUNKS = 2
BF16, F32 = jnp.bfloat16, jnp.float32
NT = (((1,), (1,)), ((), ()))


def ring_place(f, n):
    odd = lax.rem(f, 2)
    half = lax.div(f, 2)
    return half * (1 - odd) + (n - 1 - half) * odd


def ring_member(p, n):
    back = lax.div(p, (n + 1) // 2)
    return 2 * p * (1 - back) + (2 * n - 1 - 2 * p) * back


def tile_of(size, most):
    while size % most:
        most //= 2
    return most


def ring_kernel(
    R, n, T,
    x_ref, c_ref, u_ref, d_ref,
    ig_ref, gu_ref, gd_ref,
    xg, cg, xt, ug, dg, pre, agr, pg, at,
    igp, itr, isum, irr, us, ur, ds_, dr_, fu, fd, fur, fdr,
    ag_ss, ag_rs, rs_ss, rs_rs, tr_ss, tr_rs, tt_ss, tt_rs,
    it_ss, it_rs, ir_ss, ir_rs, f_ss, f_rs,
):
    r, f, t = lax.axis_index("rep"), lax.axis_index("fs"), lax.axis_index("tp")
    tok, db = x_ref.shape[0], u_ref.shape[0]
    C, w = pre.shape[0], pre.shape[2]
    hb = C * w
    rows = R * T * tok

    def hidden(place, ch):
        return pl.ds(pl.multiple_of(place * hb + ch * w, w), w)

    for ref, full in ((x_ref, xg), (c_ref, cg)):
        for q in range(n):
            full[q, 0:tok, :] = ref[:, q * db:(q + 1) * db]
    p = ring_place(f, n)

    def member(q):
        return ring_member(lax.rem(p + q + n, n), n)

    def ring_dev(sign):
        return (r, member(sign), t)

    def rep_dev(q):
        return (lax.rem(r + q + R, R), f, t)

    def tp_dev(q):
        return (r, f, lax.rem(t + q + T, T))

    barrier = pltpu.get_barrier_semaphore()
    peers = [ring_dev(1), ring_dev(-1)]
    peers += [rep_dev(q) for q in range(1, R)] + [tp_dev(q) for q in range(1, T)]
    for peer in peers:
        pl.semaphore_signal(barrier, inc=1, device_id=peer, device_id_type=MESH)
    pl.semaphore_wait(barrier, len(peers))

    def remote(src, dst, ssem, rsem, dev):
        return pltpu.make_async_remote_copy(
            src_ref=src, dst_ref=dst, send_sem=ssem, recv_sem=rsem,
            device_id=dev, device_id_type=MESH,
        )

    long, short = n // 2, (n - 1) // 2
    streams = [(0, 1, long), (0, -1, short), (1, 1, short), (1, -1, long)]
    hops = max(long, short)
    def own(g, ch):
        return u_ref.at[:, hidden(r, ch)] if g == 0 else d_ref.at[hidden(r, ch), :]

    held = (ug, dg)

    def slot(sign, s):
        return (n - s if sign > 0 else s) - 1

    def gather_copy(ch, i, s):
        g, sign, _ = streams[i]
        src = own(g, ch) if s == 1 else held[g].at[slot(sign, s - 1), ch]
        return remote(
            src, held[g].at[slot(sign, s), ch],
            ag_ss.at[ch, i, s - 1], ag_rs.at[ch, i, s - 1], ring_dev(sign),
        )

    sends = []

    def go(copy):
        copy.start()
        sends.append(copy)
        return copy

    flying = {}

    def gather_first(ch):
        for i, (g, sign, k) in enumerate(streams):
            if k >= 1:
                flying[ch, i, 1] = go(gather_copy(ch, i, 1))

    gather_first(0)

    tokens = tuple((full.at[:, 0:tok, :], full) for full in (xg, cg))

    def span(dt, dr):
        return pl.ds((dt * R + dr) * tok, tok)

    rep_copies = {}
    for dr in range(1, R):
        for j, (ref, full) in enumerate(tokens):
            rep_copies[j, dr] = go(remote(
                ref, full.at[:, span(0, dr), :], tr_ss.at[j, dr], tr_rs.at[j, dr], rep_dev(-dr)
            ))
    tp_copies = {}
    for dt in range(1, T):
        for j, (ref, full) in enumerate(tokens):
            tp_copies[j, dt, 0] = go(remote(
                ref, full.at[:, span(dt, 0), :], tt_ss.at[j, dt, 0], tt_rs.at[j, dt, 0],
                tp_dev(-dt),
            ))

    row_tile = tile_of(rows, 256)

    def gather_dot(ch, g, block, q, first=False):
        b = member(q)
        out, full = ((pre, xg), (agr, cg))[g]

        @pl.loop(0, rows // row_tile)
        def _(i):
            part = pl.ds(pl.multiple_of(i * row_tile, row_tile), row_tile)
            lhs = full[b, part, :]
            if g == 0:
                val = jnp.dot(lhs, block[...], preferred_element_type=F32)
            else:
                val = lax.dot_general(lhs, block[...], NT, preferred_element_type=F32)
            if first:
                out[ch, part, :] = val
            else:
                out[ch, part, :] += val

    def finish_tokens():
        for dr in range(1, R):
            for j, (ref, full) in enumerate(tokens):
                rep_copies[j, dr].wait_recv()
                for dt in range(1, T):
                    tp_copies[j, dt, dr] = go(remote(
                        full.at[:, span(0, dr), :], full.at[:, span(dt, dr), :],
                        tt_ss.at[j, dt, dr], tt_rs.at[j, dt, dr], tp_dev(-dt),
                    ))
        for copy in tp_copies.values():
            copy.wait_recv()

        @pl.loop(0, n)
        def _(b):
            xt[b] = xg[b].T

        for ch in range(C):
            gather_dot(ch, 0, own(0, ch), 0, True)
            gather_dot(ch, 1, own(1, ch), 0, True)

    act_tile = tile_of(rows, 128)

    def activate(ch):
        @pl.loop(0, rows // act_tile)
        def _(i):
            part = pl.ds(pl.multiple_of(i * act_tile, act_tile), act_tile)
            active = jnp.maximum(pre[ch, part, :], 0.0)
            pg[ch, part, :] = (2.0 * active * agr[ch, part, :]).astype(BF16)
            at[ch, :, part] = (active * active).astype(BF16).T

    def gather(ch, before_last):
        for s in range(1, hops + 1):
            if s == hops:
                before_last()
            for i, (g, sign, k) in enumerate(streams):
                if s <= k:
                    flying[ch, i, s].wait_recv()
                    if s < k:
                        flying[ch, i, s + 1] = go(gather_copy(ch, i, s + 1))
            if s == 1 and ch == 0:
                finish_tokens()
            for i, (g, sign, k) in enumerate(streams):
                if s <= k:
                    gather_dot(ch, g, held[g].at[slot(sign, s), ch], -sign * s)
        if hops == 0:
            if ch == 0:
                finish_tokens()
            before_last()
        activate(ch)

    def grad_block(ch, g, q, dst, arrived):
        b = member(q)
        height = (db, w)[g]
        tile = tile_of(height, 256)

        @pl.loop(0, height // tile)
        def _(i):
            part = pl.ds(pl.multiple_of(i * tile, tile), tile)
            if g == 0:
                val = jnp.dot(xt[b, part, :], pg[ch], preferred_element_type=F32)
            else:
                val = jnp.dot(at[ch, part, :], cg[b], preferred_element_type=F32)
            for a in arrived:
                val = val + a[part, :].astype(F32)
            dst[part, :] = val.astype(BF16)

    rs_send, rs_recv = (us, ds_), (ur, dr_)

    def rs_index(i, s):
        g, sign, _ = streams[i]
        return s - 1 if sign > 0 else (long, short)[g] + s - 1

    reducing = {}

    def reduce_step(ch, i, s):
        g, sign, k = streams[i]
        arrived = []
        if s > 1:
            reducing[ch, i, s - 1].wait_recv()
            arrived = [rs_recv[g].at[rs_index(i, s - 1), ch]]
        mine = rs_send[g].at[rs_index(i, s), ch]
        grad_block(ch, g, sign * (k - s + 1), mine, arrived)
        reducing[ch, i, s] = go(remote(
            mine, rs_recv[g].at[rs_index(i, s), ch],
            rs_ss.at[ch, i, s - 1], rs_rs.at[ch, i, s - 1], ring_dev(sign),
        ))

    def reduce_all(ch, s):
        for i, (g, sign, k) in enumerate(streams):
            if s <= k:
                reduce_step(ch, i, s)

    for ch in range(C):
        if ch + 1 < C:
            gather(ch, functools.partial(gather_first, ch + 1))
        elif C > 1:
            gather(ch, functools.partial(reduce_all, 0, 1))
        else:
            gather(ch, lambda: None)
            reduce_all(ch, 1)

    for q in range(n):
        b = member(q)

        @pl.loop(0, rows // row_tile)
        def _(i):
            part = pl.ds(pl.multiple_of(i * row_tile, row_tile), row_tile)
            val = 0.0
            for ch in range(C):
                block = own(0, ch) if q == 0 else ug.at[q - 1, ch]
                val = val + lax.dot_general(
                    pg[ch, part, :], block[...], NT, preferred_element_type=F32
                )
            igp[b, part, :] = val.astype(BF16)

    wide = R * tok
    it_copies = [
        go(remote(
            igp.at[:, pl.ds(dt * wide, wide), :], itr.at[dt - 1],
            it_ss.at[dt], it_rs.at[dt], tp_dev(dt),
        ))
        for dt in range(1, T)
    ]
    ir_copies = []

    def finish_tp():
        for copy in it_copies:
            copy.wait_recv()

        @pl.loop(0, n)
        def _(b):
            for dr in range(R):
                part = pl.ds(dr * tok, tok)
                val = igp[b, part, :].astype(F32)
                for dt in range(1, T):
                    val = val + itr[dt - 1, b, part, :].astype(F32)
                isum[dr, b] = val.astype(BF16)

        for dr in range(1, R):
            ir_copies.append(go(remote(
                isum.at[dr], irr.at[dr - 1], ir_ss.at[dr], ir_rs.at[dr], rep_dev(dr)
            )))

    def finish_rep():
        for copy in ir_copies:
            copy.wait_recv()

        for b in range(n):
            val = isum[0, b].astype(F32)
            for dr in range(1, R):
                val = val + irr[dr - 1, b].astype(F32)
            ig_ref[:, b * db:(b + 1) * db] = val.astype(BF16)

    finish_tp()

    finals = ((fu, fur, gu_ref), (fd, fdr, gd_ref))
    fin_copies = {}

    def put(g, place, ch, val):
        if g == 0:
            gu_ref[:, hidden(place, ch)] = val
        else:
            gd_ref[hidden(place, ch), :] = val

    def finish(ch, g):
        mine, theirs, out = finals[g]
        arrived = []
        for i, (h, sign, k) in enumerate(streams):
            if h == g and k >= 1:
                reducing[ch, i, k].wait_recv()
                arrived.append(rs_recv[g].at[rs_index(i, k), ch])
        grad_block(ch, g, 0, mine.at[ch], arrived)
        for dr in range(1, R):
            fin_copies[ch, g, dr] = go(remote(
                mine.at[ch], theirs.at[dr - 1, ch],
                f_ss.at[ch, g, dr], f_rs.at[ch, g, dr], rep_dev(-dr),
            ))
        put(g, r, ch, mine[ch])

    for ch in range(C):
        for s in range(2, hops + 1):
            reduce_all(ch, s)
            if ch == 0 and s == 2:
                finish_rep()
        if ch == 0 and hops < 2:
            finish_rep()
        if ch + 1 < C:
            reduce_all(ch + 1, 1)
        for g in range(2):
            finish(ch, g)
    for (ch, g, dr), copy in fin_copies.items():
        _, theirs, out = finals[g]
        copy.wait_recv()
        put(g, lax.rem(r + dr, R), ch, theirs[dr - 1, ch])
    for copy in sends:
        copy.wait_send()


def plane_kernel(
    Z,
    x_ref, c_ref, u_ref, d_ref,
    ig_ref, gu_ref, gd_ref,
    xg, cg, xt, ug, dg, pre, pg, at,
    igp, itr, isum, igot, ipt, ift, igo, su, sd, ru, rd, fu, fd, uo, do, yu, yd,
    out_s, yw_r, zg_r, tx_r, ty_r, tt_r, rs_r, fy_r, fx_r, ig_r, ld_s, st_s,
):
    r, f, t = lax.axis_index("rep"), lax.axis_index("fs"), lax.axis_index("tp")
    z, y = lax.div(f, 2), lax.rem(f, 2)
    tok, D = x_ref.shape
    db = u_ref.shape[0]
    C, hc = pg.shape[0], pg.shape[2]
    hw, half, wide = C * hc, tok // 2, 2 * tok
    n = 2 * Z
    xdev, ydev, tdev = (1 - r, f, t), (r, f + 1 - 2 * y, t), (r, f, 1 - t)

    def zdev(s):
        return (r, f + 2 * s, t)

    low = z < Z // 2
    m = jnp.where(low, z, Z - 1 - z)
    near = (jnp.where(low, 0, 1), jnp.where(low, 1, -1))
    far = (1 - near[0], -near[1])

    ahead = {1: z < Z - 1, -1: z > 0}

    def remote(src, dst, ssem, rsem, dev):
        return pltpu.make_async_remote_copy(
            src_ref=src, dst_ref=dst, send_sem=ssem, recv_sem=rsem,
            device_id=dev, device_id_type=MESH,
        )

    def go(make):
        make().start()

    def span(at_, size):
        return pl.ds(pl.multiple_of(at_, size), size)

    def blk(b):
        return span(b * db, db)

    def hid(q, ch):
        return span(q * hw + ch * hc, hc)

    mine, other = 2 * r + y, 2 * r + 1 - y

    def held(g, ch, b):
        return ug.at[ch, blk(b), :] if g == 0 else dg.at[ch, :, blk(b)]

    spare = (uo, do)
    weights = (u_ref, d_ref)

    def strip(g, ref, q, ch):
        return ref.at[:, hid(q, ch)] if g == 0 else ref.at[hid(q, ch), :]

    own_x, own_c = xg.at[pl.ds(0, tok), :], cg.at[pl.ds(0, tok), :]
    loads = {}
    for ch in range(C):
        for g in range(2):
            loads["other", ch, g] = (strip(g, weights[g], other, ch), spare[g].at[ch])
            loads["mine", ch, g] = (strip(g, weights[g], mine, ch), held(g, ch, f))
        if ch == 0:
            loads["x"] = (x_ref, own_x)
            loads["c"] = (c_ref, own_c)
    loads = {
        key: pltpu.make_async_copy(src, dst, ld_s.at[i])
        for i, (key, (src, dst)) in enumerate(loads.items())
    }
    for copy in loads.values():
        copy.start()

    barrier = pltpu.get_barrier_semaphore()

    def greet(dev):
        pl.semaphore_signal(barrier, inc=1, device_id=dev, device_id_type=MESH)

    for dev in (xdev, ydev, tdev):
        greet(dev)
    for s in (1, -1):
        pl.when(ahead[s])(functools.partial(greet, zdev(s)))
    pl.semaphore_wait(barrier, 3 + sum(jnp.where(ahead[s], 1, 0) for s in (1, -1)))

    def swap(ch, g):
        return remote(spare[g].at[ch], held(g, ch, f), out_s.at[0], yw_r.at[ch, g], ydev)

    def origin(s, k, e):
        return f - 2 * s * k + e * (1 - 2 * y)

    def pass_on(ch, g, s, k, e):
        block = held(g, ch, origin(s, k, e))
        i = (ch, (1 - s) // 2, k, e, g)
        return remote(block, block, out_s.at[i[1] + 1], zg_r.at[i], zdev(s))

    def landed(ch, g, s, k, e):
        block = held(g, ch, origin(s, k, e))
        i = (ch, (1 - s) // 2, k - 1, e, g)
        return remote(block, block, out_s.at[i[1] + 1], zg_r.at[i], zdev(s))

    def begin(ch, g, e, also=None):
        for s in (1, -1):
            cond = ahead[s] if also is None else ahead[s] & also
            pl.when(cond)(functools.partial(
                go, functools.partial(pass_on, ch, g, s, 0, e)))

    level = [m == m0 for m0 in range(Z // 2)]
    reached = {}
    for k in range(1, Z):
        reached[1, k], reached[-1, k] = z >= k, z < Z - k
    passing = {key: reached[key] & ahead[key[0]] for key in reached}

    outward = {1: low, -1: jnp.logical_not(low)}
    split = {}
    for (s, k), cond in passing.items():
        split[s, k, 0] = cond & outward[s]
        split[s, k, 1] = cond & outward[-s]

    def relay(ch, g, k, es=(0, 1), toward=None):
        for e in es:
            for s in (1, -1):
                cond = passing[s, k] if toward is None else split[s, k, toward]

                @pl.when(cond)
                def _():
                    landed(ch, g, s, k, e).wait_recv()
                    go(functools.partial(pass_on, ch, g, s, k, e))

    def collect(ch, g):
        for k in range(1, Z):
            for e in range(2):
                for s in (1, -1):

                    @pl.when(reached[s, k] & jnp.logical_not(ahead[s]))
                    def _():
                        landed(ch, g, s, k, e).wait_recv()

    def swapped(ch, g, also=None):
        begin(ch, g, 1, also)

    def rows(k, dt, part=(0, 2)):
        lo, hi = part
        return pl.ds((2 * k + dt) * tok + lo * half, (hi - lo) * half)

    def quarter(i):
        return span(jnp.where(low, Z - 1 - i, i) * 2 * db, 2 * db)

    A, B, AB = (0, 1), (1, 2), (0, 2)

    def hop(sems, i, dev, full, src, dst, cols):
        def make():
            where = slice(None) if cols is None else quarter(cols)
            return remote(
                full.at[rows(*src), where], full.at[rows(*dst), where],
                sems[0], sems[1].at[i], dev,
            )

        return make

    X, Y, S = (out_s.at[3], tx_r), (out_s.at[4], ty_r), (out_s.at[5], tt_r)
    moves = {}
    for i, part in enumerate((A, B)):
        moves["x", "x", i] = hop(X, i, xdev, xg, (0, 0, part), (1, 0, part), None)
        moves["y", "x", i] = hop(Y, i, ydev, xg, (0, 0, part), (2, 0, part), None)
        moves["d", "x", i] = hop(X, 2 + i, xdev, xg, (2, 0, part), (3, 0, part), None)
    moves["s", "x", 0] = hop(S, 0, tdev, xg, (0, 0, AB), (0, 1, AB), None)
    moves["s", "c", 0] = hop(S, 1, tdev, cg, (0, 0, AB), (0, 1, AB), None)
    for k in range(1, 4):
        moves["s", "x", k] = hop(S, 1 + k, tdev, xg, (k, 0, AB), (k, 1, AB), None)
    for i in range(Z):
        for p, (xp, yp) in enumerate(((B, A), (A, B))):
            moves["x%d" % p, "c", i] = hop(X, 4 + 3 * i + p, xdev, cg, (0, 0, xp), (1, 0, xp), i)
            moves["y%d" % p, "c", i] = hop(Y, 2 + 3 * i + p, ydev, cg, (0, 0, yp), (2, 0, yp), i)
        moves["dx", "c", i] = hop(X, 6 + 3 * i, xdev, cg, (2, 0, A), (3, 0, A), i)
        moves["dy", "c", i] = hop(Y, 4 + 3 * i, ydev, cg, (1, 0, B), (3, 0, B), i)
        for k in range(1, 4):
            moves["s%d" % k, "c", i] = hop(
                S, 5 + (k - 1) * Z + i, tdev, cg, (k, 0, AB), (k, 1, AB), i)

    def start(*key):
        go(moves[key])

    def arrive(*key):
        moves[key]().wait_recv()

    def flip(k):
        part = pl.ds(k * wide, wide)

        @pl.loop(0, n)
        def _(b):
            xt[blk(b), part] = xg[part, blk(b)].T

    def forward(ch, first, last):
        @pl.loop(first, last, unroll=2 if (last - first) % 2 == 0 else 1)
        def _(k):
            part = span(k * wide, wide)
            active = jnp.maximum(
                jnp.dot(xg[part, :], ug[ch], preferred_element_type=F32), 0.0)
            pre[ch, part, :] = active
            at[ch, :, part] = (active * active).astype(BF16).T

    def backward(ch):
        @pl.loop(0, 4, unroll=2)
        def _(k):
            part = span(k * wide, wide)
            val = lax.dot_general(cg[part, :], dg[ch], NT, preferred_element_type=F32)
            pg[ch, part, :] = (2.0 * pre[ch, part, :] * val).astype(BF16)

    def grad(ch, g, b):
        if g == 0:
            return jnp.dot(xt[blk(b), :], pg[ch], preferred_element_type=F32)
        return jnp.dot(at[ch], cg[:, blk(b)], preferred_element_type=F32)

    out_buf, in_buf, fin = (su, sd), (ru, rd), (fu, fd)

    def partial_copy(ch, g, way, j, e):
        d, s = way
        return remote(
            out_buf[g].at[d, j, ch, e], in_buf[g].at[d, j, ch, e],
            out_s.at[6], rs_r.at[d, j, ch, g, e], zdev(s))

    def side_of(e):
        return e * y + (1 - e) * (1 - y)

    def reduce(ch, g, way, j, m0):
        cond = level[m0]
        to = jnp.where(way[1] > 0, Z - 1 - j, j)
        more = m0 > 0 or way is far

        @pl.loop(0, 2)
        def _(e):
            val = grad(ch, g, 2 * to + side_of(e))
            if more:
                partial_copy(ch, g, way, j, e).wait_recv()
                val = val + in_buf[g][way[0], j, ch, e].astype(F32)
            out_buf[g][way[0], j, ch, e] = val.astype(BF16)
            partial_copy(ch, g, way, j, e).start()

    outs, passed = (gu_ref, gd_ref), (yu, yd)

    def store(ch, g, e):
        if ch == C:
            return pltpu.make_async_copy(igo, ig_ref, st_s.at[4 * C])
        src = passed[g].at[ch] if e else fin[g].at[ch, 1]
        dst = strip(g, outs[g], other if e else mine, ch)
        return pltpu.make_async_copy(src, dst, st_s.at[4 * ch + 2 * g + e])

    def final_y(ch, g):
        return remote(
            fin[g].at[ch, 0], passed[g].at[ch], out_s.at[7], fy_r.at[ch, g], ydev)

    def final_x(ch, g, e):
        src = passed[g].at[ch] if e else fin[g].at[ch, 1]
        i = (ch, g, e)
        return remote(
            src, strip(g, outs[g], other if e else mine, ch), out_s.at[7], fx_r.at[i], xdev)

    def final_x_in(ch, g, e):
        q = 2 * (1 - r) + (1 - y if e else y)
        src = passed[g].at[ch] if e else fin[g].at[ch, 1]
        i = (ch, g, e)
        return remote(src, strip(g, outs[g], q, ch), out_s.at[7], fx_r.at[i], xdev)

    def finish(ch, g, m0, between=None):
        cond = level[m0]
        ways = [(far, m0)] + ([(near, Z - 1 - m0)] if m0 else [])
        for e in range(2):
            val = grad(ch, g, 2 * z + side_of(e))
            for way, j in ways:
                partial_copy(ch, g, way, j, e).wait_recv()
                val = val + in_buf[g][way[0], j, ch, e].astype(F32)
            fin[g][ch, e] = val.astype(BF16)
            if e == 0:
                go(functools.partial(final_y, ch, g))
                if between:
                    between()
            else:
                go(functools.partial(final_x, ch, g, 0))
        store(ch, g, 0).start()

    def spread(ch, g, m0):
        final_y(ch, g).wait_recv()
        go(functools.partial(final_x, ch, g, 1))
        store(ch, g, 1).start()

    def ig_copy(i):
        if i == 0:
            return remote(igp.at[1], itr, out_s.at[8], ig_r.at[0], tdev)
        kind, part = (i - 1) // 2, pl.ds((i - 1) % 2 * half, half)
        if kind < 2:
            src, dst = isum.at[3 - kind, part, :], igot.at[1 - kind, part, :]
        else:
            src, dst = ipt.at[part, :], ift.at[part, :]
        return remote(src, dst, out_s.at[8], ig_r.at[i], ydev if kind < 2 else xdev)

    def ig_go(i):
        go(functools.partial(ig_copy, i))

    def ig_part():
        for dt in (1, 0):

            @pl.loop(0, n, unroll=4)
            def _(b):
                val = 0.0
                for ch in range(C):
                    lhs = jnp.concatenate([pg[ch, rows(k, dt), :] for k in range(4)], 0)
                    val = val + lax.dot_general(
                        lhs, ug[ch, blk(b), :], NT, preferred_element_type=F32)
                val = val.astype(BF16)
                for k in range(4):
                    igp[dt, k, :, blk(b)] = val[k * tok:(k + 1) * tok]

            if dt:
                ig_go(0)

    def ig_first():
        ig_copy(0).wait_recv()

        @pl.loop(0, 4)
        def _(k):
            isum[k] = (igp[0, k].astype(F32) + itr[k].astype(F32)).astype(BF16)

    def ig_diag(p):
        ig_go(1 + p)

    def ig_more(p):
        ig_go(3 + p)

    def ig_second(p):
        ig_copy(1 + p).wait_recv()
        part = pl.ds(p * half, half)
        val = isum[1, part, :].astype(F32) + igot[1, part, :].astype(F32)
        ipt[part, :] = val.astype(BF16)
        ig_go(5 + p)

    def ig_last():
        for i in range(3, 7):
            ig_copy(i).wait_recv()
        val = isum[0].astype(F32) + igot[0].astype(F32) + ift[...].astype(F32)
        igo[...] = val.astype(BF16)
        store(C, 0, 0).start()

    edge, inner = level[0], m > 0
    last = C - 1

    units = [(ch, g) for ch in range(C) for g in range(2)]

    loads["other", 0, 0].wait()
    go(functools.partial(swap, 0, 0))
    loads["mine", 0, 0].wait()
    begin(0, 0, 0)
    loads["x"].wait()
    for i in range(2):
        start("x", "x", i)
        start("y", "x", i)
    loads["mine", 0, 1].wait()
    begin(0, 1, 0)
    start("s", "x", 0)
    loads["c"].wait()
    start("s", "c", 0)
    for unit in units[1:]:
        loads[("other",) + unit].wait()
        go(functools.partial(swap, *unit))
        if unit != units[1]:
            loads[("mine",) + unit].wait()

    swap(0, 0).wait_recv()
    begin(0, 0, 1)
    for unit in units[2:]:
        begin(*unit, 0, edge)
    relay(0, 0, 1)
    arrive("s", "x", 0)
    arrive("s", "c", 0)
    flip(0)
    arrive("y", "x", 0)
    start("d", "x", 0)
    for k in range(2, Z - 1):
        relay(0, 0, k)
    for unit in units[2:3]:
        begin(*unit, 0, inner)
    for i in range(2):
        arrive("x", "x", i)
    start("s", "x", 1)
    arrive("y", "x", 1)
    start("d", "x", 1)

    def offer(i):
        for way in ("x0", "y0", "x1", "y1"):
            start(way, "c", i)

    offer(0)
    start("s", "x", 2)
    swap(0, 1).wait_recv()
    begin(0, 1, 1)
    relay(0, 1, 1, (0,))
    arrive("s", "x", 1)
    flip(1)
    for k in range(2, Z - 1):
        relay(0, 1, k, (0,))
    relay(0, 1, 1, (1,))
    arrive("s", "x", 2)
    flip(2)
    collect(0, 0)
    forward(0, 0, 3)
    for unit in units[2:]:
        swap(*unit).wait_recv()
        begin(*unit, 1, edge)
    for i in range(2):
        arrive("d", "x", i)
    start("s", "x", 3)

    def ready(i):
        for k in range(1, 4):
            arrive("s%d" % k, "c", i)
        if i < Z - 1:
            pl.when(edge)(functools.partial(reduce, 0, 1, near, i, 0))

    tasks = [(unit, k) for unit in units[2:] for k in range(1, Z - 1)]
    for i in range(Z):
        arrive("x0", "c", i)
        start("dy", "c", i)
        arrive("y0", "c", i)
        start("dx", "c", i)
        if i + 1 < Z:
            offer(i + 1)
        if i == 0:
            for k in range(2, Z - 1):
                relay(0, 1, k, (1,))
            for unit in units[2:]:
                if unit != units[2]:
                    begin(*unit, 0, inner)
                begin(*unit, 1, inner)
            for unit in units[2:]:
                for k in range(1, Z // 2):
                    relay(*unit, k, toward=0)
            arrive("s", "x", 3)
            flip(3)
            forward(0, 3, 4)
        else:
            if i > 1:
                ready(i - 1)
            if i == Z - 1:
                for m0 in range(1, Z // 2):
                    pl.when(level[m0])(functools.partial(reduce, 0, 1, near, 0, m0))
        arrive("x1", "c", i)
        start("s1", "c", i)
        arrive("y1", "c", i)
        start("s2", "c", i)
        arrive("dy", "c", i)
        arrive("dx", "c", i)
        start("s3", "c", i)
        if i == 0:
            ready(0)
        if i == 1 and tasks:
            unit, k = tasks.pop(0)
            relay(*unit, k, toward=1)
    if Z > 1:
        ready(Z - 1)

    def edges():
        collect(0, 1)
        backward(0)
        for j in range(Z - 1):
            reduce(0, 0, near, j, 0)
        for ch in range(1, C):
            collect(ch, 0)
            forward(ch, 0, 4)
            for j in range(Z - 1):
                reduce(ch, 1, near, j, 0)
            collect(ch, 1)
            backward(ch)
            if ch < C - 1:
                for j in range(Z - 1):
                    reduce(ch, 0, near, j, 0)
        ig_part()
        finish(0, 1, 0)
        ig_first()
        ig_diag(0)
        if C > 1:
            for j in range(Z - 1):
                reduce(C - 1, 0, near, j, 0)
        finish(0, 0, 0)
        ig_diag(1)
        spread(0, 1, 0)
        ig_second(0)
        for ch in range(1, C):
            finish(ch, 1, 0)
            spread(ch - 1, 0, 0)
            if ch == 1:
                ig_more(0)
                ig_second(1)
            finish(ch, 0, 0, lambda: spread(ch, 1, 0))
            if ch == 1:
                ig_more(1)
        if C == 1:
            ig_more(0)
            ig_second(1)
            ig_more(1)
        spread(C - 1, 0, 0)
        ig_last()

    def inside(m0):
        left = list(tasks)

        def relays(count):
            for _ in range(min(count, len(left))):
                unit, k = left.pop(0)
                relay(*unit, k, toward=1)

        def nears(ch, g, js):
            for j in js:
                reduce(ch, g, near, j, m0)

        def fars(ch, g):
            for j in range(m0):
                reduce(ch, g, far, j, m0)

        first, rest = range(1), range(1, Z - 1 - m0)
        keep = (Z - 2) * (C > 1)
        relays(len(left) - keep)
        nears(0, 1, rest)
        relays(keep - 1)
        backward(0)
        for ch in range(1, C):
            forward(ch, 0, 4)
        relays(1)
        fars(0, 1)
        for ch in range(1, C):
            backward(ch)
        nears(0, 0, first)
        finish(0, 1, m0)
        nears(0, 0, rest)
        spread(0, 1, m0)
        fars(0, 0)
        ig_part()
        finish(0, 0, m0)
        for ch in range(1, C):
            nears(ch, 1, first)
            if ch == 1:
                ig_first()
                ig_diag(0)
                ig_diag(1)
            spread(ch - 1, 0, m0)
            nears(ch, 1, rest)
            fars(ch, 1)
            if ch == 1:
                ig_second(0)
            finish(ch, 1, m0)
            nears(ch, 0, first)
            if ch == 1:
                ig_more(0)
                ig_second(1)
                ig_more(1)
            nears(ch, 0, rest)
            fars(ch, 0)
            spread(ch, 1, m0)
            finish(ch, 0, m0)
        if C == 1:
            ig_first()
            for p in range(2):
                ig_diag(p)
                ig_more(p)
            for p in range(2):
                ig_second(p)
        spread(C - 1, 0, m0)
        ig_last()

    pl.when(edge)(edges)
    for m0 in range(1, Z // 2):
        pl.when(level[m0])(functools.partial(inside, m0))

    def settle():
        for ch in range(C):
            for g in (1, 0):
                for e in range(2):
                    final_x_in(ch, g, e).wait_recv()
                    store(ch, g, e).wait()
        store(C, 0, 0).wait()

    def sent(i, count):
        some = xg.at[pl.ds(0, count), :]
        remote(some, some, out_s.at[i], out_s.at[i], xdev).wait_send()

    def drain():
        block = 4 * hw // n
        sent(0, block // 2)
        for z0 in range(Z - 1):
            pl.when(z == z0)(functools.partial(sent, 1, (z0 + 1) * block))
            pl.when(z == Z - 1 - z0)(functools.partial(sent, 2, (z0 + 1) * block))
        sent(3, 7 * half)
        sent(4, 5 * half)
        sent(5, 8 * tok)
        sent(6, (Z - 1) * block)
        sent(7, 3 * block // 2)
        sent(8, 7 * tok)

    settle()
    drain()


def ring_call(inputs, up_weight):
    R, n, T = axis_sizes()
    tok, D = inputs.shape
    db, hb = up_weight.shape[0], up_weight.shape[1] // R
    rows = R * T * tok
    C = tile_of(hb // 128, CHUNKS) if hb > 128 else 1
    w = hb // C
    V, S = pltpu.VMEM, pltpu.SemaphoreType.DMA
    hops = max(n // 2, 1)
    m = max(n - 1, 1)
    scratch = [
        V((n, rows, db), BF16), V((n, rows, db), BF16), V((n, db, rows), BF16),
        V((m, C, db, w), BF16), V((m, C, w, db), BF16),
        V((C, rows, w), F32), V((C, rows, w), F32), V((C, rows, w), BF16), V((C, w, rows), BF16),
        V((n, rows, db), BF16), V((max(T - 1, 1), n, R * tok, db), BF16),
        V((R, n, tok, db), BF16), V((max(R - 1, 1), n, tok, db), BF16),
        V((m, C, db, w), BF16), V((m, C, db, w), BF16),
        V((m, C, w, db), BF16), V((m, C, w, db), BF16),
        V((C, db, w), BF16), V((C, w, db), BF16),
        V((max(R - 1, 1), C, db, w), BF16), V((max(R - 1, 1), C, w, db), BF16),
        S((C, 4, hops)), S((C, 4, hops)), S((C, 4, hops)), S((C, 4, hops)),
        S((2, R)), S((2, R)), S((2, T, R)), S((2, T, R)),
        S((T,)), S((T,)), S((R,)), S((R,)), S((C, 2, R)), S((C, 2, R)),
    ]
    return functools.partial(ring_kernel, R, n, T), scratch, (R, hb), pltpu.VMEM


def finals_kernel(scale, ig, gu, gd, ig_out, gu_out, gd_out):
    ig_out[...] = ig[...]
    gu_out[...] = gu[...].astype(F32) * scale
    gd_out[...] = gd[...].astype(F32) * scale


def finals_call(ig, gu, gd, scale):
    steps = 4
    tok, D = ig.shape
    db, HB = gu.shape
    specs = [
        pl.BlockSpec((tok // steps, D), lambda i: (i, 0)),
        pl.BlockSpec((db // steps, HB), lambda i: (i, 0)),
        pl.BlockSpec((HB // steps, db), lambda i: (i, 0)),
    ]
    return pl.pallas_call(
        functools.partial(finals_kernel, scale),
        grid=(steps,),
        in_specs=specs,
        out_specs=specs,
        out_shape=(
            jax.ShapeDtypeStruct(ig.shape, BF16),
            jax.ShapeDtypeStruct(gu.shape, F32),
            jax.ShapeDtypeStruct(gd.shape, F32),
        ),
    )(ig, gu, gd)


def axis_sizes():
    return lax.axis_size("rep"), lax.axis_size("fs"), lax.axis_size("tp")


def plane_call(inputs, up_weight):
    R, n, T = axis_sizes()
    tok, D = inputs.shape
    db, HB = up_weight.shape
    Z, G = n // 2, 2 * R
    if R != 2 or T != 2 or n % 4 or tok % 32 or HB % (128 * G) or db % 128:
        return None
    hw = HB // G
    C = tile_of(hw // 128, CHUNKS)
    hc = hw // C
    rows = 8 * tok
    V, S = pltpu.VMEM, pltpu.SemaphoreType.DMA
    data = [
        ((rows, D), BF16), ((rows, D), BF16), ((D, rows), BF16),
        ((C, D, hc), BF16), ((C, hc, D), BF16),
        ((C, rows, hc), F32), ((C, rows, hc), BF16), ((C, hc, rows), BF16),
        ((2, 4, tok, D), BF16), ((4, tok, D), BF16), ((4, tok, D), BF16),
        ((2, tok, D), BF16), ((tok, D), BF16), ((tok, D), BF16),
        ((tok, D), BF16),
        ((2, Z - 1, C, 2, db, hc), BF16), ((2, Z - 1, C, 2, hc, db), BF16),
        ((2, Z - 1, C, 2, db, hc), BF16), ((2, Z - 1, C, 2, hc, db), BF16),
        ((C, 2, db, hc), BF16), ((C, 2, hc, db), BF16),
        ((C, db, hc), BF16), ((C, hc, db), BF16), ((C, db, hc), BF16), ((C, hc, db), BF16),
    ]
    size = sum(math.prod(s) * jnp.dtype(d).itemsize for s, d in data)
    if size > 50 * 2**20 or 4 * hw % n or (Z - 1) * 4 * hw > 8 * tok * n:
        return None
    sems = [
        (C, 2), (C, 2, Z - 1, 2, 2), (4 + 3 * Z,), (2 + 3 * Z,), (5 + 3 * Z,),
        (2, Z - 1, C, 2, 2), (C, 2), (C, 2, 2), (7,),
    ]
    scratch = [V(s, d) for s, d in data] + [S((9,))] + [S(s) for s in sems]
    scratch += [S((4 * C + 2,)), S((4 * C + 1,))]
    return functools.partial(plane_kernel, Z), scratch, (1, HB), pl.ANY


def shards(inputs, cotangent, up_weight, down_weight):
    R, n, T = axis_sizes()
    tok, D = inputs.shape
    db = up_weight.shape[0]
    chosen = plane_call(inputs, up_weight) or ring_call(inputs, up_weight)
    body, scratch, (parts, hb), space = chosen
    spec = pl.BlockSpec(memory_space=space)
    ig, gu, gd = pl.pallas_call(
        body,
        out_shape=(
            jax.ShapeDtypeStruct((tok, D), BF16),
            jax.ShapeDtypeStruct((db, parts * hb), BF16),
            jax.ShapeDtypeStruct((parts * hb, db), BF16),
        ),
        in_specs=[spec] * 4,
        out_specs=(spec,) * 3,
        scratch_shapes=scratch,
        compiler_params=pltpu.CompilerParams(
            collective_id=0, has_side_effects=True, vmem_limit_bytes=60 * 2**20
        ),
    )(inputs, cotangent, up_weight, down_weight)
    total_tokens = tok * R * n * T
    loss_scale = 1.0 / math.sqrt(total_tokens)
    if space is pl.ANY:
        return finals_call(ig, gu, gd, loss_scale)
    return ig, gu.astype(F32) * loss_scale, gd.astype(F32) * loss_scale


def solution(mesh):
    token, up, down = P(("rep", "fs", "tp"), None), P("fs", "tp"), P("tp", "fs")
    return jax.shard_map(
        shards,
        mesh=mesh,
        in_specs=(token, token, up, down),
        out_specs=(token, up, down),
        check_vma=False,
    )
```

```python
import functools
import math

import jax
import jax.numpy as jnp
from jax import lax
from jax.experimental import pallas as pl
from jax.experimental.pallas import tpu as pltpu
from jax.sharding import PartitionSpec as P

MESH = pl.DeviceIdType.MESH
CHUNKS = 2
PARTS = 4
BF16, F32 = jnp.bfloat16, jnp.float32
NT = (((1,), (1,)), ((), ()))


def ring_place(f, n):
    odd = lax.rem(f, 2)
    half = lax.div(f, 2)
    return half * (1 - odd) + (n - 1 - half) * odd


def ring_member(p, n):
    back = lax.div(p, (n + 1) // 2)
    return 2 * p * (1 - back) + (2 * n - 1 - 2 * p) * back


def tile_of(size, most):
    while size % most:
        most //= 2
    return most


def ring_kernel(
    R, n, T,
    x_ref, c_ref, u_ref, d_ref,
    ig_ref, gu_ref, gd_ref,
    xg, cg, xt, ug, dg, pre, agr, pg, at,
    igp, itr, isum, irr, us, ur, ds_, dr_, fu, fd, fur, fdr,
    ag_ss, ag_rs, rs_ss, rs_rs, tr_ss, tr_rs, tt_ss, tt_rs,
    it_ss, it_rs, ir_ss, ir_rs, f_ss, f_rs,
):
    r, f, t = lax.axis_index("rep"), lax.axis_index("fs"), lax.axis_index("tp")
    tok, db = x_ref.shape[0], u_ref.shape[0]
    C, w = pre.shape[0], pre.shape[2]
    hb = C * w
    rows = R * T * tok

    def hidden(place, ch):
        return pl.ds(pl.multiple_of(place * hb + ch * w, w), w)

    for ref, full in ((x_ref, xg), (c_ref, cg)):
        for q in range(n):
            full[q, 0:tok, :] = ref[:, q * db:(q + 1) * db]
    p = ring_place(f, n)

    def member(q):
        return ring_member(lax.rem(p + q + n, n), n)

    def ring_dev(sign):
        return (r, member(sign), t)

    def rep_dev(q):
        return (lax.rem(r + q + R, R), f, t)

    def tp_dev(q):
        return (r, f, lax.rem(t + q + T, T))

    barrier = pltpu.get_barrier_semaphore()
    peers = [ring_dev(1), ring_dev(-1)]
    peers += [rep_dev(q) for q in range(1, R)] + [tp_dev(q) for q in range(1, T)]
    for peer in peers:
        pl.semaphore_signal(barrier, inc=1, device_id=peer, device_id_type=MESH)
    pl.semaphore_wait(barrier, len(peers))

    def remote(src, dst, ssem, rsem, dev):
        return pltpu.make_async_remote_copy(
            src_ref=src, dst_ref=dst, send_sem=ssem, recv_sem=rsem,
            device_id=dev, device_id_type=MESH,
        )

    long, short = n // 2, (n - 1) // 2
    streams = [(0, 1, long), (0, -1, short), (1, 1, short), (1, -1, long)]
    hops = max(long, short)
    def own(g, ch):
        return u_ref.at[:, hidden(r, ch)] if g == 0 else d_ref.at[hidden(r, ch), :]

    held = (ug, dg)

    def slot(sign, s):
        return (n - s if sign > 0 else s) - 1

    def gather_copy(ch, i, s):
        g, sign, _ = streams[i]
        src = own(g, ch) if s == 1 else held[g].at[slot(sign, s - 1), ch]
        return remote(
            src, held[g].at[slot(sign, s), ch],
            ag_ss.at[ch, i, s - 1], ag_rs.at[ch, i, s - 1], ring_dev(sign),
        )

    sends = []

    def go(copy):
        copy.start()
        sends.append(copy)
        return copy

    flying = {}

    def gather_first(ch):
        for i, (g, sign, k) in enumerate(streams):
            if k >= 1:
                flying[ch, i, 1] = go(gather_copy(ch, i, 1))

    gather_first(0)

    tokens = tuple((full.at[:, 0:tok, :], full) for full in (xg, cg))

    def span(dt, dr):
        return pl.ds((dt * R + dr) * tok, tok)

    rep_copies = {}
    for dr in range(1, R):
        for j, (ref, full) in enumerate(tokens):
            rep_copies[j, dr] = go(remote(
                ref, full.at[:, span(0, dr), :], tr_ss.at[j, dr], tr_rs.at[j, dr], rep_dev(-dr)
            ))
    tp_copies = {}
    for dt in range(1, T):
        for j, (ref, full) in enumerate(tokens):
            tp_copies[j, dt, 0] = go(remote(
                ref, full.at[:, span(dt, 0), :], tt_ss.at[j, dt, 0], tt_rs.at[j, dt, 0],
                tp_dev(-dt),
            ))

    row_tile = tile_of(rows, 256)

    def gather_dot(ch, g, block, q, first=False):
        b = member(q)
        out, full = ((pre, xg), (agr, cg))[g]

        @pl.loop(0, rows // row_tile)
        def _(i):
            part = pl.ds(pl.multiple_of(i * row_tile, row_tile), row_tile)
            lhs = full[b, part, :]
            if g == 0:
                val = jnp.dot(lhs, block[...], preferred_element_type=F32)
            else:
                val = lax.dot_general(lhs, block[...], NT, preferred_element_type=F32)
            if first:
                out[ch, part, :] = val
            else:
                out[ch, part, :] += val

    def finish_tokens():
        for dr in range(1, R):
            for j, (ref, full) in enumerate(tokens):
                rep_copies[j, dr].wait_recv()
                for dt in range(1, T):
                    tp_copies[j, dt, dr] = go(remote(
                        full.at[:, span(0, dr), :], full.at[:, span(dt, dr), :],
                        tt_ss.at[j, dt, dr], tt_rs.at[j, dt, dr], tp_dev(-dt),
                    ))
        for copy in tp_copies.values():
            copy.wait_recv()

        @pl.loop(0, n)
        def _(b):
            xt[b] = xg[b].T

        for ch in range(C):
            gather_dot(ch, 0, own(0, ch), 0, True)
            gather_dot(ch, 1, own(1, ch), 0, True)

    act_tile = tile_of(rows, 128)

    def activate(ch):
        @pl.loop(0, rows // act_tile)
        def _(i):
            part = pl.ds(pl.multiple_of(i * act_tile, act_tile), act_tile)
            active = jnp.maximum(pre[ch, part, :], 0.0)
            pg[ch, part, :] = (2.0 * active * agr[ch, part, :]).astype(BF16)
            at[ch, :, part] = (active * active).astype(BF16).T

    def gather(ch, before_last):
        for s in range(1, hops + 1):
            if s == hops:
                before_last()
            for i, (g, sign, k) in enumerate(streams):
                if s <= k:
                    flying[ch, i, s].wait_recv()
                    if s < k:
                        flying[ch, i, s + 1] = go(gather_copy(ch, i, s + 1))
            if s == 1 and ch == 0:
                finish_tokens()
            for i, (g, sign, k) in enumerate(streams):
                if s <= k:
                    gather_dot(ch, g, held[g].at[slot(sign, s), ch], -sign * s)
        if hops == 0:
            if ch == 0:
                finish_tokens()
            before_last()
        activate(ch)

    def grad_block(ch, g, q, dst, arrived):
        b = member(q)
        height = (db, w)[g]
        tile = tile_of(height, 256)

        @pl.loop(0, height // tile)
        def _(i):
            part = pl.ds(pl.multiple_of(i * tile, tile), tile)
            if g == 0:
                val = jnp.dot(xt[b, part, :], pg[ch], preferred_element_type=F32)
            else:
                val = jnp.dot(at[ch, part, :], cg[b], preferred_element_type=F32)
            for a in arrived:
                val = val + a[part, :].astype(F32)
            dst[part, :] = val.astype(BF16)

    rs_send, rs_recv = (us, ds_), (ur, dr_)

    def rs_index(i, s):
        g, sign, _ = streams[i]
        return s - 1 if sign > 0 else (long, short)[g] + s - 1

    reducing = {}

    def reduce_step(ch, i, s):
        g, sign, k = streams[i]
        arrived = []
        if s > 1:
            reducing[ch, i, s - 1].wait_recv()
            arrived = [rs_recv[g].at[rs_index(i, s - 1), ch]]
        mine = rs_send[g].at[rs_index(i, s), ch]
        grad_block(ch, g, sign * (k - s + 1), mine, arrived)
        reducing[ch, i, s] = go(remote(
            mine, rs_recv[g].at[rs_index(i, s), ch],
            rs_ss.at[ch, i, s - 1], rs_rs.at[ch, i, s - 1], ring_dev(sign),
        ))

    def reduce_all(ch, s):
        for i, (g, sign, k) in enumerate(streams):
            if s <= k:
                reduce_step(ch, i, s)

    for ch in range(C):
        if ch + 1 < C:
            gather(ch, functools.partial(gather_first, ch + 1))
        elif C > 1:
            gather(ch, functools.partial(reduce_all, 0, 1))
        else:
            gather(ch, lambda: None)
            reduce_all(ch, 1)

    for q in range(n):
        b = member(q)

        @pl.loop(0, rows // row_tile)
        def _(i):
            part = pl.ds(pl.multiple_of(i * row_tile, row_tile), row_tile)
            val = 0.0
            for ch in range(C):
                block = own(0, ch) if q == 0 else ug.at[q - 1, ch]
                val = val + lax.dot_general(
                    pg[ch, part, :], block[...], NT, preferred_element_type=F32
                )
            igp[b, part, :] = val.astype(BF16)

    wide = R * tok
    it_copies = [
        go(remote(
            igp.at[:, pl.ds(dt * wide, wide), :], itr.at[dt - 1],
            it_ss.at[dt], it_rs.at[dt], tp_dev(dt),
        ))
        for dt in range(1, T)
    ]
    ir_copies = []

    def finish_tp():
        for copy in it_copies:
            copy.wait_recv()

        @pl.loop(0, n)
        def _(b):
            for dr in range(R):
                part = pl.ds(dr * tok, tok)
                val = igp[b, part, :].astype(F32)
                for dt in range(1, T):
                    val = val + itr[dt - 1, b, part, :].astype(F32)
                isum[dr, b] = val.astype(BF16)

        for dr in range(1, R):
            ir_copies.append(go(remote(
                isum.at[dr], irr.at[dr - 1], ir_ss.at[dr], ir_rs.at[dr], rep_dev(dr)
            )))

    def finish_rep():
        for copy in ir_copies:
            copy.wait_recv()

        for b in range(n):
            val = isum[0, b].astype(F32)
            for dr in range(1, R):
                val = val + irr[dr - 1, b].astype(F32)
            ig_ref[:, b * db:(b + 1) * db] = val.astype(BF16)

    finish_tp()

    finals = ((fu, fur, gu_ref), (fd, fdr, gd_ref))
    fin_copies = {}

    def put(g, place, ch, val):
        if g == 0:
            gu_ref[:, hidden(place, ch)] = val
        else:
            gd_ref[hidden(place, ch), :] = val

    def finish(ch, g):
        mine, theirs, out = finals[g]
        arrived = []
        for i, (h, sign, k) in enumerate(streams):
            if h == g and k >= 1:
                reducing[ch, i, k].wait_recv()
                arrived.append(rs_recv[g].at[rs_index(i, k), ch])
        grad_block(ch, g, 0, mine.at[ch], arrived)
        for dr in range(1, R):
            fin_copies[ch, g, dr] = go(remote(
                mine.at[ch], theirs.at[dr - 1, ch],
                f_ss.at[ch, g, dr], f_rs.at[ch, g, dr], rep_dev(-dr),
            ))
        put(g, r, ch, mine[ch])

    for ch in range(C):
        for s in range(2, hops + 1):
            reduce_all(ch, s)
            if ch == 0 and s == 2:
                finish_rep()
        if ch == 0 and hops < 2:
            finish_rep()
        if ch + 1 < C:
            reduce_all(ch + 1, 1)
        for g in range(2):
            finish(ch, g)
    for (ch, g, dr), copy in fin_copies.items():
        _, theirs, out = finals[g]
        copy.wait_recv()
        put(g, lax.rem(r + dr, R), ch, theirs[dr - 1, ch])
    for copy in sends:
        copy.wait_send()


def plane_kernel(
    Z,
    x_ref, c_ref, u_ref, d_ref,
    ig_ref, gu_ref, gd_ref,
    xg, cg, xt, ug, dg, pre, pg, at,
    igp, itr, isum, igot, ipt, ift, igo, su, sd, ru, rd, fu, fd, uo, do, yu, yd,
    out_s, yw_r, zg_r, tx_r, ty_r, tt_r, rs_r, fy_r, fx_r, ig_r, ld_s, st_s,
):
    r, f, t = lax.axis_index("rep"), lax.axis_index("fs"), lax.axis_index("tp")
    z, y = lax.div(f, 2), lax.rem(f, 2)
    tok, D = x_ref.shape
    db = u_ref.shape[0]
    C, hc = pg.shape[0], pg.shape[2]
    hw, half, wide = C * hc, tok // 2, 2 * tok
    n = 2 * Z
    xdev, ydev, tdev = (1 - r, f, t), (r, f + 1 - 2 * y, t), (r, f, 1 - t)

    def zdev(s):
        return (r, f + 2 * s, t)

    low = z < Z // 2
    m = jnp.where(low, z, Z - 1 - z)
    near = (jnp.where(low, 0, 1), jnp.where(low, 1, -1))
    far = (1 - near[0], -near[1])

    ahead = {1: z < Z - 1, -1: z > 0}

    def remote(src, dst, ssem, rsem, dev):
        return pltpu.make_async_remote_copy(
            src_ref=src, dst_ref=dst, send_sem=ssem, recv_sem=rsem,
            device_id=dev, device_id_type=MESH,
        )

    def go(make):
        make().start()

    def span(at_, size):
        return pl.ds(pl.multiple_of(at_, size), size)

    def blk(b):
        return span(b * db, db)

    def hid(q, ch):
        return span(q * hw + ch * hc, hc)

    mine, other = 2 * r + y, 2 * r + 1 - y

    def held(g, ch, b):
        return ug.at[ch, blk(b), :] if g == 0 else dg.at[ch, :, blk(b)]

    spare = (uo, do)
    weights = (u_ref, d_ref)

    def strip(g, ref, q, ch):
        return ref.at[:, hid(q, ch)] if g == 0 else ref.at[hid(q, ch), :]

    own_x, own_c = xg.at[pl.ds(0, tok), :], cg.at[pl.ds(0, tok), :]
    loads = {}
    for ch in range(C):
        for g in range(2):
            loads["other", ch, g] = (strip(g, weights[g], other, ch), spare[g].at[ch])
            loads["mine", ch, g] = (strip(g, weights[g], mine, ch), held(g, ch, f))
        if ch == 0:
            loads["x"] = (x_ref, own_x)
            loads["c"] = (c_ref, own_c)
    loads = {
        key: pltpu.make_async_copy(src, dst, ld_s.at[i])
        for i, (key, (src, dst)) in enumerate(loads.items())
    }
    for copy in loads.values():
        copy.start()

    barrier = pltpu.get_barrier_semaphore()

    def greet(dev):
        pl.semaphore_signal(barrier, inc=1, device_id=dev, device_id_type=MESH)

    for dev in (xdev, ydev, tdev):
        greet(dev)
    for s in (1, -1):
        pl.when(ahead[s])(functools.partial(greet, zdev(s)))
    pl.semaphore_wait(barrier, 3 + sum(jnp.where(ahead[s], 1, 0) for s in (1, -1)))

    def swap(ch, g):
        return remote(spare[g].at[ch], held(g, ch, f), out_s.at[0], yw_r.at[ch, g], ydev)

    def origin(s, k, e):
        return f - 2 * s * k + e * (1 - 2 * y)

    def pass_on(ch, g, s, k, e):
        block = held(g, ch, origin(s, k, e))
        i = (ch, (1 - s) // 2, k, e, g)
        return remote(block, block, out_s.at[i[1] + 1], zg_r.at[i], zdev(s))

    def landed(ch, g, s, k, e):
        block = held(g, ch, origin(s, k, e))
        i = (ch, (1 - s) // 2, k - 1, e, g)
        return remote(block, block, out_s.at[i[1] + 1], zg_r.at[i], zdev(s))

    def begin(ch, g, e, also=None):
        for s in (1, -1):
            cond = ahead[s] if also is None else ahead[s] & also
            pl.when(cond)(functools.partial(
                go, functools.partial(pass_on, ch, g, s, 0, e)))

    level = [m == m0 for m0 in range(Z // 2)]
    reached = {}
    for k in range(1, Z):
        reached[1, k], reached[-1, k] = z >= k, z < Z - k
    passing = {key: reached[key] & ahead[key[0]] for key in reached}

    outward = {1: low, -1: jnp.logical_not(low)}
    split = {}
    for (s, k), cond in passing.items():
        split[s, k, 0] = cond & outward[s]
        split[s, k, 1] = cond & outward[-s]

    def relay(ch, g, k, es=(0, 1), toward=None):
        for e in es:
            for s in (1, -1):
                cond = passing[s, k] if toward is None else split[s, k, toward]

                @pl.when(cond)
                def _():
                    landed(ch, g, s, k, e).wait_recv()
                    go(functools.partial(pass_on, ch, g, s, k, e))

    def collect(ch, g):
        for k in range(1, Z):
            for e in range(2):
                for s in (1, -1):

                    @pl.when(reached[s, k] & jnp.logical_not(ahead[s]))
                    def _():
                        landed(ch, g, s, k, e).wait_recv()

    def swapped(ch, g, also=None):
        begin(ch, g, 1, also)

    def rows(k, dt, part=(0, 2)):
        lo, hi = part
        return pl.ds((2 * k + dt) * tok + lo * half, (hi - lo) * half)

    def quarter(i):
        return span(jnp.where(low, Z - 1 - i, i) * 2 * db, 2 * db)

    A, B, AB = (0, 1), (1, 2), (0, 2)

    def hop(sems, i, dev, full, src, dst, cols):
        def make():
            where = slice(None) if cols is None else quarter(cols)
            return remote(
                full.at[rows(*src), where], full.at[rows(*dst), where],
                sems[0], sems[1].at[i], dev,
            )

        return make

    X, Y, S = (out_s.at[3], tx_r), (out_s.at[4], ty_r), (out_s.at[5], tt_r)
    moves = {}
    for i, part in enumerate((A, B)):
        moves["x", "x", i] = hop(X, i, xdev, xg, (0, 0, part), (1, 0, part), None)
        moves["y", "x", i] = hop(Y, i, ydev, xg, (0, 0, part), (2, 0, part), None)
        moves["d", "x", i] = hop(X, 2 + i, xdev, xg, (2, 0, part), (3, 0, part), None)
    moves["s", "x", 0] = hop(S, 0, tdev, xg, (0, 0, AB), (0, 1, AB), None)
    moves["s", "c", 0] = hop(S, 1, tdev, cg, (0, 0, AB), (0, 1, AB), None)
    for k in range(1, 4):
        moves["s", "x", k] = hop(S, 1 + k, tdev, xg, (k, 0, AB), (k, 1, AB), None)
    for i in range(Z):
        for p, (xp, yp) in enumerate(((B, A), (A, B))):
            moves["x%d" % p, "c", i] = hop(X, 4 + 3 * i + p, xdev, cg, (0, 0, xp), (1, 0, xp), i)
            moves["y%d" % p, "c", i] = hop(Y, 2 + 3 * i + p, ydev, cg, (0, 0, yp), (2, 0, yp), i)
        moves["dx", "c", i] = hop(X, 6 + 3 * i, xdev, cg, (2, 0, A), (3, 0, A), i)
        moves["dy", "c", i] = hop(Y, 4 + 3 * i, ydev, cg, (1, 0, B), (3, 0, B), i)
        for k in range(1, 4):
            moves["s%d" % k, "c", i] = hop(
                S, 5 + (k - 1) * Z + i, tdev, cg, (k, 0, AB), (k, 1, AB), i)

    def start(*key):
        go(moves[key])

    def arrive(*key):
        moves[key]().wait_recv()

    def flip(k):
        part = pl.ds(k * wide, wide)

        @pl.loop(0, n)
        def _(b):
            xt[blk(b), part] = xg[part, blk(b)].T

    def forward(ch, first, last):
        @pl.loop(first, last, unroll=2 if (last - first) % 2 == 0 else 1)
        def _(k):
            part = span(k * wide, wide)
            active = jnp.maximum(
                jnp.dot(xg[part, :], ug[ch], preferred_element_type=F32), 0.0)
            pre[ch, part, :] = active
            at[ch, :, part] = (active * active).astype(BF16).T

    def backward(ch):
        @pl.loop(0, 4, unroll=2)
        def _(k):
            part = span(k * wide, wide)
            val = lax.dot_general(cg[part, :], dg[ch], NT, preferred_element_type=F32)
            pg[ch, part, :] = (2.0 * pre[ch, part, :] * val).astype(BF16)

    def grad(ch, g, b):
        if g == 0:
            return jnp.dot(xt[blk(b), :], pg[ch], preferred_element_type=F32)
        return jnp.dot(at[ch], cg[:, blk(b)], preferred_element_type=F32)

    out_buf, in_buf, fin = (su, sd), (ru, rd), (fu, fd)

    def partial_copy(ch, g, way, j, e):
        d, s = way
        return remote(
            out_buf[g].at[d, j, ch, e], in_buf[g].at[d, j, ch, e],
            out_s.at[6], rs_r.at[d, j, ch, g, e], zdev(s))

    def side_of(e):
        return e * y + (1 - e) * (1 - y)

    def reduce(ch, g, way, j, m0, es=None):
        cond = level[m0]
        to = jnp.where(way[1] > 0, Z - 1 - j, j)
        more = m0 > 0 or way is far

        def step(e):
            val = grad(ch, g, 2 * to + side_of(e))
            if more:
                partial_copy(ch, g, way, j, e).wait_recv()
                val = val + in_buf[g][way[0], j, ch, e].astype(F32)
            out_buf[g][way[0], j, ch, e] = val.astype(BF16)
            partial_copy(ch, g, way, j, e).start()

        if es is None:
            pl.loop(0, 2)(step)
        else:
            for e in es:
                step(e)

    outs, passed = (gu_ref, gd_ref), (yu, yd)

    def store(ch, g, e):
        if ch == C:
            return pltpu.make_async_copy(igo, ig_ref, st_s.at[1])
        src = passed[g].at[ch] if e else fin[g].at[ch, 1]
        dst = strip(g, outs[g], other if e else mine, ch)
        return pltpu.make_async_copy(src, dst, st_s.at[0])

    def final_y(ch, g):
        return remote(
            fin[g].at[ch, 0], passed[g].at[ch], out_s.at[7], fy_r.at[ch, g], ydev)

    def final_x(ch, g, e):
        src = passed[g].at[ch] if e else fin[g].at[ch, 1]
        return remote(
            src, strip(g, outs[g], other if e else mine, ch), out_s.at[7], fx_r.at[0], xdev)

    def finish(ch, g, m0, between=None):
        cond = level[m0]
        ways = [(far, m0)] + ([(near, Z - 1 - m0)] if m0 else [])
        for e in range(2):
            val = grad(ch, g, 2 * z + side_of(e))
            for way, j in ways:
                partial_copy(ch, g, way, j, e).wait_recv()
                val = val + in_buf[g][way[0], j, ch, e].astype(F32)
            fin[g][ch, e] = val.astype(BF16)
            if e == 0:
                go(functools.partial(final_y, ch, g))
                if between:
                    between()
            else:
                go(functools.partial(final_x, ch, g, 0))
        store(ch, g, 0).start()

    def spread(ch, g, m0):
        final_y(ch, g).wait_recv()
        go(functools.partial(final_x, ch, g, 1))
        store(ch, g, 1).start()

    def cols(p):
        return pl.ds(p * (D // 2), D // 2)

    def ig_copy(i):
        part = cols((i + 1) % 2)
        if i > 6:
            part = cols(i - 7)
            src, dst = igp.at[1, :, :, part], itr.at[:, :, part]
            return remote(src, dst, out_s.at[8], ig_r.at[i - 1], tdev)
        kind = (i - 1) // 2
        if kind < 2:
            src, dst = isum.at[3 - kind, :, part], igot.at[1 - kind, :, part]
        else:
            src, dst = ipt.at[:, part], ift.at[:, part]
        return remote(src, dst, out_s.at[8], ig_r.at[i - 1], ydev if kind < 2 else xdev)

    def ig_go(i):
        go(functools.partial(ig_copy, i))

    def ig_part(dt, p):
        @pl.loop(p * (n // 2), (p + 1) * (n // 2), unroll=n // 2)
        def _(b):
            val = 0.0
            for ch in range(C):
                lhs = jnp.concatenate([pg[ch, rows(k, dt), :] for k in range(4)], 0)
                val = val + lax.dot_general(
                    lhs, ug[ch, blk(b), :], NT, preferred_element_type=F32)
            val = val.astype(BF16)
            for k in range(4):
                igp[dt, k, :, blk(b)] = val[k * tok:(k + 1) * tok]

        if dt:
            ig_go(7 + p)

    def ig_first(p):
        ig_copy(7 + p).wait_recv()

        @pl.loop(0, 4)
        def _(k):
            val = igp[0, k, :, cols(p)].astype(F32) + itr[k, :, cols(p)].astype(F32)
            isum[k, :, cols(p)] = val.astype(BF16)

    def ig_diag(p):
        ig_go(1 + p)

    def ig_more(p):
        ig_go(3 + p)

    def ig_second(p):
        ig_copy(1 + p).wait_recv()
        val = isum[1, :, cols(p)].astype(F32) + igot[1, :, cols(p)].astype(F32)
        ipt[:, cols(p)] = val.astype(BF16)
        ig_go(5 + p)

    def ig_last():
        for i in range(3, 7):
            ig_copy(i).wait_recv()
        val = isum[0].astype(F32) + igot[0].astype(F32) + ift[...].astype(F32)
        igo[...] = val.astype(BF16)
        store(C, 0, 0).start()

    edge, inner = level[0], m > 0
    last = C - 1

    units = [(ch, g) for ch in range(C) for g in range(2)]

    loads["other", 0, 0].wait()
    go(functools.partial(swap, 0, 0))
    loads["mine", 0, 0].wait()
    begin(0, 0, 0)
    loads["x"].wait()
    for i in range(2):
        start("x", "x", i)
        start("y", "x", i)
    loads["mine", 0, 1].wait()
    begin(0, 1, 0)
    start("s", "x", 0)
    loads["c"].wait()
    start("s", "c", 0)
    for unit in units[1:]:
        loads[("other",) + unit].wait()
        go(functools.partial(swap, *unit))
        if unit != units[1]:
            loads[("mine",) + unit].wait()

    swap(0, 0).wait_recv()
    begin(0, 0, 1)
    for unit in units[2:]:
        begin(*unit, 0, edge)
    relay(0, 0, 1)
    arrive("s", "x", 0)
    arrive("s", "c", 0)
    flip(0)
    arrive("y", "x", 0)
    start("d", "x", 0)
    for k in range(2, Z - 1):
        relay(0, 0, k)
    for unit in units[2:3]:
        begin(*unit, 0, inner)
    for i in range(2):
        arrive("x", "x", i)
    start("s", "x", 1)
    arrive("y", "x", 1)
    start("d", "x", 1)

    def offer(i):
        for way in ("x0", "y0", "x1", "y1"):
            start(way, "c", i)

    offer(0)
    start("s", "x", 2)
    swap(0, 1).wait_recv()
    begin(0, 1, 1)
    relay(0, 1, 1, (0,))
    arrive("s", "x", 1)
    flip(1)
    for k in range(2, Z - 1):
        relay(0, 1, k, (0,))
    relay(0, 1, 1, (1,))
    arrive("s", "x", 2)
    flip(2)
    collect(0, 0)
    forward(0, 0, 3)
    for unit in units[2:]:
        swap(*unit).wait_recv()
        begin(*unit, 1, edge)
    for i in range(2):
        arrive("d", "x", i)
    start("s", "x", 3)

    def ready(i):
        for k in range(1, 4):
            arrive("s%d" % k, "c", i)
        if i < Z - 1:
            pl.when(edge)(functools.partial(reduce, 0, 1, near, i, 0))

    tasks = [(unit, k) for unit in units[2:] for k in range(1, Z - 1)]
    for i in range(Z):
        arrive("x0", "c", i)
        start("dy", "c", i)
        arrive("y0", "c", i)
        start("dx", "c", i)
        if i + 1 < Z:
            offer(i + 1)
        if i == 0:
            for k in range(2, Z - 1):
                relay(0, 1, k, (1,))
            for unit in units[2:]:
                if unit != units[2]:
                    begin(*unit, 0, inner)
                begin(*unit, 1, inner)
            for unit in units[2:]:
                for k in range(1, Z // 2):
                    relay(*unit, k, toward=0)
            arrive("s", "x", 3)
            flip(3)
            forward(0, 3, 4)
        else:
            if i > 1:
                ready(i - 1)
            if i == Z - 1:
                for m0 in range(1, Z // 2):
                    pl.when(level[m0])(functools.partial(reduce, 0, 1, near, 0, m0))
        arrive("x1", "c", i)
        start("s1", "c", i)
        arrive("y1", "c", i)
        start("s2", "c", i)
        arrive("dy", "c", i)
        arrive("dx", "c", i)
        start("s3", "c", i)
        if i == 0:
            ready(0)
        if i == 1 and tasks:
            unit, k = tasks.pop(0)
            relay(*unit, k, toward=1)
    if Z > 1:
        ready(Z - 1)

    def edges():
        collect(0, 1)
        backward(0)
        for j in range(Z - 1):
            reduce(0, 0, near, j, 0)
        for ch in range(1, C):
            collect(ch, 0)
            forward(ch, 0, 4)
            for j in range(Z - 1):
                reduce(ch, 1, near, j, 0)
            collect(ch, 1)
            backward(ch)
            if ch < C - 1:
                for j in range(Z - 1):
                    reduce(ch, 0, near, j, 0)
        ig_part(1, 0)
        ig_part(1, 1)

        def meanwhile():
            ig_part(0, 0)
            ig_first(0)
            ig_diag(0)
            ig_part(0, 1)

        finish(0, 1, 0, meanwhile)
        ig_first(1)
        if C > 1:
            for j in range(Z - 1):
                reduce(C - 1, 0, near, j, 0)
        ig_diag(1)
        spread(0, 1, 0)
        finish(0, 0, 0)
        ig_second(0)
        for ch in range(1, C):
            finish(ch, 1, 0)
            spread(ch - 1, 0, 0)
            if ch == 1:
                ig_more(0)
                ig_second(1)
            spread(ch, 1, 0)
            finish(ch, 0, 0)
            if ch == 1:
                ig_more(1)
        if C == 1:
            ig_more(0)
            ig_second(1)
            ig_more(1)
        spread(C - 1, 0, 0)
        ig_last()

    def inside(m0):
        left = list(tasks)

        def relays(count):
            for _ in range(min(count, len(left))):
                unit, k = left.pop(0)
                relay(*unit, k, toward=1)

        def nears(ch, g, js):
            for j in js:
                reduce(ch, g, near, j, m0)

        def fars(ch, g):
            for j in range(m0):
                reduce(ch, g, far, j, m0)

        def both(ch, g):
            for e in range(2):
                for j in range(m0):
                    reduce(ch, g, far, j, m0, (e,))
                for j in rest:
                    reduce(ch, g, near, j, m0, (e,))

        first, rest = range(1), range(1, Z - 1 - m0)
        keep = (Z - 2) * (C > 1)
        relays(len(left) - keep)
        nears(0, 1, rest)
        relays(keep - 1)
        backward(0)
        for ch in range(1, C):
            forward(ch, 0, 4)
        relays(1)
        fars(0, 1)
        for ch in range(1, C):
            backward(ch)
        nears(0, 0, first)
        finish(0, 1, m0)
        both(0, 0)
        spread(0, 1, m0)
        for dt in (1, 0):
            for p in range(2):
                ig_part(dt, p)
        finish(0, 0, m0)
        for ch in range(1, C):
            nears(ch, 1, first)
            if ch == 1:
                for p in range(2):
                    ig_first(p)
                    ig_diag(p)
            spread(ch - 1, 0, m0)
            both(ch, 1)
            if ch == 1:
                ig_second(0)
            finish(ch, 1, m0)
            nears(ch, 0, first)
            if ch == 1:
                ig_more(0)
                ig_second(1)
                ig_more(1)
            both(ch, 0)
            spread(ch, 1, m0)
            finish(ch, 0, m0)
        if C == 1:
            for p in range(2):
                ig_first(p)
                ig_diag(p)
                ig_more(p)
            for p in range(2):
                ig_second(p)
        spread(C - 1, 0, m0)
        ig_last()

    pl.when(edge)(edges)
    for m0 in range(1, Z // 2):
        pl.when(level[m0])(functools.partial(inside, m0))

    def settle():
        remote(gu_ref, gu_ref, out_s.at[7], fx_r.at[0], xdev).wait_recv()
        pltpu.make_async_copy(gu_ref, gu_ref, st_s.at[0]).wait()
        store(C, 0, 0).wait()

    def sent(i, count):
        some = xg.at[pl.ds(0, count), :]
        remote(some, some, out_s.at[i], out_s.at[i], xdev).wait_send()

    def drain():
        block = 4 * hw // n
        sent(0, block // 2)
        for z0 in range(Z - 1):
            pl.when(z == z0)(functools.partial(sent, 1, (z0 + 1) * block))
            pl.when(z == Z - 1 - z0)(functools.partial(sent, 2, (z0 + 1) * block))
        sent(3, 7 * half)
        sent(4, 5 * half)
        sent(5, 8 * tok)
        sent(6, (Z - 1) * block)
        sent(7, 3 * block // 2)
        sent(8, 7 * tok)

    settle()
    drain()


def ring_call(inputs, up_weight):
    R, n, T = axis_sizes()
    tok, D = inputs.shape
    db, hb = up_weight.shape[0], up_weight.shape[1] // R
    rows = R * T * tok
    C = tile_of(hb // 128, CHUNKS) if hb > 128 else 1
    w = hb // C
    V, S = pltpu.VMEM, pltpu.SemaphoreType.DMA
    hops = max(n // 2, 1)
    m = max(n - 1, 1)
    scratch = [
        V((n, rows, db), BF16), V((n, rows, db), BF16), V((n, db, rows), BF16),
        V((m, C, db, w), BF16), V((m, C, w, db), BF16),
        V((C, rows, w), F32), V((C, rows, w), F32), V((C, rows, w), BF16), V((C, w, rows), BF16),
        V((n, rows, db), BF16), V((max(T - 1, 1), n, R * tok, db), BF16),
        V((R, n, tok, db), BF16), V((max(R - 1, 1), n, tok, db), BF16),
        V((m, C, db, w), BF16), V((m, C, db, w), BF16),
        V((m, C, w, db), BF16), V((m, C, w, db), BF16),
        V((C, db, w), BF16), V((C, w, db), BF16),
        V((max(R - 1, 1), C, db, w), BF16), V((max(R - 1, 1), C, w, db), BF16),
        S((C, 4, hops)), S((C, 4, hops)), S((C, 4, hops)), S((C, 4, hops)),
        S((2, R)), S((2, R)), S((2, T, R)), S((2, T, R)),
        S((T,)), S((T,)), S((R,)), S((R,)), S((C, 2, R)), S((C, 2, R)),
    ]
    return functools.partial(ring_kernel, R, n, T), scratch, (R, hb), pltpu.VMEM


def finals_kernel(scale, *refs):
    sources, targets, raw, wide = refs[:3], refs[3:6], refs[6:9], refs[9:11]
    load, store = refs[11:]
    jobs = []
    for a in (1, 2, 0):
        rows = sources[a].shape[0]
        for p in range(PARTS):
            part = pl.ds(p * (rows // PARTS), rows // PARTS)
            jobs.append((a, p, part))
    loads, stores = [], []
    for a, p, part in jobs:
        copy = pltpu.make_async_copy(
            sources[a].at[part, :], raw[a].at[part, :], load.at[a, p])
        copy.start()
        loads.append(copy)
    for (a, p, part), copy in zip(jobs, loads):
        copy.wait()
        ready = raw[a]
        if a:
            ready = wide[a - 1]
            ready[part, :] = raw[a][part, :].astype(F32) * scale
        copy = pltpu.make_async_copy(
            ready.at[part, :], targets[a].at[part, :], store.at[a, p])
        copy.start()
        stores.append(copy)
    for copy in stores:
        copy.wait()


def finals_call(ig, gu, gd, scale):
    any_space = pl.BlockSpec(memory_space=pl.ANY)
    V, S = pltpu.VMEM, pltpu.SemaphoreType.DMA
    return pl.pallas_call(
        functools.partial(finals_kernel, scale),
        in_specs=[any_space] * 3,
        out_specs=(any_space,) * 3,
        out_shape=(
            jax.ShapeDtypeStruct(ig.shape, BF16),
            jax.ShapeDtypeStruct(gu.shape, F32),
            jax.ShapeDtypeStruct(gd.shape, F32),
        ),
        scratch_shapes=[
            V(ig.shape, BF16), V(gu.shape, BF16), V(gd.shape, BF16),
            V(gu.shape, F32), V(gd.shape, F32), S((3, PARTS)), S((3, PARTS)),
        ],
    )(ig, gu, gd)


def axis_sizes():
    return lax.axis_size("rep"), lax.axis_size("fs"), lax.axis_size("tp")


def plane_call(inputs, up_weight):
    R, n, T = axis_sizes()
    tok, D = inputs.shape
    db, HB = up_weight.shape
    Z, G = n // 2, 2 * R
    if R != 2 or T != 2 or n % 4 or tok % 32 or HB % (128 * G) or db % 128:
        return None
    hw = HB // G
    C = tile_of(hw // 128, CHUNKS)
    hc = hw // C
    rows = 8 * tok
    V, S = pltpu.VMEM, pltpu.SemaphoreType.DMA
    data = [
        ((rows, D), BF16), ((rows, D), BF16), ((D, rows), BF16),
        ((C, D, hc), BF16), ((C, hc, D), BF16),
        ((C, rows, hc), F32), ((C, rows, hc), BF16), ((C, hc, rows), BF16),
        ((2, 4, tok, D), BF16), ((4, tok, D), BF16), ((4, tok, D), BF16),
        ((2, tok, D), BF16), ((tok, D), BF16), ((tok, D), BF16),
        ((tok, D), BF16),
        ((2, Z - 1, C, 2, db, hc), BF16), ((2, Z - 1, C, 2, hc, db), BF16),
        ((2, Z - 1, C, 2, db, hc), BF16), ((2, Z - 1, C, 2, hc, db), BF16),
        ((C, 2, db, hc), BF16), ((C, 2, hc, db), BF16),
        ((C, db, hc), BF16), ((C, hc, db), BF16), ((C, db, hc), BF16), ((C, hc, db), BF16),
    ]
    size = sum(math.prod(s) * jnp.dtype(d).itemsize for s, d in data)
    if size > 50 * 2**20 or 4 * hw % n or (Z - 1) * 4 * hw > 8 * tok * n:
        return None
    sems = [
        (C, 2), (C, 2, Z - 1, 2, 2), (4 + 3 * Z,), (2 + 3 * Z,), (5 + 3 * Z,),
        (2, Z - 1, C, 2, 2), (C, 2), (1,), (8,),
    ]
    scratch = [V(s, d) for s, d in data] + [S((9,))] + [S(s) for s in sems]
    scratch += [S((4 * C + 2,)), S((2,))]
    return functools.partial(plane_kernel, Z), scratch, (1, HB), pl.ANY


def shards(inputs, cotangent, up_weight, down_weight):
    R, n, T = axis_sizes()
    tok, D = inputs.shape
    db = up_weight.shape[0]
    chosen = plane_call(inputs, up_weight) or ring_call(inputs, up_weight)
    body, scratch, (parts, hb), space = chosen
    spec = pl.BlockSpec(memory_space=space)
    ig, gu, gd = pl.pallas_call(
        body,
        out_shape=(
            jax.ShapeDtypeStruct((tok, D), BF16),
            jax.ShapeDtypeStruct((db, parts * hb), BF16),
            jax.ShapeDtypeStruct((parts * hb, db), BF16),
        ),
        in_specs=[spec] * 4,
        out_specs=(spec,) * 3,
        scratch_shapes=scratch,
        compiler_params=pltpu.CompilerParams(
            collective_id=0, has_side_effects=True, vmem_limit_bytes=60 * 2**20
        ),
    )(inputs, cotangent, up_weight, down_weight)
    total_tokens = tok * R * n * T
    loss_scale = 1.0 / math.sqrt(total_tokens)
    if space is pl.ANY:
        return finals_call(ig, gu, gd, loss_scale)
    return ig, gu.astype(F32) * loss_scale, gd.astype(F32) * loss_scale


def solution(mesh):
    token, up, down = P(("rep", "fs", "tp"), None), P("fs", "tp"), P("tp", "fs")
    return jax.shard_map(
        shards,
        mesh=mesh,
        in_specs=(token, token, up, down),
        out_specs=(token, up, down),
        check_vma=False,
    )
```

```python
import functools
import math

import jax
import jax.numpy as jnp
from jax import lax
from jax.experimental import pallas as pl
from jax.experimental.pallas import tpu as pltpu
from jax.sharding import PartitionSpec as P

MESH = pl.DeviceIdType.MESH
CHUNKS = 2
PARTS = 4
BF16, F32 = jnp.bfloat16, jnp.float32
NT = (((1,), (1,)), ((), ()))


def ring_place(f, n):
    odd = lax.rem(f, 2)
    half = lax.div(f, 2)
    return half * (1 - odd) + (n - 1 - half) * odd


def ring_member(p, n):
    back = lax.div(p, (n + 1) // 2)
    return 2 * p * (1 - back) + (2 * n - 1 - 2 * p) * back


def tile_of(size, most):
    while size % most:
        most //= 2
    return most


def ring_kernel(
    R, n, T,
    x_ref, c_ref, u_ref, d_ref,
    ig_ref, gu_ref, gd_ref,
    xg, cg, xt, ug, dg, pre, agr, pg, at,
    igp, itr, isum, irr, us, ur, ds_, dr_, fu, fd, fur, fdr,
    ag_ss, ag_rs, rs_ss, rs_rs, tr_ss, tr_rs, tt_ss, tt_rs,
    it_ss, it_rs, ir_ss, ir_rs, f_ss, f_rs,
):
    r, f, t = lax.axis_index("rep"), lax.axis_index("fs"), lax.axis_index("tp")
    tok, db = x_ref.shape[0], u_ref.shape[0]
    C, w = pre.shape[0], pre.shape[2]
    hb = C * w
    rows = R * T * tok

    def hidden(place, ch):
        return pl.ds(pl.multiple_of(place * hb + ch * w, w), w)

    for ref, full in ((x_ref, xg), (c_ref, cg)):
        for q in range(n):
            full[q, 0:tok, :] = ref[:, q * db:(q + 1) * db]
    p = ring_place(f, n)

    def member(q):
        return ring_member(lax.rem(p + q + n, n), n)

    def ring_dev(sign):
        return (r, member(sign), t)

    def rep_dev(q):
        return (lax.rem(r + q + R, R), f, t)

    def tp_dev(q):
        return (r, f, lax.rem(t + q + T, T))

    barrier = pltpu.get_barrier_semaphore()
    peers = [ring_dev(1), ring_dev(-1)]
    peers += [rep_dev(q) for q in range(1, R)] + [tp_dev(q) for q in range(1, T)]
    for peer in peers:
        pl.semaphore_signal(barrier, inc=1, device_id=peer, device_id_type=MESH)
    pl.semaphore_wait(barrier, len(peers))

    def remote(src, dst, ssem, rsem, dev):
        return pltpu.make_async_remote_copy(
            src_ref=src, dst_ref=dst, send_sem=ssem, recv_sem=rsem,
            device_id=dev, device_id_type=MESH,
        )

    long, short = n // 2, (n - 1) // 2
    streams = [(0, 1, long), (0, -1, short), (1, 1, short), (1, -1, long)]
    hops = max(long, short)
    def own(g, ch):
        return u_ref.at[:, hidden(r, ch)] if g == 0 else d_ref.at[hidden(r, ch), :]

    held = (ug, dg)

    def slot(sign, s):
        return (n - s if sign > 0 else s) - 1

    def gather_copy(ch, i, s):
        g, sign, _ = streams[i]
        src = own(g, ch) if s == 1 else held[g].at[slot(sign, s - 1), ch]
        return remote(
            src, held[g].at[slot(sign, s), ch],
            ag_ss.at[ch, i, s - 1], ag_rs.at[ch, i, s - 1], ring_dev(sign),
        )

    sends = []

    def go(copy):
        copy.start()
        sends.append(copy)
        return copy

    flying = {}

    def gather_first(ch):
        for i, (g, sign, k) in enumerate(streams):
            if k >= 1:
                flying[ch, i, 1] = go(gather_copy(ch, i, 1))

    gather_first(0)

    tokens = tuple((full.at[:, 0:tok, :], full) for full in (xg, cg))

    def span(dt, dr):
        return pl.ds((dt * R + dr) * tok, tok)

    rep_copies = {}
    for dr in range(1, R):
        for j, (ref, full) in enumerate(tokens):
            rep_copies[j, dr] = go(remote(
                ref, full.at[:, span(0, dr), :], tr_ss.at[j, dr], tr_rs.at[j, dr], rep_dev(-dr)
            ))
    tp_copies = {}
    for dt in range(1, T):
        for j, (ref, full) in enumerate(tokens):
            tp_copies[j, dt, 0] = go(remote(
                ref, full.at[:, span(dt, 0), :], tt_ss.at[j, dt, 0], tt_rs.at[j, dt, 0],
                tp_dev(-dt),
            ))

    row_tile = tile_of(rows, 256)

    def gather_dot(ch, g, block, q, first=False):
        b = member(q)
        out, full = ((pre, xg), (agr, cg))[g]

        @pl.loop(0, rows // row_tile)
        def _(i):
            part = pl.ds(pl.multiple_of(i * row_tile, row_tile), row_tile)
            lhs = full[b, part, :]
            if g == 0:
                val = jnp.dot(lhs, block[...], preferred_element_type=F32)
            else:
                val = lax.dot_general(lhs, block[...], NT, preferred_element_type=F32)
            if first:
                out[ch, part, :] = val
            else:
                out[ch, part, :] += val

    def finish_tokens():
        for dr in range(1, R):
            for j, (ref, full) in enumerate(tokens):
                rep_copies[j, dr].wait_recv()
                for dt in range(1, T):
                    tp_copies[j, dt, dr] = go(remote(
                        full.at[:, span(0, dr), :], full.at[:, span(dt, dr), :],
                        tt_ss.at[j, dt, dr], tt_rs.at[j, dt, dr], tp_dev(-dt),
                    ))
        for copy in tp_copies.values():
            copy.wait_recv()

        @pl.loop(0, n)
        def _(b):
            xt[b] = xg[b].T

        for ch in range(C):
            gather_dot(ch, 0, own(0, ch), 0, True)
            gather_dot(ch, 1, own(1, ch), 0, True)

    act_tile = tile_of(rows, 128)

    def activate(ch):
        @pl.loop(0, rows // act_tile)
        def _(i):
            part = pl.ds(pl.multiple_of(i * act_tile, act_tile), act_tile)
            active = jnp.maximum(pre[ch, part, :], 0.0)
            pg[ch, part, :] = (2.0 * active * agr[ch, part, :]).astype(BF16)
            at[ch, :, part] = (active * active).astype(BF16).T

    def gather(ch, before_last):
        for s in range(1, hops + 1):
            if s == hops:
                before_last()
            for i, (g, sign, k) in enumerate(streams):
                if s <= k:
                    flying[ch, i, s].wait_recv()
                    if s < k:
                        flying[ch, i, s + 1] = go(gather_copy(ch, i, s + 1))
            if s == 1 and ch == 0:
                finish_tokens()
            for i, (g, sign, k) in enumerate(streams):
                if s <= k:
                    gather_dot(ch, g, held[g].at[slot(sign, s), ch], -sign * s)
        if hops == 0:
            if ch == 0:
                finish_tokens()
            before_last()
        activate(ch)

    def grad_block(ch, g, q, dst, arrived):
        b = member(q)
        height = (db, w)[g]
        tile = tile_of(height, 256)

        @pl.loop(0, height // tile)
        def _(i):
            part = pl.ds(pl.multiple_of(i * tile, tile), tile)
            if g == 0:
                val = jnp.dot(xt[b, part, :], pg[ch], preferred_element_type=F32)
            else:
                val = jnp.dot(at[ch, part, :], cg[b], preferred_element_type=F32)
            for a in arrived:
                val = val + a[part, :].astype(F32)
            dst[part, :] = val.astype(BF16)

    rs_send, rs_recv = (us, ds_), (ur, dr_)

    def rs_index(i, s):
        g, sign, _ = streams[i]
        return s - 1 if sign > 0 else (long, short)[g] + s - 1

    reducing = {}

    def reduce_step(ch, i, s):
        g, sign, k = streams[i]
        arrived = []
        if s > 1:
            reducing[ch, i, s - 1].wait_recv()
            arrived = [rs_recv[g].at[rs_index(i, s - 1), ch]]
        mine = rs_send[g].at[rs_index(i, s), ch]
        grad_block(ch, g, sign * (k - s + 1), mine, arrived)
        reducing[ch, i, s] = go(remote(
            mine, rs_recv[g].at[rs_index(i, s), ch],
            rs_ss.at[ch, i, s - 1], rs_rs.at[ch, i, s - 1], ring_dev(sign),
        ))

    def reduce_all(ch, s):
        for i, (g, sign, k) in enumerate(streams):
            if s <= k:
                reduce_step(ch, i, s)

    for ch in range(C):
        if ch + 1 < C:
            gather(ch, functools.partial(gather_first, ch + 1))
        elif C > 1:
            gather(ch, functools.partial(reduce_all, 0, 1))
        else:
            gather(ch, lambda: None)
            reduce_all(ch, 1)

    for q in range(n):
        b = member(q)

        @pl.loop(0, rows // row_tile)
        def _(i):
            part = pl.ds(pl.multiple_of(i * row_tile, row_tile), row_tile)
            val = 0.0
            for ch in range(C):
                block = own(0, ch) if q == 0 else ug.at[q - 1, ch]
                val = val + lax.dot_general(
                    pg[ch, part, :], block[...], NT, preferred_element_type=F32
                )
            igp[b, part, :] = val.astype(BF16)

    wide = R * tok
    it_copies = [
        go(remote(
            igp.at[:, pl.ds(dt * wide, wide), :], itr.at[dt - 1],
            it_ss.at[dt], it_rs.at[dt], tp_dev(dt),
        ))
        for dt in range(1, T)
    ]
    ir_copies = []

    def finish_tp():
        for copy in it_copies:
            copy.wait_recv()

        @pl.loop(0, n)
        def _(b):
            for dr in range(R):
                part = pl.ds(dr * tok, tok)
                val = igp[b, part, :].astype(F32)
                for dt in range(1, T):
                    val = val + itr[dt - 1, b, part, :].astype(F32)
                isum[dr, b] = val.astype(BF16)

        for dr in range(1, R):
            ir_copies.append(go(remote(
                isum.at[dr], irr.at[dr - 1], ir_ss.at[dr], ir_rs.at[dr], rep_dev(dr)
            )))

    def finish_rep():
        for copy in ir_copies:
            copy.wait_recv()

        for b in range(n):
            val = isum[0, b].astype(F32)
            for dr in range(1, R):
                val = val + irr[dr - 1, b].astype(F32)
            ig_ref[:, b * db:(b + 1) * db] = val.astype(BF16)

    finish_tp()

    finals = ((fu, fur, gu_ref), (fd, fdr, gd_ref))
    fin_copies = {}

    def put(g, place, ch, val):
        if g == 0:
            gu_ref[:, hidden(place, ch)] = val
        else:
            gd_ref[hidden(place, ch), :] = val

    def finish(ch, g):
        mine, theirs, out = finals[g]
        arrived = []
        for i, (h, sign, k) in enumerate(streams):
            if h == g and k >= 1:
                reducing[ch, i, k].wait_recv()
                arrived.append(rs_recv[g].at[rs_index(i, k), ch])
        grad_block(ch, g, 0, mine.at[ch], arrived)
        for dr in range(1, R):
            fin_copies[ch, g, dr] = go(remote(
                mine.at[ch], theirs.at[dr - 1, ch],
                f_ss.at[ch, g, dr], f_rs.at[ch, g, dr], rep_dev(-dr),
            ))
        put(g, r, ch, mine[ch])

    for ch in range(C):
        for s in range(2, hops + 1):
            reduce_all(ch, s)
            if ch == 0 and s == 2:
                finish_rep()
        if ch == 0 and hops < 2:
            finish_rep()
        if ch + 1 < C:
            reduce_all(ch + 1, 1)
        for g in range(2):
            finish(ch, g)
    for (ch, g, dr), copy in fin_copies.items():
        _, theirs, out = finals[g]
        copy.wait_recv()
        put(g, lax.rem(r + dr, R), ch, theirs[dr - 1, ch])
    for copy in sends:
        copy.wait_send()


def plane_kernel(
    Z,
    x_ref, c_ref, u_ref, d_ref,
    ig_ref, gu_ref, gd_ref,
    xg, cg, xt, ug, dg, pre, pg, at,
    igp, itr, isum, igot, ipt, ift, igo, su, sd, ru, rd, fu, fd, uo, do, yu, yd,
    out_s, yw_r, zg_r, tx_r, ty_r, tt_r, rs_r, fy_r, fx_r, ig_r, ld_s, st_s,
):
    r, f, t = lax.axis_index("rep"), lax.axis_index("fs"), lax.axis_index("tp")
    z, y = lax.div(f, 2), lax.rem(f, 2)
    tok, D = x_ref.shape
    db = u_ref.shape[0]
    C, hc = pg.shape[0], pg.shape[2]
    hw, half, wide = C * hc, tok // 2, 2 * tok
    n = 2 * Z
    xdev, ydev, tdev = (1 - r, f, t), (r, f + 1 - 2 * y, t), (r, f, 1 - t)

    def zdev(s):
        return (r, f + 2 * s, t)

    low = z < Z // 2
    m = jnp.where(low, z, Z - 1 - z)
    near = (jnp.where(low, 0, 1), jnp.where(low, 1, -1))
    far = (1 - near[0], -near[1])

    ahead = {1: z < Z - 1, -1: z > 0}

    def remote(src, dst, ssem, rsem, dev):
        return pltpu.make_async_remote_copy(
            src_ref=src, dst_ref=dst, send_sem=ssem, recv_sem=rsem,
            device_id=dev, device_id_type=MESH,
        )

    def go(make):
        make().start()

    def span(at_, size):
        return pl.ds(pl.multiple_of(at_, size), size)

    def blk(b):
        return span(b * db, db)

    def hid(q, ch):
        return span(q * hw + ch * hc, hc)

    mine, other = 2 * r + y, 2 * r + 1 - y

    def held(g, ch, b):
        return ug.at[ch, blk(b), :] if g == 0 else dg.at[ch, :, blk(b)]

    spare = (uo, do)
    weights = (u_ref, d_ref)

    def strip(g, ref, q, ch):
        return ref.at[:, hid(q, ch)] if g == 0 else ref.at[hid(q, ch), :]

    own_x, own_c = xg.at[pl.ds(0, tok), :], cg.at[pl.ds(0, tok), :]
    loads = {}
    for ch in range(C):
        for g in range(2):
            loads["other", ch, g] = (strip(g, weights[g], other, ch), spare[g].at[ch])
            loads["mine", ch, g] = (strip(g, weights[g], mine, ch), held(g, ch, f))
        if ch == 0:
            loads["x"] = (x_ref, own_x)
            loads["c"] = (c_ref, own_c)
    loads = {
        key: pltpu.make_async_copy(src, dst, ld_s.at[i])
        for i, (key, (src, dst)) in enumerate(loads.items())
    }
    for copy in loads.values():
        copy.start()

    barrier = pltpu.get_barrier_semaphore()

    def greet(dev):
        pl.semaphore_signal(barrier, inc=1, device_id=dev, device_id_type=MESH)

    for dev in (xdev, ydev, tdev):
        greet(dev)
    for s in (1, -1):
        pl.when(ahead[s])(functools.partial(greet, zdev(s)))
    pl.semaphore_wait(barrier, 3 + sum(jnp.where(ahead[s], 1, 0) for s in (1, -1)))

    def swap(ch, g):
        return remote(spare[g].at[ch], held(g, ch, f), out_s.at[0], yw_r.at[ch, g], ydev)

    def origin(s, k, e):
        return f - 2 * s * k + e * (1 - 2 * y)

    def pass_on(ch, g, s, k, e):
        block = held(g, ch, origin(s, k, e))
        i = (ch, z - s * k, e, g)
        return remote(block, block, out_s.at[(3 - s) // 2], zg_r.at[i], zdev(s))

    def landed(ch, g, s, k, e):
        block = held(g, ch, origin(s, k, e))
        i = (ch, z - s * k, e, g)
        return remote(block, block, out_s.at[(3 - s) // 2], zg_r.at[i], zdev(s))

    def begin(ch, g, e, also=None):
        for s in (1, -1):
            cond = ahead[s] if also is None else ahead[s] & also
            pl.when(cond)(functools.partial(
                go, functools.partial(pass_on, ch, g, s, 0, e)))

    level = [m == m0 for m0 in range(Z // 2)]
    reached = {}
    for k in range(1, Z):
        reached[1, k], reached[-1, k] = z >= k, z < Z - k
    passing = {key: reached[key] & ahead[key[0]] for key in reached}

    outward = {1: low, -1: jnp.logical_not(low)}
    split = {}
    for (s, k), cond in passing.items():
        split[s, k, 0] = cond & outward[s]
        split[s, k, 1] = cond & outward[-s]

    def relay(ch, g, k, es=(0, 1), toward=None):
        for e in es:
            for s in (1, -1):
                cond = passing[s, k] if toward is None else split[s, k, toward]

                @pl.when(cond)
                def _():
                    landed(ch, g, s, k, e).wait_recv()
                    go(functools.partial(pass_on, ch, g, s, k, e))

    def collect(ch, g):
        for k in range(1, Z):
            for e in range(2):
                for s in (1, -1):

                    @pl.when(reached[s, k] & jnp.logical_not(ahead[s]))
                    def _():
                        landed(ch, g, s, k, e).wait_recv()

    def swapped(ch, g, also=None):
        begin(ch, g, 1, also)

    def rows(k, dt, part=(0, 2)):
        lo, hi = part
        return pl.ds((2 * k + dt) * tok + lo * half, (hi - lo) * half)

    def quarter(i):
        return span(jnp.where(low, Z - 1 - i, i) * 2 * db, 2 * db)

    A, B, AB = (0, 1), (1, 2), (0, 2)

    def hop(sems, i, dev, full, src, dst, cols):
        def make():
            where = slice(None) if cols is None else quarter(cols)
            return remote(
                full.at[rows(*src), where], full.at[rows(*dst), where],
                sems[0], sems[1].at[i], dev,
            )

        return make

    X, Y, S = (out_s.at[3], tx_r), (out_s.at[4], ty_r), (out_s.at[5], tt_r)
    moves = {}
    for i, part in enumerate((A, B)):
        moves["x", "x", i] = hop(X, i, xdev, xg, (0, 0, part), (1, 0, part), None)
        moves["y", "x", i] = hop(Y, i, ydev, xg, (0, 0, part), (2, 0, part), None)
        moves["d", "x", i] = hop(X, 2 + i, xdev, xg, (2, 0, part), (3, 0, part), None)
    moves["s", "x", 0] = hop(S, 0, tdev, xg, (0, 0, AB), (0, 1, AB), None)
    moves["s", "c", 0] = hop(S, 1, tdev, cg, (0, 0, AB), (0, 1, AB), None)
    for k in range(1, 4):
        moves["s", "x", k] = hop(S, 1 + k, tdev, xg, (k, 0, AB), (k, 1, AB), None)
    for i in range(Z):
        for p, (xp, yp) in enumerate(((B, A), (A, B))):
            moves["x%d" % p, "c", i] = hop(X, 4 + 3 * i + p, xdev, cg, (0, 0, xp), (1, 0, xp), i)
            moves["y%d" % p, "c", i] = hop(Y, 2 + 3 * i + p, ydev, cg, (0, 0, yp), (2, 0, yp), i)
        moves["dx", "c", i] = hop(X, 6 + 3 * i, xdev, cg, (2, 0, A), (3, 0, A), i)
        moves["dy", "c", i] = hop(Y, 4 + 3 * i, ydev, cg, (1, 0, B), (3, 0, B), i)
        for k in range(1, 4):
            moves["s%d" % k, "c", i] = hop(
                S, 5 + i, tdev, cg, (k, 0, AB), (k, 1, AB), i)

    def start(*key):
        go(moves[key])

    def arrive(*key):
        moves[key]().wait_recv()

    def flip(k):
        part = pl.ds(k * wide, wide)

        @pl.loop(0, n)
        def _(b):
            xt[blk(b), part] = xg[part, blk(b)].T

    def forward(ch, first, last):
        @pl.loop(first, last, unroll=2 if (last - first) % 2 == 0 else 1)
        def _(k):
            part = span(k * wide, wide)
            active = jnp.maximum(
                jnp.dot(xg[part, :], ug[ch], preferred_element_type=F32), 0.0)
            pre[ch, part, :] = active
            at[ch, :, part] = (active * active).astype(BF16).T

    def backward(ch):
        @pl.loop(0, 4, unroll=2)
        def _(k):
            part = span(k * wide, wide)
            val = lax.dot_general(cg[part, :], dg[ch], NT, preferred_element_type=F32)
            pg[ch, part, :] = (2.0 * pre[ch, part, :] * val).astype(BF16)

    def grad(ch, g, b):
        if g == 0:
            return jnp.dot(xt[blk(b), :], pg[ch], preferred_element_type=F32)
        return jnp.dot(at[ch], cg[:, blk(b)], preferred_element_type=F32)

    out_buf, in_buf, fin = (su, sd), (ru, rd), (fu, fd)

    def partial_copy(ch, g, way, j, e):
        d, s = way
        return remote(
            out_buf[g].at[d, j, ch, e], in_buf[g].at[d, j, ch, e],
            out_s.at[6], rs_r.at[d, j, ch, g, e], zdev(s))

    def side_of(e):
        return e * y + (1 - e) * (1 - y)

    def reduce(ch, g, way, j, m0, es=None):
        cond = level[m0]
        to = jnp.where(way[1] > 0, Z - 1 - j, j)
        more = m0 > 0 or way is far

        def step(e):
            val = grad(ch, g, 2 * to + side_of(e))
            if more:
                partial_copy(ch, g, way, j, e).wait_recv()
                val = val + in_buf[g][way[0], j, ch, e].astype(F32)
            out_buf[g][way[0], j, ch, e] = val.astype(BF16)
            partial_copy(ch, g, way, j, e).start()

        if es is None:
            pl.loop(0, 2)(step)
        else:
            for e in es:
                step(e)

    outs, passed = (gu_ref, gd_ref), (yu, yd)

    def store(ch, g, e):
        if ch == C:
            return pltpu.make_async_copy(igo, ig_ref, st_s.at[1])
        src = passed[g].at[ch] if e else fin[g].at[ch, 1]
        dst = strip(g, outs[g], other if e else mine, ch)
        return pltpu.make_async_copy(src, dst, st_s.at[0])

    def final_y(ch, g):
        return remote(
            fin[g].at[ch, 0], passed[g].at[ch], out_s.at[7], fy_r.at[ch, g], ydev)

    def final_x(ch, g, e):
        src = passed[g].at[ch] if e else fin[g].at[ch, 1]
        return remote(
            src, strip(g, outs[g], other if e else mine, ch), out_s.at[7], fx_r.at[0], xdev)

    def finish(ch, g, m0, between=None):
        cond = level[m0]
        ways = [(far, m0)] + ([(near, Z - 1 - m0)] if m0 else [])
        for e in range(2):
            val = grad(ch, g, 2 * z + side_of(e))
            for way, j in ways:
                partial_copy(ch, g, way, j, e).wait_recv()
                val = val + in_buf[g][way[0], j, ch, e].astype(F32)
            fin[g][ch, e] = val.astype(BF16)
            if e == 0:
                go(functools.partial(final_y, ch, g))
                if between:
                    between()
            else:
                go(functools.partial(final_x, ch, g, 0))
        store(ch, g, 0).start()

    def spread(ch, g, m0):
        final_y(ch, g).wait_recv()
        go(functools.partial(final_x, ch, g, 1))
        store(ch, g, 1).start()

    def cols(p):
        return pl.ds(p * (D // 2), D // 2)

    def ig_copy(i):
        part = cols((i + 1) % 2)
        if i > 6:
            part = cols(i - 7)
            src, dst = igp.at[1, :, :, part], itr.at[:, :, part]
            return remote(src, dst, out_s.at[8], ig_r.at[i - 1], tdev)
        kind = (i - 1) // 2
        if kind < 2:
            src, dst = isum.at[3 - kind, :, part], igot.at[1 - kind, :, part]
        else:
            src, dst = ipt.at[:, part], ift.at[:, part]
        return remote(src, dst, out_s.at[8], ig_r.at[i - 1], ydev if kind < 2 else xdev)

    def ig_go(i):
        go(functools.partial(ig_copy, i))

    def ig_part(dt, p):
        @pl.loop(p * (n // 2), (p + 1) * (n // 2), unroll=n // 2)
        def _(b):
            val = 0.0
            for ch in range(C):
                lhs = jnp.concatenate([pg[ch, rows(k, dt), :] for k in range(4)], 0)
                val = val + lax.dot_general(
                    lhs, ug[ch, blk(b), :], NT, preferred_element_type=F32)
            val = val.astype(BF16)
            for k in range(4):
                igp[dt, k, :, blk(b)] = val[k * tok:(k + 1) * tok]

        if dt:
            ig_go(7 + p)

    def ig_first(p):
        ig_copy(7 + p).wait_recv()

        @pl.loop(0, 4)
        def _(k):
            val = igp[0, k, :, cols(p)].astype(F32) + itr[k, :, cols(p)].astype(F32)
            isum[k, :, cols(p)] = val.astype(BF16)

    def ig_diag(p):
        ig_go(1 + p)

    def ig_more(p):
        ig_go(3 + p)

    def ig_second(p):
        ig_copy(1 + p).wait_recv()
        val = isum[1, :, cols(p)].astype(F32) + igot[1, :, cols(p)].astype(F32)
        ipt[:, cols(p)] = val.astype(BF16)
        ig_go(5 + p)

    def ig_last():
        for i in range(3, 7):
            ig_copy(i).wait_recv()
        val = isum[0].astype(F32) + igot[0].astype(F32) + ift[...].astype(F32)
        igo[...] = val.astype(BF16)
        store(C, 0, 0).start()

    edge, inner = level[0], m > 0
    last = C - 1

    units = [(ch, g) for ch in range(C) for g in range(2)]

    loads["other", 0, 0].wait()
    go(functools.partial(swap, 0, 0))
    loads["mine", 0, 0].wait()
    begin(0, 0, 0)
    loads["x"].wait()
    for i in range(2):
        start("x", "x", i)
        start("y", "x", i)
    loads["mine", 0, 1].wait()
    begin(0, 1, 0)
    start("s", "x", 0)
    loads["c"].wait()
    start("s", "c", 0)
    for unit in units[1:]:
        loads[("other",) + unit].wait()
        go(functools.partial(swap, *unit))
        if unit != units[1]:
            loads[("mine",) + unit].wait()

    swap(0, 0).wait_recv()
    begin(0, 0, 1)
    for unit in units[2:]:
        begin(*unit, 0, edge)
    relay(0, 0, 1)
    arrive("s", "x", 0)
    arrive("s", "c", 0)
    flip(0)
    arrive("y", "x", 0)
    start("d", "x", 0)
    for k in range(2, Z - 1):
        relay(0, 0, k)
    for unit in units[2:3]:
        begin(*unit, 0, inner)
    for i in range(2):
        arrive("x", "x", i)
    start("s", "x", 1)
    arrive("y", "x", 1)
    start("d", "x", 1)

    def offer(i):
        for way in ("x0", "y0", "x1", "y1"):
            start(way, "c", i)

    offer(0)
    start("s", "x", 2)
    swap(0, 1).wait_recv()
    begin(0, 1, 1)
    relay(0, 1, 1, (0,))
    arrive("s", "x", 1)
    flip(1)
    for k in range(2, Z - 1):
        relay(0, 1, k, (0,))
    relay(0, 1, 1, (1,))
    arrive("s", "x", 2)
    flip(2)
    collect(0, 0)
    forward(0, 0, 3)
    for unit in units[2:]:
        swap(*unit).wait_recv()
        begin(*unit, 1, edge)
    for i in range(2):
        arrive("d", "x", i)
    start("s", "x", 3)

    def ready(i):
        three = cg.at[pl.ds(0, 3 * tok), quarter(i)]
        remote(three, three, out_s.at[5], tt_r.at[5 + i], tdev).wait_recv()
        if i < Z - 1:
            pl.when(edge)(functools.partial(reduce, 0, 1, near, i, 0))

    tasks = [(unit, k) for unit in units[2:] for k in range(1, Z - 1)]
    for i in range(Z):
        arrive("x0", "c", i)
        start("dy", "c", i)
        arrive("y0", "c", i)
        start("dx", "c", i)
        if i + 1 < Z:
            offer(i + 1)
        if i == 0:
            for k in range(2, Z - 1):
                relay(0, 1, k, (1,))
            for unit in units[2:]:
                if unit != units[2]:
                    begin(*unit, 0, inner)
                begin(*unit, 1, inner)
            for unit in units[2:]:
                for k in range(1, Z // 2):
                    relay(*unit, k, toward=0)
            arrive("s", "x", 3)
            flip(3)
            forward(0, 3, 4)
        else:
            if i > 1:
                ready(i - 1)
            if i == Z - 1:
                for m0 in range(1, Z // 2):
                    pl.when(level[m0])(functools.partial(reduce, 0, 1, near, 0, m0))
        arrive("x1", "c", i)
        start("s1", "c", i)
        arrive("y1", "c", i)
        start("s2", "c", i)
        arrive("dy", "c", i)
        arrive("dx", "c", i)
        start("s3", "c", i)
        if i == 0:
            ready(0)
        if i == 1 and tasks:
            unit, k = tasks.pop(0)
            relay(*unit, k, toward=1)
    if Z > 1:
        ready(Z - 1)

    def edges():
        collect(0, 1)
        backward(0)
        for j in range(Z - 1):
            reduce(0, 0, near, j, 0)
        for ch in range(1, C):
            collect(ch, 0)
            forward(ch, 0, 4)
            for j in range(Z - 1):
                reduce(ch, 1, near, j, 0)
            collect(ch, 1)
            backward(ch)
            if ch < C - 1:
                for j in range(Z - 1):
                    reduce(ch, 0, near, j, 0)
        ig_part(1, 0)
        ig_part(1, 1)

        def meanwhile():
            ig_part(0, 0)
            ig_first(0)
            ig_diag(0)
            ig_part(0, 1)

        finish(0, 1, 0, meanwhile)
        ig_first(1)
        if C > 1:
            for j in range(Z - 1):
                reduce(C - 1, 0, near, j, 0)
        ig_diag(1)
        spread(0, 1, 0)
        finish(0, 0, 0)
        ig_second(0)
        for ch in range(1, C):
            finish(ch, 1, 0)
            spread(ch - 1, 0, 0)
            if ch == 1:
                ig_more(0)
                ig_second(1)
            spread(ch, 1, 0)
            finish(ch, 0, 0)
            if ch == 1:
                ig_more(1)
        if C == 1:
            ig_more(0)
            ig_second(1)
            ig_more(1)
        spread(C - 1, 0, 0)
        ig_last()

    def inside(m0):
        left = list(tasks)

        def relays(count):
            for _ in range(min(count, len(left))):
                unit, k = left.pop(0)
                relay(*unit, k, toward=1)

        def nears(ch, g, js):
            for j in js:
                reduce(ch, g, near, j, m0)

        def fars(ch, g):
            for j in range(m0):
                reduce(ch, g, far, j, m0)

        def both(ch, g):
            for e in range(2):
                for j in range(m0):
                    reduce(ch, g, far, j, m0, (e,))
                for j in rest:
                    reduce(ch, g, near, j, m0, (e,))

        first, rest = range(1), range(1, Z - 1 - m0)
        keep = (Z - 2) * (C > 1)
        relays(len(left) - keep)
        nears(0, 1, rest)
        relays(keep - 1)
        backward(0)
        for ch in range(1, C):
            forward(ch, 0, 4)
        relays(1)
        fars(0, 1)
        for ch in range(1, C):
            backward(ch)
        nears(0, 0, first)
        finish(0, 1, m0)
        both(0, 0)
        spread(0, 1, m0)
        for dt in (1, 0):
            for p in range(2):
                ig_part(dt, p)
        finish(0, 0, m0)
        for ch in range(1, C):
            nears(ch, 1, first)
            if ch == 1:
                for p in range(2):
                    ig_first(p)
                    ig_diag(p)
            spread(ch - 1, 0, m0)
            both(ch, 1)
            if ch == 1:
                ig_second(0)
            reduce(ch, 0, near, 0, m0, (0,))
            finish(ch, 1, m0)
            reduce(ch, 0, near, 0, m0, (1,))
            if ch == 1:
                ig_more(0)
                ig_second(1)
                ig_more(1)
            both(ch, 0)
            spread(ch, 1, m0)
            finish(ch, 0, m0)
        if C == 1:
            for p in range(2):
                ig_first(p)
                ig_diag(p)
                ig_more(p)
            for p in range(2):
                ig_second(p)
        spread(C - 1, 0, m0)
        ig_last()

    pl.when(edge)(edges)
    for m0 in range(1, Z // 2):
        pl.when(level[m0])(functools.partial(inside, m0))

    def settle():
        remote(gu_ref, gu_ref, out_s.at[7], fx_r.at[0], xdev).wait_recv()
        pltpu.make_async_copy(gu_ref, gu_ref, st_s.at[0]).wait()
        store(C, 0, 0).wait()

    def sent(i, count):
        some = xg.at[pl.ds(0, count), :]
        remote(some, some, out_s.at[i], out_s.at[i], xdev).wait_send()

    def drain():
        block = 4 * hw // n
        sent(0, block // 2)
        for z0 in range(Z - 1):
            pl.when(z == z0)(functools.partial(sent, 1, (z0 + 1) * block))
            pl.when(z == Z - 1 - z0)(functools.partial(sent, 2, (z0 + 1) * block))
        sent(3, 7 * half)
        sent(4, 5 * half)
        sent(5, 8 * tok)
        sent(6, (Z - 1) * block)
        sent(7, 3 * block // 2)
        sent(8, 7 * tok)

    settle()
    drain()


def ring_call(inputs, up_weight):
    R, n, T = axis_sizes()
    tok, D = inputs.shape
    db, hb = up_weight.shape[0], up_weight.shape[1] // R
    rows = R * T * tok
    C = tile_of(hb // 128, CHUNKS) if hb > 128 else 1
    w = hb // C
    V, S = pltpu.VMEM, pltpu.SemaphoreType.DMA
    hops = max(n // 2, 1)
    m = max(n - 1, 1)
    scratch = [
        V((n, rows, db), BF16), V((n, rows, db), BF16), V((n, db, rows), BF16),
        V((m, C, db, w), BF16), V((m, C, w, db), BF16),
        V((C, rows, w), F32), V((C, rows, w), F32), V((C, rows, w), BF16), V((C, w, rows), BF16),
        V((n, rows, db), BF16), V((max(T - 1, 1), n, R * tok, db), BF16),
        V((R, n, tok, db), BF16), V((max(R - 1, 1), n, tok, db), BF16),
        V((m, C, db, w), BF16), V((m, C, db, w), BF16),
        V((m, C, w, db), BF16), V((m, C, w, db), BF16),
        V((C, db, w), BF16), V((C, w, db), BF16),
        V((max(R - 1, 1), C, db, w), BF16), V((max(R - 1, 1), C, w, db), BF16),
        S((C, 4, hops)), S((C, 4, hops)), S((C, 4, hops)), S((C, 4, hops)),
        S((2, R)), S((2, R)), S((2, T, R)), S((2, T, R)),
        S((T,)), S((T,)), S((R,)), S((R,)), S((C, 2, R)), S((C, 2, R)),
    ]
    return functools.partial(ring_kernel, R, n, T), scratch, (R, hb), pltpu.VMEM


def finals_kernel(scale, *refs):
    sources, targets, raw, wide = refs[:3], refs[3:6], refs[6:9], refs[9:11]
    load, store = refs[11:]
    jobs = []
    for a in (1, 2, 0):
        rows = sources[a].shape[0]
        for p in range(PARTS):
            part = pl.ds(p * (rows // PARTS), rows // PARTS)
            jobs.append((a, p, part))
    loads, stores = [], []
    for a, p, part in jobs:
        copy = pltpu.make_async_copy(
            sources[a].at[part, :], raw[a].at[part, :], load.at[a, p])
        copy.start()
        loads.append(copy)
    for (a, p, part), copy in zip(jobs, loads):
        copy.wait()
        ready = raw[a]
        if a:
            ready = wide[a - 1]
            ready[part, :] = raw[a][part, :].astype(F32) * scale
        copy = pltpu.make_async_copy(
            ready.at[part, :], targets[a].at[part, :], store.at[a, p])
        copy.start()
        stores.append(copy)
    for copy in stores:
        copy.wait()


def finals_call(ig, gu, gd, scale):
    any_space = pl.BlockSpec(memory_space=pl.ANY)
    V, S = pltpu.VMEM, pltpu.SemaphoreType.DMA
    return pl.pallas_call(
        functools.partial(finals_kernel, scale),
        in_specs=[any_space] * 3,
        out_specs=(any_space,) * 3,
        out_shape=(
            jax.ShapeDtypeStruct(ig.shape, BF16),
            jax.ShapeDtypeStruct(gu.shape, F32),
            jax.ShapeDtypeStruct(gd.shape, F32),
        ),
        scratch_shapes=[
            V(ig.shape, BF16), V(gu.shape, BF16), V(gd.shape, BF16),
            V(gu.shape, F32), V(gd.shape, F32), S((3, PARTS)), S((3, PARTS)),
        ],
    )(ig, gu, gd)


def axis_sizes():
    return lax.axis_size("rep"), lax.axis_size("fs"), lax.axis_size("tp")


def plane_call(inputs, up_weight):
    R, n, T = axis_sizes()
    tok, D = inputs.shape
    db, HB = up_weight.shape
    Z, G = n // 2, 2 * R
    if R != 2 or T != 2 or n % 4 or tok % 32 or HB % (128 * G) or db % 128:
        return None
    hw = HB // G
    C = tile_of(hw // 128, CHUNKS)
    hc = hw // C
    rows = 8 * tok
    V, S = pltpu.VMEM, pltpu.SemaphoreType.DMA
    data = [
        ((rows, D), BF16), ((rows, D), BF16), ((D, rows), BF16),
        ((C, D, hc), BF16), ((C, hc, D), BF16),
        ((C, rows, hc), F32), ((C, rows, hc), BF16), ((C, hc, rows), BF16),
        ((2, 4, tok, D), BF16), ((4, tok, D), BF16), ((4, tok, D), BF16),
        ((2, tok, D), BF16), ((tok, D), BF16), ((tok, D), BF16),
        ((tok, D), BF16),
        ((2, Z - 1, C, 2, db, hc), BF16), ((2, Z - 1, C, 2, hc, db), BF16),
        ((2, Z - 1, C, 2, db, hc), BF16), ((2, Z - 1, C, 2, hc, db), BF16),
        ((C, 2, db, hc), BF16), ((C, 2, hc, db), BF16),
        ((C, db, hc), BF16), ((C, hc, db), BF16), ((C, db, hc), BF16), ((C, hc, db), BF16),
    ]
    size = sum(math.prod(s) * jnp.dtype(d).itemsize for s, d in data)
    if size > 50 * 2**20 or 4 * hw % n or (Z - 1) * 4 * hw > 8 * tok * n:
        return None
    sems = [
        (C, 2), (C, Z, 2, 2), (4 + 3 * Z,), (2 + 3 * Z,), (5 + Z,),
        (2, Z - 1, C, 2, 2), (C, 2), (1,), (8,),
    ]
    scratch = [V(s, d) for s, d in data] + [S((9,))] + [S(s) for s in sems]
    scratch += [S((4 * C + 2,)), S((2,))]
    return functools.partial(plane_kernel, Z), scratch, (1, HB), pl.ANY


def shards(inputs, cotangent, up_weight, down_weight):
    R, n, T = axis_sizes()
    tok, D = inputs.shape
    db = up_weight.shape[0]
    chosen = plane_call(inputs, up_weight) or ring_call(inputs, up_weight)
    body, scratch, (parts, hb), space = chosen
    spec = pl.BlockSpec(memory_space=space)
    ig, gu, gd = pl.pallas_call(
        body,
        out_shape=(
            jax.ShapeDtypeStruct((tok, D), BF16),
            jax.ShapeDtypeStruct((db, parts * hb), BF16),
            jax.ShapeDtypeStruct((parts * hb, db), BF16),
        ),
        in_specs=[spec] * 4,
        out_specs=(spec,) * 3,
        scratch_shapes=scratch,
        compiler_params=pltpu.CompilerParams(
            collective_id=0, has_side_effects=True, vmem_limit_bytes=60 * 2**20
        ),
    )(inputs, cotangent, up_weight, down_weight)
    total_tokens = tok * R * n * T
    loss_scale = 1.0 / math.sqrt(total_tokens)
    if space is pl.ANY:
        return finals_call(ig, gu, gd, loss_scale)
    return ig, gu.astype(F32) * loss_scale, gd.astype(F32) * loss_scale


def solution(mesh):
    token, up, down = P(("rep", "fs", "tp"), None), P("fs", "tp"), P("tp", "fs")
    return jax.shard_map(
        shards,
        mesh=mesh,
        in_specs=(token, token, up, down),
        out_specs=(token, up, down),
        check_vma=False,
    )
```

```python
import functools
import math

import jax
import jax.numpy as jnp
from jax import lax
from jax.experimental import pallas as pl
from jax.experimental.pallas import tpu as pltpu
from jax.sharding import PartitionSpec as P

MESH = pl.DeviceIdType.MESH
CHUNKS = 2
PARTS = 4
BF16, F32 = jnp.bfloat16, jnp.float32
NT = (((1,), (1,)), ((), ()))


def ring_place(f, n):
    odd = lax.rem(f, 2)
    half = lax.div(f, 2)
    return half * (1 - odd) + (n - 1 - half) * odd


def ring_member(p, n):
    back = lax.div(p, (n + 1) // 2)
    return 2 * p * (1 - back) + (2 * n - 1 - 2 * p) * back


def tile_of(size, most):
    while size % most:
        most //= 2
    return most


def ring_kernel(
    R, n, T,
    x_ref, c_ref, u_ref, d_ref,
    ig_ref, gu_ref, gd_ref,
    xg, cg, xt, ug, dg, pre, agr, pg, at,
    igp, itr, isum, irr, us, ur, ds_, dr_, fu, fd, fur, fdr,
    ag_ss, ag_rs, rs_ss, rs_rs, tr_ss, tr_rs, tt_ss, tt_rs,
    it_ss, it_rs, ir_ss, ir_rs, f_ss, f_rs,
):
    r, f, t = lax.axis_index("rep"), lax.axis_index("fs"), lax.axis_index("tp")
    tok, db = x_ref.shape[0], u_ref.shape[0]
    C, w = pre.shape[0], pre.shape[2]
    hb = C * w
    rows = R * T * tok

    def hidden(place, ch):
        return pl.ds(pl.multiple_of(place * hb + ch * w, w), w)

    for ref, full in ((x_ref, xg), (c_ref, cg)):
        for q in range(n):
            full[q, 0:tok, :] = ref[:, q * db:(q + 1) * db]
    p = ring_place(f, n)

    def member(q):
        return ring_member(lax.rem(p + q + n, n), n)

    def ring_dev(sign):
        return (r, member(sign), t)

    def rep_dev(q):
        return (lax.rem(r + q + R, R), f, t)

    def tp_dev(q):
        return (r, f, lax.rem(t + q + T, T))

    barrier = pltpu.get_barrier_semaphore()
    peers = [ring_dev(1), ring_dev(-1)]
    peers += [rep_dev(q) for q in range(1, R)] + [tp_dev(q) for q in range(1, T)]
    for peer in peers:
        pl.semaphore_signal(barrier, inc=1, device_id=peer, device_id_type=MESH)
    pl.semaphore_wait(barrier, len(peers))

    def remote(src, dst, ssem, rsem, dev):
        return pltpu.make_async_remote_copy(
            src_ref=src, dst_ref=dst, send_sem=ssem, recv_sem=rsem,
            device_id=dev, device_id_type=MESH,
        )

    long, short = n // 2, (n - 1) // 2
    streams = [(0, 1, long), (0, -1, short), (1, 1, short), (1, -1, long)]
    hops = max(long, short)
    def own(g, ch):
        return u_ref.at[:, hidden(r, ch)] if g == 0 else d_ref.at[hidden(r, ch), :]

    held = (ug, dg)

    def slot(sign, s):
        return (n - s if sign > 0 else s) - 1

    def gather_copy(ch, i, s):
        g, sign, _ = streams[i]
        src = own(g, ch) if s == 1 else held[g].at[slot(sign, s - 1), ch]
        return remote(
            src, held[g].at[slot(sign, s), ch],
            ag_ss.at[ch, i, s - 1], ag_rs.at[ch, i, s - 1], ring_dev(sign),
        )

    sends = []

    def go(copy):
        copy.start()
        sends.append(copy)
        return copy

    flying = {}

    def gather_first(ch):
        for i, (g, sign, k) in enumerate(streams):
            if k >= 1:
                flying[ch, i, 1] = go(gather_copy(ch, i, 1))

    gather_first(0)

    tokens = tuple((full.at[:, 0:tok, :], full) for full in (xg, cg))

    def span(dt, dr):
        return pl.ds((dt * R + dr) * tok, tok)

    rep_copies = {}
    for dr in range(1, R):
        for j, (ref, full) in enumerate(tokens):
            rep_copies[j, dr] = go(remote(
                ref, full.at[:, span(0, dr), :], tr_ss.at[j, dr], tr_rs.at[j, dr], rep_dev(-dr)
            ))
    tp_copies = {}
    for dt in range(1, T):
        for j, (ref, full) in enumerate(tokens):
            tp_copies[j, dt, 0] = go(remote(
                ref, full.at[:, span(dt, 0), :], tt_ss.at[j, dt, 0], tt_rs.at[j, dt, 0],
                tp_dev(-dt),
            ))

    row_tile = tile_of(rows, 256)

    def gather_dot(ch, g, block, q, first=False):
        b = member(q)
        out, full = ((pre, xg), (agr, cg))[g]

        @pl.loop(0, rows // row_tile)
        def _(i):
            part = pl.ds(pl.multiple_of(i * row_tile, row_tile), row_tile)
            lhs = full[b, part, :]
            if g == 0:
                val = jnp.dot(lhs, block[...], preferred_element_type=F32)
            else:
                val = lax.dot_general(lhs, block[...], NT, preferred_element_type=F32)
            if first:
                out[ch, part, :] = val
            else:
                out[ch, part, :] += val

    def finish_tokens():
        for dr in range(1, R):
            for j, (ref, full) in enumerate(tokens):
                rep_copies[j, dr].wait_recv()
                for dt in range(1, T):
                    tp_copies[j, dt, dr] = go(remote(
                        full.at[:, span(0, dr), :], full.at[:, span(dt, dr), :],
                        tt_ss.at[j, dt, dr], tt_rs.at[j, dt, dr], tp_dev(-dt),
                    ))
        for copy in tp_copies.values():
            copy.wait_recv()

        @pl.loop(0, n)
        def _(b):
            xt[b] = xg[b].T

        for ch in range(C):
            gather_dot(ch, 0, own(0, ch), 0, True)
            gather_dot(ch, 1, own(1, ch), 0, True)

    act_tile = tile_of(rows, 128)

    def activate(ch):
        @pl.loop(0, rows // act_tile)
        def _(i):
            part = pl.ds(pl.multiple_of(i * act_tile, act_tile), act_tile)
            active = jnp.maximum(pre[ch, part, :], 0.0)
            pg[ch, part, :] = (2.0 * active * agr[ch, part, :]).astype(BF16)
            at[ch, :, part] = (active * active).astype(BF16).T

    def gather(ch, before_last):
        for s in range(1, hops + 1):
            if s == hops:
                before_last()
            for i, (g, sign, k) in enumerate(streams):
                if s <= k:
                    flying[ch, i, s].wait_recv()
                    if s < k:
                        flying[ch, i, s + 1] = go(gather_copy(ch, i, s + 1))
            if s == 1 and ch == 0:
                finish_tokens()
            for i, (g, sign, k) in enumerate(streams):
                if s <= k:
                    gather_dot(ch, g, held[g].at[slot(sign, s), ch], -sign * s)
        if hops == 0:
            if ch == 0:
                finish_tokens()
            before_last()
        activate(ch)

    def grad_block(ch, g, q, dst, arrived):
        b = member(q)
        height = (db, w)[g]
        tile = tile_of(height, 256)

        @pl.loop(0, height // tile)
        def _(i):
            part = pl.ds(pl.multiple_of(i * tile, tile), tile)
            if g == 0:
                val = jnp.dot(xt[b, part, :], pg[ch], preferred_element_type=F32)
            else:
                val = jnp.dot(at[ch, part, :], cg[b], preferred_element_type=F32)
            for a in arrived:
                val = val + a[part, :].astype(F32)
            dst[part, :] = val.astype(BF16)

    rs_send, rs_recv = (us, ds_), (ur, dr_)

    def rs_index(i, s):
        g, sign, _ = streams[i]
        return s - 1 if sign > 0 else (long, short)[g] + s - 1

    reducing = {}

    def reduce_step(ch, i, s):
        g, sign, k = streams[i]
        arrived = []
        if s > 1:
            reducing[ch, i, s - 1].wait_recv()
            arrived = [rs_recv[g].at[rs_index(i, s - 1), ch]]
        mine = rs_send[g].at[rs_index(i, s), ch]
        grad_block(ch, g, sign * (k - s + 1), mine, arrived)
        reducing[ch, i, s] = go(remote(
            mine, rs_recv[g].at[rs_index(i, s), ch],
            rs_ss.at[ch, i, s - 1], rs_rs.at[ch, i, s - 1], ring_dev(sign),
        ))

    def reduce_all(ch, s):
        for i, (g, sign, k) in enumerate(streams):
            if s <= k:
                reduce_step(ch, i, s)

    for ch in range(C):
        if ch + 1 < C:
            gather(ch, functools.partial(gather_first, ch + 1))
        elif C > 1:
            gather(ch, functools.partial(reduce_all, 0, 1))
        else:
            gather(ch, lambda: None)
            reduce_all(ch, 1)

    for q in range(n):
        b = member(q)

        @pl.loop(0, rows // row_tile)
        def _(i):
            part = pl.ds(pl.multiple_of(i * row_tile, row_tile), row_tile)
            val = 0.0
            for ch in range(C):
                block = own(0, ch) if q == 0 else ug.at[q - 1, ch]
                val = val + lax.dot_general(
                    pg[ch, part, :], block[...], NT, preferred_element_type=F32
                )
            igp[b, part, :] = val.astype(BF16)

    wide = R * tok
    it_copies = [
        go(remote(
            igp.at[:, pl.ds(dt * wide, wide), :], itr.at[dt - 1],
            it_ss.at[dt], it_rs.at[dt], tp_dev(dt),
        ))
        for dt in range(1, T)
    ]
    ir_copies = []

    def finish_tp():
        for copy in it_copies:
            copy.wait_recv()

        @pl.loop(0, n)
        def _(b):
            for dr in range(R):
                part = pl.ds(dr * tok, tok)
                val = igp[b, part, :].astype(F32)
                for dt in range(1, T):
                    val = val + itr[dt - 1, b, part, :].astype(F32)
                isum[dr, b] = val.astype(BF16)

        for dr in range(1, R):
            ir_copies.append(go(remote(
                isum.at[dr], irr.at[dr - 1], ir_ss.at[dr], ir_rs.at[dr], rep_dev(dr)
            )))

    def finish_rep():
        for copy in ir_copies:
            copy.wait_recv()

        for b in range(n):
            val = isum[0, b].astype(F32)
            for dr in range(1, R):
                val = val + irr[dr - 1, b].astype(F32)
            ig_ref[:, b * db:(b + 1) * db] = val.astype(BF16)

    finish_tp()

    finals = ((fu, fur, gu_ref), (fd, fdr, gd_ref))
    fin_copies = {}

    def put(g, place, ch, val):
        if g == 0:
            gu_ref[:, hidden(place, ch)] = val
        else:
            gd_ref[hidden(place, ch), :] = val

    def finish(ch, g):
        mine, theirs, out = finals[g]
        arrived = []
        for i, (h, sign, k) in enumerate(streams):
            if h == g and k >= 1:
                reducing[ch, i, k].wait_recv()
                arrived.append(rs_recv[g].at[rs_index(i, k), ch])
        grad_block(ch, g, 0, mine.at[ch], arrived)
        for dr in range(1, R):
            fin_copies[ch, g, dr] = go(remote(
                mine.at[ch], theirs.at[dr - 1, ch],
                f_ss.at[ch, g, dr], f_rs.at[ch, g, dr], rep_dev(-dr),
            ))
        put(g, r, ch, mine[ch])

    for ch in range(C):
        for s in range(2, hops + 1):
            reduce_all(ch, s)
            if ch == 0 and s == 2:
                finish_rep()
        if ch == 0 and hops < 2:
            finish_rep()
        if ch + 1 < C:
            reduce_all(ch + 1, 1)
        for g in range(2):
            finish(ch, g)
    for (ch, g, dr), copy in fin_copies.items():
        _, theirs, out = finals[g]
        copy.wait_recv()
        put(g, lax.rem(r + dr, R), ch, theirs[dr - 1, ch])
    for copy in sends:
        copy.wait_send()


def plane_kernel(
    Z,
    x_ref, c_ref, u_ref, d_ref,
    ig_ref, gu_ref, gd_ref,
    xg, cg, xt, ug, dg, pre, pg, at,
    igp, itr, isum, igot, ipt, ift, igo, su, sd, ru, rd, fu, fd, uo, do, yu, yd,
    out_s, yw_r, zg_r, tx_r, ty_r, tt_r, rs_r, fy_r, fx_r, ig_r, ld_s, st_s,
):
    r, f, t = lax.axis_index("rep"), lax.axis_index("fs"), lax.axis_index("tp")
    z, y = lax.div(f, 2), lax.rem(f, 2)
    tok, D = x_ref.shape
    db = u_ref.shape[0]
    C, hc = pg.shape[0], pg.shape[2]
    hw, half, wide = C * hc, tok // 2, 2 * tok
    n = 2 * Z
    xdev, ydev, tdev = (1 - r, f, t), (r, f + 1 - 2 * y, t), (r, f, 1 - t)

    def zdev(s):
        return (r, f + 2 * s, t)

    low = z < Z // 2
    m = jnp.where(low, z, Z - 1 - z)
    near = (jnp.where(low, 0, 1), jnp.where(low, 1, -1))
    far = (1 - near[0], -near[1])

    ahead = {1: z < Z - 1, -1: z > 0}

    def remote(src, dst, ssem, rsem, dev):
        return pltpu.make_async_remote_copy(
            src_ref=src, dst_ref=dst, send_sem=ssem, recv_sem=rsem,
            device_id=dev, device_id_type=MESH,
        )

    def go(make):
        make().start()

    def span(at_, size):
        return pl.ds(pl.multiple_of(at_, size), size)

    def blk(b):
        return span(b * db, db)

    def hid(q, ch):
        return span(q * hw + ch * hc, hc)

    mine, other = 2 * r + y, 2 * r + 1 - y

    def held(g, ch, b):
        return ug.at[ch, blk(b), :] if g == 0 else dg.at[ch, :, blk(b)]

    spare = (uo, do)
    weights = (u_ref, d_ref)

    def strip(g, ref, q, ch):
        return ref.at[:, hid(q, ch)] if g == 0 else ref.at[hid(q, ch), :]

    own_x, own_c = xg.at[pl.ds(0, tok), :], cg.at[pl.ds(0, tok), :]
    loads = {}
    for ch in range(C):
        for g in range(2):
            loads["other", ch, g] = (strip(g, weights[g], other, ch), spare[g].at[ch])
            loads["mine", ch, g] = (strip(g, weights[g], mine, ch), held(g, ch, f))
        if ch == 0:
            loads["x"] = (x_ref, own_x)
            loads["c"] = (c_ref, own_c)
    loads = {
        key: pltpu.make_async_copy(src, dst, ld_s.at[i])
        for i, (key, (src, dst)) in enumerate(loads.items())
    }
    for copy in loads.values():
        copy.start()

    barrier = pltpu.get_barrier_semaphore()

    def greet(dev):
        pl.semaphore_signal(barrier, inc=1, device_id=dev, device_id_type=MESH)

    for dev in (xdev, ydev, tdev):
        greet(dev)
    for s in (1, -1):
        pl.when(ahead[s])(functools.partial(greet, zdev(s)))
    pl.semaphore_wait(barrier, 3 + sum(jnp.where(ahead[s], 1, 0) for s in (1, -1)))

    def swap(ch, g):
        return remote(spare[g].at[ch], held(g, ch, f), out_s.at[0], yw_r.at[ch, g], ydev)

    def origin(s, k, e):
        return f - 2 * s * k + e * (1 - 2 * y)

    def pass_on(ch, g, s, k, e):
        block = held(g, ch, origin(s, k, e))
        i = (ch, z - s * k, e, g)
        return remote(block, block, out_s.at[(3 - s) // 2], zg_r.at[i], zdev(s))

    def landed(ch, g, s, k, e):
        block = held(g, ch, origin(s, k, e))
        i = (ch, z - s * k, e, g)
        return remote(block, block, out_s.at[(3 - s) // 2], zg_r.at[i], zdev(s))

    def begin(ch, g, e, also=None):
        for s in (1, -1):
            cond = ahead[s] if also is None else ahead[s] & also
            pl.when(cond)(functools.partial(
                go, functools.partial(pass_on, ch, g, s, 0, e)))

    level = [m == m0 for m0 in range(Z // 2)]
    reached = {}
    for k in range(1, Z):
        reached[1, k], reached[-1, k] = z >= k, z < Z - k
    passing = {key: reached[key] & ahead[key[0]] for key in reached}

    outward = {1: low, -1: jnp.logical_not(low)}
    split = {}
    for (s, k), cond in passing.items():
        split[s, k, 0] = cond & outward[s]
        split[s, k, 1] = cond & outward[-s]

    def relay(ch, g, k, es=(0, 1), toward=None):
        for e in es:
            for s in (1, -1):
                cond = passing[s, k] if toward is None else split[s, k, toward]

                @pl.when(cond)
                def _():
                    landed(ch, g, s, k, e).wait_recv()
                    go(functools.partial(pass_on, ch, g, s, k, e))

    def collect(ch, g):
        for k in range(1, Z):
            for e in range(2):
                for s in (1, -1):

                    @pl.when(reached[s, k] & jnp.logical_not(ahead[s]))
                    def _():
                        landed(ch, g, s, k, e).wait_recv()

    def swapped(ch, g, also=None):
        begin(ch, g, 1, also)

    def rows(k, dt, part=(0, 2)):
        lo, hi = part
        return pl.ds((2 * k + dt) * tok + lo * half, (hi - lo) * half)

    def quarter(i):
        return span(jnp.where(low, Z - 1 - i, i) * 2 * db, 2 * db)

    A, B, AB = (0, 1), (1, 2), (0, 2)

    def hop(sems, i, dev, full, src, dst, cols):
        def make():
            where = slice(None) if cols is None else quarter(cols)
            return remote(
                full.at[rows(*src), where], full.at[rows(*dst), where],
                sems[0], sems[1].at[i], dev,
            )

        return make

    X, Y, S = (out_s.at[3], tx_r), (out_s.at[4], ty_r), (out_s.at[5], tt_r)
    moves = {}
    for i, part in enumerate((A, B)):
        moves["x", "x", i] = hop(X, i, xdev, xg, (0, 0, part), (1, 0, part), None)
        moves["y", "x", i] = hop(Y, i, ydev, xg, (0, 0, part), (2, 0, part), None)
        moves["d", "x", i] = hop(X, 2 + i, xdev, xg, (2, 0, part), (3, 0, part), None)
    moves["s", "x", 0] = hop(S, 0, tdev, xg, (0, 0, AB), (0, 1, AB), None)
    moves["s", "c", 0] = hop(S, 1, tdev, cg, (0, 0, AB), (0, 1, AB), None)
    for k in range(1, 4):
        moves["s", "x", k] = hop(S, 1 + k, tdev, xg, (k, 0, AB), (k, 1, AB), None)
    for i in range(Z):
        for p, (xp, yp) in enumerate(((B, A), (A, B))):
            moves["x%d" % p, "c", i] = hop(X, 4 + 3 * i + p, xdev, cg, (0, 0, xp), (1, 0, xp), i)
            moves["y%d" % p, "c", i] = hop(Y, 2 + 3 * i + p, ydev, cg, (0, 0, yp), (2, 0, yp), i)
        moves["dx", "c", i] = hop(X, 6 + 3 * i, xdev, cg, (2, 0, A), (3, 0, A), i)
        moves["dy", "c", i] = hop(Y, 4 + 3 * i, ydev, cg, (1, 0, B), (3, 0, B), i)
        for k in range(1, 4):
            moves["s%d" % k, "c", i] = hop(
                S, 5 + i, tdev, cg, (k, 0, AB), (k, 1, AB), i)

    def start(*key):
        go(moves[key])

    def arrive(*key):
        moves[key]().wait_recv()

    def flip(k):
        part = pl.ds(k * wide, wide)

        @pl.loop(0, n)
        def _(b):
            xt[blk(b), part] = xg[part, blk(b)].T

    def forward(ch, first, last):
        @pl.loop(first, last, unroll=2 if (last - first) % 2 == 0 else 1)
        def _(k):
            part = span(k * wide, wide)
            active = jnp.maximum(
                jnp.dot(xg[part, :], ug[ch], preferred_element_type=F32), 0.0)
            pre[ch, part, :] = active
            at[ch, :, part] = (active * active).astype(BF16).T

    def backward(ch):
        @pl.loop(0, 4, unroll=2)
        def _(k):
            part = span(k * wide, wide)
            val = lax.dot_general(cg[part, :], dg[ch], NT, preferred_element_type=F32)
            pg[ch, part, :] = (2.0 * pre[ch, part, :] * val).astype(BF16)

    def grad(ch, g, b):
        if g == 0:
            return jnp.dot(xt[blk(b), :], pg[ch], preferred_element_type=F32)
        return jnp.dot(at[ch], cg[:, blk(b)], preferred_element_type=F32)

    out_buf, in_buf, fin = (su, sd), (ru, rd), (fu, fd)

    def partial_copy(ch, g, way, j, e):
        d, s = way
        return remote(
            out_buf[g].at[d, j, ch, e], in_buf[g].at[d, j, ch, e],
            out_s.at[6], rs_r.at[j + d * (Z - 2 * j), ch, g, e], zdev(s))

    def side_of(e):
        return e * y + (1 - e) * (1 - y)

    def reduce(ch, g, way, j, m0, es=None):
        cond = level[m0]
        to = jnp.where(way[1] > 0, Z - 1 - j, j)
        more = m0 > 0 or way is far

        def step(e):
            val = grad(ch, g, 2 * to + side_of(e))
            if more:
                partial_copy(ch, g, way, j, e).wait_recv()
                val = val + in_buf[g][way[0], j, ch, e].astype(F32)
            out_buf[g][way[0], j, ch, e] = val.astype(BF16)
            partial_copy(ch, g, way, j, e).start()

        if es is None:
            pl.loop(0, 2)(step)
        else:
            for e in es:
                step(e)

    outs, passed = (gu_ref, gd_ref), (yu, yd)

    def store(ch, g, e):
        if ch == C:
            return pltpu.make_async_copy(igo, ig_ref, st_s.at[1])
        src = passed[g].at[ch] if e else fin[g].at[ch, 1]
        dst = strip(g, outs[g], other if e else mine, ch)
        return pltpu.make_async_copy(src, dst, st_s.at[0])

    def final_y(ch, g):
        return remote(
            fin[g].at[ch, 0], passed[g].at[ch], out_s.at[7], fy_r.at[ch, g], ydev)

    def final_x(ch, g, e):
        src = passed[g].at[ch] if e else fin[g].at[ch, 1]
        return remote(
            src, strip(g, outs[g], other if e else mine, ch), out_s.at[7], fx_r.at[0], xdev)

    def finish(ch, g, m0, between=None):
        cond = level[m0]
        ways = [(far, m0)] + ([(near, Z - 1 - m0)] if m0 else [])
        for e in range(2):
            val = grad(ch, g, 2 * z + side_of(e))
            for way, j in ways:
                partial_copy(ch, g, way, j, e).wait_recv()
                val = val + in_buf[g][way[0], j, ch, e].astype(F32)
            fin[g][ch, e] = val.astype(BF16)
            if e == 0:
                go(functools.partial(final_y, ch, g))
                if between:
                    between()
            else:
                go(functools.partial(final_x, ch, g, 0))
        store(ch, g, 0).start()

    def spread(ch, g, m0):
        final_y(ch, g).wait_recv()
        go(functools.partial(final_x, ch, g, 1))
        store(ch, g, 1).start()

    def cols(p):
        return pl.ds(p * (D // 2), D // 2)

    def ig_copy(i):
        part = cols((i + 1) % 2)
        if i > 6:
            part = cols(i - 7)
            src, dst = igp.at[1, :, :, part], itr.at[:, :, part]
            return remote(src, dst, out_s.at[8], ig_r.at[i - 1], tdev)
        kind = (i - 1) // 2
        if kind < 2:
            src, dst = isum.at[3 - kind, :, part], igot.at[1 - kind, :, part]
        else:
            src, dst = ipt.at[:, part], ift.at[:, part]
        return remote(src, dst, out_s.at[8], ig_r.at[i - 1], ydev if kind < 2 else xdev)

    def ig_go(i):
        go(functools.partial(ig_copy, i))

    def ig_part(dt, p):
        @pl.loop(p * (n // 2), (p + 1) * (n // 2), unroll=n // 2)
        def _(b):
            val = 0.0
            for ch in range(C):
                lhs = jnp.concatenate([pg[ch, rows(k, dt), :] for k in range(4)], 0)
                val = val + lax.dot_general(
                    lhs, ug[ch, blk(b), :], NT, preferred_element_type=F32)
            val = val.astype(BF16)
            for k in range(4):
                igp[dt, k, :, blk(b)] = val[k * tok:(k + 1) * tok]

        if dt:
            ig_go(7 + p)

    def ig_first(p):
        ig_copy(7 + p).wait_recv()

        @pl.loop(0, 4)
        def _(k):
            val = igp[0, k, :, cols(p)].astype(F32) + itr[k, :, cols(p)].astype(F32)
            isum[k, :, cols(p)] = val.astype(BF16)

    def ig_diag(p):
        ig_go(1 + p)

    def ig_more(p):
        ig_go(3 + p)

    def ig_second(p):
        ig_copy(1 + p).wait_recv()
        val = isum[1, :, cols(p)].astype(F32) + igot[1, :, cols(p)].astype(F32)
        ipt[:, cols(p)] = val.astype(BF16)
        ig_go(5 + p)

    def ig_last():
        for i in range(3, 7):
            ig_copy(i).wait_recv()
        val = isum[0].astype(F32) + igot[0].astype(F32) + ift[...].astype(F32)
        igo[...] = val.astype(BF16)
        store(C, 0, 0).start()

    edge, inner = level[0], m > 0
    last = C - 1

    units = [(ch, g) for ch in range(C) for g in range(2)]

    loads["other", 0, 0].wait()
    go(functools.partial(swap, 0, 0))
    loads["mine", 0, 0].wait()
    begin(0, 0, 0)
    loads["x"].wait()
    for i in range(2):
        start("x", "x", i)
        start("y", "x", i)
    loads["mine", 0, 1].wait()
    begin(0, 1, 0)
    start("s", "x", 0)
    loads["c"].wait()
    start("s", "c", 0)
    for unit in units[1:]:
        loads[("other",) + unit].wait()
        go(functools.partial(swap, *unit))
        if unit != units[1]:
            loads[("mine",) + unit].wait()

    swap(0, 0).wait_recv()
    begin(0, 0, 1)
    for unit in units[2:]:
        begin(*unit, 0, edge)
    relay(0, 0, 1)
    arrive("s", "x", 0)
    arrive("s", "c", 0)
    flip(0)
    arrive("y", "x", 0)
    start("d", "x", 0)
    for k in range(2, Z - 1):
        relay(0, 0, k)
    for unit in units[2:3]:
        begin(*unit, 0, inner)
    for i in range(2):
        arrive("x", "x", i)
    start("s", "x", 1)
    arrive("y", "x", 1)
    start("d", "x", 1)

    def offer(i):
        for way in ("x0", "y0", "x1", "y1"):
            start(way, "c", i)

    offer(0)
    start("s", "x", 2)
    swap(0, 1).wait_recv()
    begin(0, 1, 1)
    relay(0, 1, 1, (0,))
    arrive("s", "x", 1)
    flip(1)
    for k in range(2, Z - 1):
        relay(0, 1, k, (0,))
    relay(0, 1, 1, (1,))
    arrive("s", "x", 2)
    flip(2)
    collect(0, 0)
    forward(0, 0, 3)
    for unit in units[2:]:
        swap(*unit).wait_recv()
        begin(*unit, 1, edge)
    for i in range(2):
        arrive("d", "x", i)
    start("s", "x", 3)

    def ready(i):
        three = cg.at[pl.ds(0, 3 * tok), quarter(i)]
        remote(three, three, out_s.at[5], tt_r.at[5 + i], tdev).wait_recv()
        if i < Z - 1:
            pl.when(edge)(functools.partial(reduce, 0, 1, near, i, 0))

    tasks = [(unit, k) for unit in units[2:] for k in range(1, Z - 1)]
    for i in range(Z):
        arrive("x0", "c", i)
        start("dy", "c", i)
        arrive("y0", "c", i)
        start("dx", "c", i)
        if i + 1 < Z:
            offer(i + 1)
        if i == 0:
            for k in range(2, Z - 1):
                relay(0, 1, k, (1,))
            for unit in units[2:]:
                if unit != units[2]:
                    begin(*unit, 0, inner)
                begin(*unit, 1, inner)
            for unit in units[2:]:
                for k in range(1, Z // 2):
                    relay(*unit, k, toward=0)
            arrive("s", "x", 3)
            flip(3)
            forward(0, 3, 4)
        else:
            if i > 1:
                ready(i - 1)
            if i == Z - 1:
                for m0 in range(1, Z // 2):
                    pl.when(level[m0])(functools.partial(reduce, 0, 1, near, 0, m0))
        arrive("x1", "c", i)
        start("s1", "c", i)
        arrive("y1", "c", i)
        start("s2", "c", i)
        arrive("dy", "c", i)
        arrive("dx", "c", i)
        start("s3", "c", i)
        if i == 0:
            ready(0)
        if i == 1 and tasks:
            unit, k = tasks.pop(0)
            relay(*unit, k, toward=1)
    if Z > 1:
        ready(Z - 1)

    def edges():
        collect(0, 1)
        backward(0)
        for j in range(Z - 1):
            reduce(0, 0, near, j, 0)
        for ch in range(1, C):
            collect(ch, 0)
            forward(ch, 0, 4)
            for j in range(Z - 1):
                reduce(ch, 1, near, j, 0)
            collect(ch, 1)
            backward(ch)
            if ch < C - 1:
                for j in range(Z - 1):
                    reduce(ch, 0, near, j, 0)
        ig_part(1, 0)
        ig_part(1, 1)

        def meanwhile():
            ig_part(0, 0)
            ig_first(0)
            ig_diag(0)
            ig_part(0, 1)

        finish(0, 1, 0, meanwhile)
        ig_first(1)
        if C > 1:
            for j in range(Z - 1):
                reduce(C - 1, 0, near, j, 0)
        ig_diag(1)
        spread(0, 1, 0)
        finish(0, 0, 0)
        ig_second(0)
        for ch in range(1, C):
            finish(ch, 1, 0)
            spread(ch - 1, 0, 0)
            if ch == 1:
                ig_more(0)
                ig_second(1)
            spread(ch, 1, 0)
            finish(ch, 0, 0)
            if ch == 1:
                ig_more(1)
        if C == 1:
            ig_more(0)
            ig_second(1)
            ig_more(1)
        spread(C - 1, 0, 0)
        ig_last()

    def inside(m0):
        left = list(tasks)

        def relays(count):
            for _ in range(min(count, len(left))):
                unit, k = left.pop(0)
                relay(*unit, k, toward=1)

        def nears(ch, g, js):
            for j in js:
                reduce(ch, g, near, j, m0)

        def fars(ch, g):
            for j in range(m0):
                reduce(ch, g, far, j, m0)

        def both(ch, g):
            for e in range(2):
                for j in range(m0):
                    reduce(ch, g, far, j, m0, (e,))
                for j in rest:
                    reduce(ch, g, near, j, m0, (e,))

        first, rest = range(1), range(1, Z - 1 - m0)
        keep = (Z - 2) * (C > 1)
        relays(len(left) - keep)
        nears(0, 1, rest)
        relays(keep - 1)
        backward(0)
        for ch in range(1, C):
            forward(ch, 0, 4)
        relays(1)
        fars(0, 1)
        for ch in range(1, C):
            backward(ch)
        nears(0, 0, first)
        finish(0, 1, m0)
        both(0, 0)
        spread(0, 1, m0)
        for dt in (1, 0):
            for p in range(2):
                ig_part(dt, p)
        finish(0, 0, m0)
        for ch in range(1, C):
            nears(ch, 1, first)
            if ch == 1:
                for p in range(2):
                    ig_first(p)
                    ig_diag(p)
            spread(ch - 1, 0, m0)
            both(ch, 1)
            if ch == 1:
                ig_second(0)
            reduce(ch, 0, near, 0, m0, (0,))
            finish(ch, 1, m0)
            reduce(ch, 0, near, 0, m0, (1,))
            if ch == 1:
                ig_more(0)
                ig_second(1)
                ig_more(1)
            both(ch, 0)
            spread(ch, 1, m0)
            finish(ch, 0, m0)
        if C == 1:
            for p in range(2):
                ig_first(p)
                ig_diag(p)
                ig_more(p)
            for p in range(2):
                ig_second(p)
        spread(C - 1, 0, m0)
        ig_last()

    pl.when(edge)(edges)
    for m0 in range(1, Z // 2):
        pl.when(level[m0])(functools.partial(inside, m0))

    def settle():
        remote(gu_ref, gu_ref, out_s.at[7], fx_r.at[0], xdev).wait_recv()
        pltpu.make_async_copy(gu_ref, gu_ref, st_s.at[0]).wait()
        store(C, 0, 0).wait()

    def sent(i, count):
        some = xg.at[pl.ds(0, count), :]
        remote(some, some, out_s.at[i], out_s.at[i], xdev).wait_send()

    def drain():
        block = 4 * hw // n
        sent(0, block // 2)
        for z0 in range(Z - 1):
            pl.when(z == z0)(functools.partial(sent, 1, (z0 + 1) * block))
            pl.when(z == Z - 1 - z0)(functools.partial(sent, 2, (z0 + 1) * block))
        sent(3, 7 * half)
        sent(4, 5 * half)
        sent(5, 8 * tok)
        sent(6, (Z - 1) * block)
        sent(7, 3 * block // 2)
        sent(8, 7 * tok)

    settle()
    drain()


def ring_call(inputs, up_weight):
    R, n, T = axis_sizes()
    tok, D = inputs.shape
    db, hb = up_weight.shape[0], up_weight.shape[1] // R
    rows = R * T * tok
    C = tile_of(hb // 128, CHUNKS) if hb > 128 else 1
    w = hb // C
    V, S = pltpu.VMEM, pltpu.SemaphoreType.DMA
    hops = max(n // 2, 1)
    m = max(n - 1, 1)
    scratch = [
        V((n, rows, db), BF16), V((n, rows, db), BF16), V((n, db, rows), BF16),
        V((m, C, db, w), BF16), V((m, C, w, db), BF16),
        V((C, rows, w), F32), V((C, rows, w), F32), V((C, rows, w), BF16), V((C, w, rows), BF16),
        V((n, rows, db), BF16), V((max(T - 1, 1), n, R * tok, db), BF16),
        V((R, n, tok, db), BF16), V((max(R - 1, 1), n, tok, db), BF16),
        V((m, C, db, w), BF16), V((m, C, db, w), BF16),
        V((m, C, w, db), BF16), V((m, C, w, db), BF16),
        V((C, db, w), BF16), V((C, w, db), BF16),
        V((max(R - 1, 1), C, db, w), BF16), V((max(R - 1, 1), C, w, db), BF16),
        S((C, 4, hops)), S((C, 4, hops)), S((C, 4, hops)), S((C, 4, hops)),
        S((2, R)), S((2, R)), S((2, T, R)), S((2, T, R)),
        S((T,)), S((T,)), S((R,)), S((R,)), S((C, 2, R)), S((C, 2, R)),
    ]
    return functools.partial(ring_kernel, R, n, T), scratch, (R, hb), pltpu.VMEM


def finals_kernel(scale, *refs):
    sources, targets, raw, wide = refs[:3], refs[3:6], refs[6:9], refs[9:11]
    load, store = refs[11:]
    jobs = []
    for a in (1, 2, 0):
        rows = sources[a].shape[0]
        for p in range(PARTS):
            part = pl.ds(p * (rows // PARTS), rows // PARTS)
            jobs.append((a, p, part))
    loads = []
    for a, p, part in jobs:
        copy = pltpu.make_async_copy(
            sources[a].at[part, :], raw[a].at[part, :], load.at[a, p])
        copy.start()
        loads.append(copy)
    for (a, p, part), copy in zip(jobs, loads):
        copy.wait()
        ready = raw[a]
        if a:
            ready = wide[a - 1]
            ready[part, :] = raw[a][part, :].astype(F32) * scale
        copy = pltpu.make_async_copy(
            ready.at[part, :], targets[a].at[part, :], store.at[a])
        copy.start()
    for a in range(3):
        whole = wide[a - 1] if a else raw[a]
        pltpu.make_async_copy(whole, targets[a], store.at[a]).wait()


def finals_call(ig, gu, gd, scale):
    any_space = pl.BlockSpec(memory_space=pl.ANY)
    V, S = pltpu.VMEM, pltpu.SemaphoreType.DMA
    return pl.pallas_call(
        functools.partial(finals_kernel, scale),
        in_specs=[any_space] * 3,
        out_specs=(any_space,) * 3,
        out_shape=(
            jax.ShapeDtypeStruct(ig.shape, BF16),
            jax.ShapeDtypeStruct(gu.shape, F32),
            jax.ShapeDtypeStruct(gd.shape, F32),
        ),
        scratch_shapes=[
            V(ig.shape, BF16), V(gu.shape, BF16), V(gd.shape, BF16),
            V(gu.shape, F32), V(gd.shape, F32), S((3, PARTS)), S((3,)),
        ],
    )(ig, gu, gd)


def axis_sizes():
    return lax.axis_size("rep"), lax.axis_size("fs"), lax.axis_size("tp")


def plane_call(inputs, up_weight):
    R, n, T = axis_sizes()
    tok, D = inputs.shape
    db, HB = up_weight.shape
    Z, G = n // 2, 2 * R
    if R != 2 or T != 2 or n % 4 or tok % 32 or HB % (128 * G) or db % 128:
        return None
    hw = HB // G
    C = tile_of(hw // 128, CHUNKS)
    hc = hw // C
    rows = 8 * tok
    V, S = pltpu.VMEM, pltpu.SemaphoreType.DMA
    data = [
        ((rows, D), BF16), ((rows, D), BF16), ((D, rows), BF16),
        ((C, D, hc), BF16), ((C, hc, D), BF16),
        ((C, rows, hc), F32), ((C, rows, hc), BF16), ((C, hc, rows), BF16),
        ((2, 4, tok, D), BF16), ((4, tok, D), BF16), ((4, tok, D), BF16),
        ((2, tok, D), BF16), ((tok, D), BF16), ((tok, D), BF16),
        ((tok, D), BF16),
        ((2, Z - 1, C, 2, db, hc), BF16), ((2, Z - 1, C, 2, hc, db), BF16),
        ((2, Z - 1, C, 2, db, hc), BF16), ((2, Z - 1, C, 2, hc, db), BF16),
        ((C, 2, db, hc), BF16), ((C, 2, hc, db), BF16),
        ((C, db, hc), BF16), ((C, hc, db), BF16), ((C, db, hc), BF16), ((C, hc, db), BF16),
    ]
    size = sum(math.prod(s) * jnp.dtype(d).itemsize for s, d in data)
    if size > 50 * 2**20 or 4 * hw % n or (Z - 1) * 4 * hw > 8 * tok * n:
        return None
    sems = [
        (C, 2), (C, Z, 2, 2), (4 + 3 * Z,), (2 + 3 * Z,), (5 + Z,),
        (Z + 1, C, 2, 2), (C, 2), (1,), (8,),
    ]
    scratch = [V(s, d) for s, d in data] + [S((9,))] + [S(s) for s in sems]
    scratch += [S((4 * C + 2,)), S((2,))]
    return functools.partial(plane_kernel, Z), scratch, (1, HB), pl.ANY


def shards(inputs, cotangent, up_weight, down_weight):
    R, n, T = axis_sizes()
    tok, D = inputs.shape
    db = up_weight.shape[0]
    chosen = plane_call(inputs, up_weight) or ring_call(inputs, up_weight)
    body, scratch, (parts, hb), space = chosen
    spec = pl.BlockSpec(memory_space=space)
    ig, gu, gd = pl.pallas_call(
        body,
        out_shape=(
            jax.ShapeDtypeStruct((tok, D), BF16),
            jax.ShapeDtypeStruct((db, parts * hb), BF16),
            jax.ShapeDtypeStruct((parts * hb, db), BF16),
        ),
        in_specs=[spec] * 4,
        out_specs=(spec,) * 3,
        scratch_shapes=scratch,
        compiler_params=pltpu.CompilerParams(
            collective_id=0, has_side_effects=True, vmem_limit_bytes=60 * 2**20
        ),
    )(inputs, cotangent, up_weight, down_weight)
    total_tokens = tok * R * n * T
    loss_scale = 1.0 / math.sqrt(total_tokens)
    if space is pl.ANY:
        return finals_call(ig, gu, gd, loss_scale)
    return ig, gu.astype(F32) * loss_scale, gd.astype(F32) * loss_scale


def solution(mesh):
    token, up, down = P(("rep", "fs", "tp"), None), P("fs", "tp"), P("tp", "fs")
    return jax.shard_map(
        shards,
        mesh=mesh,
        in_specs=(token, token, up, down),
        out_specs=(token, up, down),
        check_vma=False,
    )
```
